32 devices in a mesh: sp: 16 (over z, y, x), tp: 2 (over core).
Axes of the slice: x: 2, y: 2, z: 4, core: 2. Of those that a mesh axis runs over, the one named last changes fastest.
Arguments:
- tokens: bfloat16 [6144, 2048], P('sp', 'tp'), may hold values from -6 to 6
- input_gain: float32 [2048], replicated, may hold values from 0.1 to 1.9
- query_weight: bfloat16 [2048, 1024], P(None, 'tp'), may hold values from -0.5 to 0.5
- query_rot_weight: bfloat16 [2048, 512], P(None, 'tp'), may hold values from -0.125 to 0.125
- kv_down: bfloat16 [2048, 256], replicated, may hold values from -0.5 to 0.5
- rot_down: bfloat16 [2048, 32], replicated, may hold values from -0.125 to 0.125
- kv_gain: float32 [256], replicated, may hold values from 0.1 to 1.9
- key_up: bfloat16 [256, 1024], P(None, 'tp'), may hold values from -0.5 to 0.5
- value_up: bfloat16 [256, 1024], P(None, 'tp'), may hold values from -4 to 4
- conv_value_weight: bfloat16 [2048, 1024], P(None, 'tp'), may hold values from -0.125 to 0.125
- conv_gate_weight: bfloat16 [2048, 1024], P(None, 'tp'), may hold values from -0.125 to 0.125
- conv_taps: float32 [31, 1024], P(None, 'tp'), may hold values from -8 to 8
- conv_ln_gain: float32 [1024], P('tp'), may hold values from 0.1 to 1.9
- conv_ln_bias: float32 [1024], P('tp'), may hold values from -3 to 3
- att_out_gain: float32 [1024], P('tp'), may hold values from 0.1 to 1.9
- conv_out_gain: float32 [1024], P('tp'), may hold values from 0.1 to 1.9
- att_out_weight: bfloat16 [1024, 2048], P('tp'), may hold values from -0.125 to 0.125
- conv_out_weight: bfloat16 [1024, 2048], P('tp'), may hold values from -0.125 to 0.125
Outputs:
- mixed: bfloat16 [6144, 2048], P('sp', 'tp')
The draws below stay inside these ranges and needn't reach their ends.
All inputs are finite; a program needn't handle non-finite values.
Results may differ from the reference program's by a relative error of at most 0.017.
Values may be sent and summed in bfloat16 or wider, within the bound.
A program may use at most 128 MiB of HBM per device.

```python
import math
import jax
import jax.numpy as jnp
from jax import lax

D_MODEL = 2048
HEADS = 16
NOPE_DIM = 64
ROT_DIM = 32
VALUE_DIM = 64
KV_RANK = 256
CONV_CH = 1024
KERNEL = 31
TOKENS = 6144
ATT_WIDTH = 1024
N_TP = 2


def latent_weights(key):
    down_map = jax.random.normal(jax.random.fold_in(key, 101), (D_MODEL, KV_RANK), jnp.float32) / math.sqrt(D_MODEL)
    upward = jax.random.normal(jax.random.fold_in(key, 102), (KV_RANK, HEADS * NOPE_DIM), jnp.float32) / math.sqrt(KV_RANK)
    return (jnp.clip(down_map, -0.5, 0.5), jnp.clip(upward, -0.5, 0.5))


def rising_scales(key, entries):
    position = jnp.arange(entries, dtype=jnp.float32) / max(entries - 1, 1)
    jitter = jax.random.uniform(key, (entries,), jnp.float32)
    return 10.0 ** (0.5 * position + 0.5 * jitter - 0.5)


def draw_tokens(key, part):
    base_draw = jax.random.normal(jax.random.fold_in(key, 1), (TOKENS, D_MODEL), jnp.float32)
    return jnp.clip(base_draw, -6.0, 6.0).astype(jnp.bfloat16)


def draw_query_weight(key, part):
    base_draw = jax.random.normal(jax.random.fold_in(key, 104), (D_MODEL, HEADS * NOPE_DIM), jnp.float32) / math.sqrt(D_MODEL)
    return jnp.clip(base_draw, -0.5, 0.5).astype(jnp.bfloat16)


def draw_kv_down(key, part):
    return latent_weights(key)[0].astype(jnp.bfloat16)


def draw_key_up(key, part):
    return latent_weights(key)[1].astype(jnp.bfloat16)


def draw_value_up(key, part):
    base_draw = jax.random.normal(jax.random.fold_in(key, 201), (KV_RANK, HEADS * VALUE_DIM), jnp.float32) / math.sqrt(KV_RANK)
    scales = jnp.repeat(rising_scales(jax.random.fold_in(key, 202), HEADS), VALUE_DIM)
    return jnp.clip(base_draw * scales[None, :], -4.0, 4.0).astype(jnp.bfloat16)


def draw_conv_taps(key, part):
    base_draw = jax.random.normal(jax.random.fold_in(key, 301), (KERNEL, CONV_CH), jnp.float32) / math.sqrt(KERNEL)
    scales = rising_scales(jax.random.fold_in(key, 302), CONV_CH)
    return jnp.clip(base_draw * scales[None, :], -8.0, 8.0).astype(jnp.float32)


def steps_of(stream_key, dims, shards, least, largest):
    def one(dim, parts):
        heights = jax.random.uniform(jax.random.fold_in(jax.random.fold_in(stream_key, 6), dim), (parts,), jnp.float32, least / len(shards), largest / len(shards))
        return jnp.repeat(jnp.exp(heights), dims[dim] // parts).reshape((-1,) + (1,) * (len(dims) - dim - 1))

    level = one(*shards[0])
    for cut in shards[1:]:
        level = level * one(*cut)
    return level


def centred(own_key, dims, width, limit, split=(), held_as=jnp.bfloat16):
    values = width * jax.random.normal(own_key, dims, jnp.float32)
    if split:
        values = values * steps_of(own_key, dims, split, -0.22, 0.18)
    return jnp.clip(values, -limit, limit).astype(held_as)


def setup_inputs(seed: int = 0) -> dict:
    key_of = jax.random.split(jax.random.key(seed), 19)
    tokens = draw_tokens(jax.random.fold_in(key_of[18], 71), 0)
    input_gain = jnp.clip(1.0 + 0.18 * jax.random.normal(key_of[1], (D_MODEL,), jnp.float32), 0.1, 1.9)
    query_weight = draw_query_weight(jax.random.fold_in(key_of[18], 71), 0)
    query_rot_weight = centred(key_of[3], (D_MODEL, HEADS * ROT_DIM), D_MODEL ** -0.5, 0.125, ((1, 2),))
    kv_down = draw_kv_down(jax.random.fold_in(key_of[18], 71), 0)
    rot_down = centred(key_of[5], (D_MODEL, ROT_DIM), D_MODEL ** -0.5, 0.125)
    kv_gain = jnp.clip(1.0 + 0.18 * jax.random.normal(key_of[6], (KV_RANK,), jnp.float32), 0.1, 1.9)
    key_up = draw_key_up(jax.random.fold_in(key_of[18], 71), 0)
    value_up = draw_value_up(jax.random.fold_in(key_of[18], 71), 0)
    conv_value_weight = centred(key_of[9], (D_MODEL, CONV_CH), D_MODEL ** -0.5, 0.125, ((1, 2),))
    conv_gate_weight = centred(key_of[10], (D_MODEL, CONV_CH), D_MODEL ** -0.5, 0.125, ((1, 2),))
    conv_taps = draw_conv_taps(jax.random.fold_in(key_of[18], 71), 0)
    conv_ln_gain = jnp.clip(1.0 + 0.18 * jax.random.normal(key_of[12], (CONV_CH,), jnp.float32), 0.1, 1.9)
    conv_ln_bias = centred(key_of[13], (CONV_CH,), 0.5, 3.0, ((0, 2),), jnp.float32)
    att_out_gain = jnp.clip(1.0 + 0.18 * jax.random.normal(key_of[14], (ATT_WIDTH,), jnp.float32), 0.1, 1.9)
    conv_out_gain = jnp.clip(1.0 + 0.18 * jax.random.normal(key_of[15], (CONV_CH,), jnp.float32), 0.1, 1.9)
    att_out_weight = centred(key_of[16], (ATT_WIDTH, D_MODEL), (ATT_WIDTH + CONV_CH) ** -0.5, 0.125, ((0, 2),))
    conv_out_weight = centred(key_of[17], (CONV_CH, D_MODEL), (ATT_WIDTH + CONV_CH) ** -0.5, 0.125, ((0, 2),))
    return {"tokens": tokens, "input_gain": input_gain, "query_weight": query_weight, "query_rot_weight": query_rot_weight, "kv_down": kv_down, "rot_down": rot_down, "kv_gain": kv_gain, "key_up": key_up, "value_up": value_up, "conv_value_weight": conv_value_weight, "conv_gate_weight": conv_gate_weight, "conv_taps": conv_taps, "conv_ln_gain": conv_ln_gain, "conv_ln_bias": conv_ln_bias, "att_out_gain": att_out_gain, "conv_out_gain": conv_out_gain, "att_out_weight": att_out_weight, "conv_out_weight": conv_out_weight}


norm_eps = 1e-06
rope_base = 10000.0

def lifted(array):
    return lax.optimization_barrier(array).astype(jnp.float32)

def rotary_tables(positions, half_dim):
    frequency = rope_base ** (-jnp.arange(half_dim, dtype=jnp.float32) / half_dim)
    angles = positions.astype(jnp.float32)[:, None] * frequency[None, :]
    return (jnp.cos(angles), jnp.sin(angles))

def rotate_half(values, cos_table, sine_table):
    half_dim = cos_table.shape[-1]
    front_half = values[..., :half_dim]
    back_half = values[..., half_dim:]
    return jnp.concatenate([front_half * cos_table - back_half * sine_table, back_half * cos_table + front_half * sine_table], axis=-1)

def reference(tokens, input_gain, query_weight, query_rot_weight, kv_down, rot_down, kv_gain, key_up, value_up, conv_value_weight, conv_gate_weight, conv_taps, conv_ln_gain, conv_ln_bias, att_out_gain, conv_out_gain, att_out_weight, conv_out_weight):
    tokens_wide = tokens.astype(jnp.float32)
    row_scale = lax.rsqrt(lax.optimization_barrier(jnp.mean(tokens_wide * tokens_wide, axis=1, keepdims=True)) + norm_eps)
    scaled = (tokens_wide * input_gain[None, :]).astype(jnp.bfloat16)

    def project(weight):
        return jnp.dot(scaled.astype(jnp.float32), weight.astype(jnp.float32), preferred_element_type=jnp.float32)
    positions = jnp.arange(TOKENS, dtype=jnp.int32)
    cos_table, sine_table = rotary_tables(positions, ROT_DIM // 2)
    queries = (project(query_weight) * row_scale).astype(jnp.bfloat16).reshape(TOKENS, HEADS, NOPE_DIM)
    query_rot = rotate_half((project(query_rot_weight) * row_scale).reshape(TOKENS, HEADS, ROT_DIM), cos_table[:, None, :], sine_table[:, None, :]).astype(jnp.bfloat16)
    latent_raw = project(kv_down)
    latent = (latent_raw * lax.rsqrt(lax.optimization_barrier(jnp.mean(latent_raw * latent_raw, axis=1, keepdims=True)) + norm_eps) * kv_gain[None, :]).astype(jnp.bfloat16)
    key_rot = rotate_half(project(rot_down) * row_scale, cos_table, sine_table).astype(jnp.bfloat16)
    keys = jnp.dot(latent.astype(jnp.float32), key_up.astype(jnp.float32), preferred_element_type=jnp.float32).astype(jnp.bfloat16).reshape(TOKENS, HEADS, NOPE_DIM)
    values = jnp.dot(latent.astype(jnp.float32), value_up.astype(jnp.float32), preferred_element_type=jnp.float32).astype(jnp.bfloat16).reshape(TOKENS, HEADS, VALUE_DIM)
    queries_heads = jnp.transpose(lifted(queries), (1, 0, 2))
    qrot_heads = jnp.transpose(lifted(query_rot), (1, 0, 2))
    keys_heads = jnp.transpose(lifted(keys), (1, 0, 2))
    values_heads = jnp.transpose(lifted(values), (1, 0, 2))
    krot_wide = lifted(key_rot)
    inv_scale = 1.0 / math.sqrt(NOPE_DIM + ROT_DIM)
    block_len = min(512, TOKENS)
    pieces = []
    for block_idx in range(TOKENS // block_len):
        row_low = block_idx * block_len
        row_high = row_low + block_len
        key_pos = jnp.arange(row_high, dtype=jnp.int32)
        query_pos = jnp.arange(row_low, row_high, dtype=jnp.int32)
        visible = key_pos[None, :] <= query_pos[:, None]
        krot_part = krot_wide[:row_high]

        def one_head(members):
            query_head, qrot_head, key_head, value_head = members
            scores = (jnp.dot(query_head, key_head.T) + jnp.dot(qrot_head, krot_part.T)) * inv_scale
            row_max = lax.optimization_barrier(jnp.max(jnp.where(visible, scores, -jnp.inf), axis=1, keepdims=True))
            exp_scores = jnp.where(visible, jnp.exp(scores - row_max), 0.0)
            denominator = lax.optimization_barrier(jnp.sum(exp_scores, axis=1, keepdims=True))
            weighted = jnp.dot(lifted(exp_scores.astype(jnp.bfloat16)), value_head)
            return weighted / denominator
        head_out = lax.map(one_head, (queries_heads[:, row_low:row_high], qrot_heads[:, row_low:row_high], keys_heads[:, :row_high], values_heads[:, :row_high]))
        pieces.append(jnp.transpose(head_out, (1, 0, 2)).astype(jnp.bfloat16))
    attended = jnp.concatenate(pieces, axis=0).reshape(TOKENS, ATT_WIDTH)
    gated_input = (project(conv_value_weight) * row_scale * jax.nn.sigmoid(project(conv_gate_weight) * row_scale)).astype(jnp.bfloat16)
    padded = jnp.pad(lifted(gated_input), ((KERNEL - 1, 0), (0, 0)))
    conv_out = jnp.zeros((TOKENS, CONV_CH), jnp.float32)
    for tap_idx in range(KERNEL):
        conv_out = conv_out + conv_taps[tap_idx][None, :] * padded[tap_idx:tap_idx + TOKENS]
    mean_val = lax.optimization_barrier(jnp.mean(conv_out, axis=1, keepdims=True))
    spread = lax.optimization_barrier(jnp.mean(conv_out * conv_out, axis=1, keepdims=True)) - mean_val * mean_val
    swished = jax.nn.silu((conv_out - mean_val) * lax.rsqrt(spread + norm_eps) * conv_ln_gain[None, :] + conv_ln_bias[None, :])
    conv_mixed = (swished * lax.rsqrt(lax.optimization_barrier(jnp.mean(swished * swished, axis=1, keepdims=True)) + norm_eps) * conv_out_gain[None, :]).astype(jnp.bfloat16)
    att_wide = lifted(attended)
    att_mixed = (att_wide * lax.rsqrt(lax.optimization_barrier(jnp.mean(att_wide * att_wide, axis=1, keepdims=True)) + norm_eps) * att_out_gain[None, :]).astype(jnp.bfloat16)
    att_share = ATT_WIDTH // N_TP
    conv_share = CONV_CH // N_TP
    result = jnp.zeros((TOKENS, D_MODEL), jnp.float32)
    for group_idx in range(N_TP):
        att_low = group_idx * att_share
        conv_low = group_idx * conv_share
        partial_value = jnp.dot(att_mixed[:, att_low:att_low + att_share].astype(jnp.float32), att_out_weight[att_low:att_low + att_share].astype(jnp.float32), preferred_element_type=jnp.float32) + jnp.dot(conv_mixed[:, conv_low:conv_low + conv_share].astype(jnp.float32), conv_out_weight[conv_low:conv_low + conv_share].astype(jnp.float32), preferred_element_type=jnp.float32)
        result = result + lifted(partial_value.astype(jnp.bfloat16))
    return result.astype(jnp.bfloat16)
```

```python
import math

import jax
import jax.numpy as jnp
import numpy as np
from jax import lax
from jax.experimental import pallas as pl
from jax.experimental.pallas import tpu as pltpu
from jax.sharding import PartitionSpec as P

D_MODEL = 2048
NOPE_DIM = 64
ROT_DIM = 32
VALUE_DIM = 64
CONV_CH = 1024
KERNEL = 31
ATT_WIDTH = 1024


norm_eps = 1e-06
far_below = -1e30
rope_base = 10000.0


def shifted(block, axis, distance):
    devices = range(lax.axis_size(axis))
    route = [(i - distance, i) for i in devices if i - distance in devices]
    return lax.ppermute(block, axis, route)


def rotary_tables(positions, half_dim):
    frequency = rope_base ** (-jnp.arange(half_dim, dtype=jnp.float32) / half_dim)
    angles = positions.astype(jnp.float32)[:, None] * frequency[None, :]
    return (jnp.cos(angles), jnp.sin(angles))


def rotate_half(values, cos_table, sine_table):
    half_dim = cos_table.shape[-1]
    front_half = values[..., :half_dim]
    back_half = values[..., half_dim:]
    return jnp.concatenate(
        [
            front_half * cos_table - back_half * sine_table,
            back_half * cos_table + front_half * sine_table,
        ],
        axis=-1,
    )


MESH = pl.DeviceIdType.MESH


def push(src, dst, send, recv, target):
    return pltpu.make_async_remote_copy(
        src_ref=src,
        dst_ref=dst,
        send_sem=send,
        recv_sem=recv,
        device_id=target,
        device_id_type=MESH,
    )


def other_core():
    return {"sp": lax.axis_index("sp"), "tp": 1 - lax.axis_index("tp")}


PLANE = 4


def layer_kernel(
    tok_hbm, gain_ref, kv_gain_ref, base_ref, seat_ref, taps_ref, ln_gain_ref, ln_bias_ref,
    att_gain_ref, conv_gain_ref,
    kvd_hbm, rotw_hbm, cgw_hbm, cvw_hbm, qw_hbm, qrw_hbm, kup_hbm, vup_hbm, att_hbm, conv_hbm,
    out_ref,
    kvd, rotw, cgw, cvw, qw, qrw, kup, vup, att_w, conv_w, vup_t,
    tok, landed, scaled, narrow, gated, rim, wide, conv, sq_mine, sq_other,
    lat_ref, q2, kn, kr, vt, run_max, acc, s_ref, att_t, end_mine, end_other, part, arrived,
    w_sem, tok_load, tok_send, tok_recv, rim_send, rim_recv, sq_send, sq_recv,
    csq_send, csq_recv, asq_send, asq_recv, part_send, part_recv,
    col_send, plane_send, core_send, link_recv, core_recv,
):
    mine = lax.axis_index("tp")
    me = lax.axis_index("sp")
    seats = lax.axis_size("sp")
    rows, width = tok.shape
    blocks = lat_ref.shape[0]
    rank = kvd.shape[1]
    layers = blocks // PLANE
    layer = me // PLANE
    spot = me % PLANE
    height = lat_ref.shape[1] // 2
    half = pl.ds(pl.multiple_of(mine * height, 16), height)
    other = other_core()
    ahead = {"sp": (me + 1) % seats, "tp": mine}
    behind = {"sp": (me + seats - 1) % seats, "tp": mine}

    loads = [
        pltpu.make_async_copy(src, dst, w_sem.at[index])
        for index, (src, dst) in enumerate(
            (
                (kvd_hbm, kvd), (rotw_hbm, rotw), (cgw_hbm, cgw), (cvw_hbm, cvw),
                (qw_hbm, qw), (qrw_hbm, qrw), (kup_hbm, kup), (vup_hbm, vup),
                (att_hbm, att_w), (conv_hbm, conv_w),
            )
        )
    ]
    fetch = pltpu.make_async_copy(tok_hbm, tok, tok_load)
    fetch.start()
    for load in loads:
        load.start()

    def spot_at(distance):
        return (spot + distance) % PLANE

    def at(layer_id, spot_id):
        return {"sp": layer_id * PLANE + spot_id, "tp": mine}

    barrier = pltpu.get_barrier_semaphore()
    peers = (
        [at((layer + d) % layers, spot) for d in range(1, layers)]
        + [at(layer, spot_at(d)) for d in range(1, PLANE)]
        + [other]
    )
    for peer in peers:
        pl.semaphore_signal(barrier, inc=1, device_id=peer, device_id_type=MESH)

    @pl.when(me < seats - 1)
    def _():
        pl.semaphore_signal(barrier, inc=1, device_id=ahead, device_id_type=MESH)

    @pl.when(me > 0)
    def _():
        pl.semaphore_signal(barrier, inc=1, device_id=behind, device_id_type=MESH)

    q2[...] = jnp.zeros(q2.shape, jnp.bfloat16)
    pairs, _, both = q2.shape
    keys_wide = kn.shape[0]
    ones_low = VALUE_DIM
    ones_high = vt.shape[1] - VALUE_DIM
    vt[:, ones_low:ones_high, :] = jnp.ones((pairs, ones_high - ones_low, keys_wide), jnp.bfloat16)
    pl.semaphore_wait(
        barrier, len(peers) + jnp.minimum(me, 1) + jnp.minimum(seats - 1 - me, 1)
    )
    fetch.wait()
    tok_copy = push(tok, landed, tok_send, tok_recv, other)
    tok_copy.start()

    def place(block, index):
        cols = pl.ds(pl.multiple_of(index * width, 128), width)
        full = block[...].astype(jnp.float32)
        scaled[:, cols] = (full * gain_ref[:, cols]).astype(jnp.bfloat16)
        return jnp.sum(full * full, axis=1, keepdims=True)

    squares = place(tok, mine)
    loads[7].wait()
    vup_t[...] = vup[...].astype(jnp.float32).T.astype(jnp.bfloat16)
    column = lax.broadcasted_iota(jnp.int32, seat_ref.shape, 1)
    seat_turn = jnp.sum(
        jnp.where(column == me, seat_ref[...], 0.0), axis=1, keepdims=True
    )
    turn = ROT_DIM // 2
    seat_cos, seat_sin = seat_turn[:turn], seat_turn[turn:]
    base_cos, base_sin = base_ref[:turn], base_ref[turn:]
    cos_table = seat_cos * base_cos - seat_sin * base_sin
    sin_table = seat_sin * base_cos + seat_cos * base_sin

    def rotate(block):
        front = block[:turn]
        back = block[turn : 2 * turn]
        return jnp.concatenate(
            [front * cos_table - back * sin_table, back * cos_table + front * sin_table], axis=0
        )

    tok_copy.wait()
    squares = squares + place(landed, 1 - mine)
    row_scale = lax.rsqrt(squares / (2 * width) + norm_eps)

    def project(weight):
        return jnp.dot(scaled[...], weight[...], preferred_element_type=jnp.float32)

    loads[0].wait()
    loads[1].wait()
    raw = project(kvd)
    latent = (
        raw
        * lax.rsqrt(jnp.mean(raw * raw, axis=1, keepdims=True) + norm_eps)
        * kv_gain_ref[...]
    )
    lat_ref[me, :rows, :] = latent.astype(jnp.bfloat16)
    narrow[...] = jnp.broadcast_to(row_scale, narrow.shape)
    key_turn = lax.dot_general(
        rotw[...], scaled[...], (((1,), (1,)), ((), ())), preferred_element_type=jnp.float32
    )
    key_rot = rotate(key_turn * narrow[...].T[:ROT_DIM]).astype(jnp.bfloat16)
    across = rank // 128
    for piece in range(across * ((rows // 128 + across - 1) // across)):
        band = rows + piece // across * ROT_DIM
        lanes = slice(piece % across * 128, piece % across * 128 + 128)
        lat_ref[me, band : band + ROT_DIM, lanes] = (
            key_rot[:, piece * 128 : piece * 128 + 128]
            if piece < rows // 128
            else jnp.zeros((ROT_DIM, 128), jnp.bfloat16)
        )

    def column_copy(distance):
        return push(
            lat_ref.at[me, half],
            lat_ref.at[me, half],
            col_send.at[distance - 1],
            link_recv.at[me],
            at(jnp.minimum(layer + distance, layers - 1), spot),
        )

    def plane_copy(block, distance):
        return push(
            lat_ref.at[block, half],
            lat_ref.at[block, half],
            plane_send.at[block // PLANE, distance - 1],
            link_recv.at[block],
            at(layer, spot_at(distance)),
        )

    def core_copy(block):
        spread = lat_ref.at[block, half]
        return push(spread, spread, core_send.at[block], core_recv.at[block], other)

    for d in range(1, PLANE):
        plane_copy(me, d).start()
    for d in range(1, layers):

        @pl.when(layer + d < layers)
        def _(d=d):
            column_copy(d).start()

    def arrive(block):
        spread = lat_ref.at[block, half]
        push(spread, spread, core_send.at[block], link_recv.at[block], other).wait_recv()

    def relay(step):
        @pl.when(step <= layer)
        def _():
            block = (layer - step) * PLANE + spot
            arrive(block)
            for d in range(1, PLANE):
                plane_copy(block, d).start()
            core_copy(block).start()

    def hand_over(step):
        @pl.when(step <= layer)
        def _():
            for d in range(1, PLANE):
                block = (layer - step) * PLANE + spot_at(d)
                arrive(block)
                core_copy(block).start()

    loads[2].wait()
    loads[3].wait()
    gate = project(cgw) * row_scale
    gated[...] = (project(cvw) * row_scale * jax.nn.sigmoid(gate)).astype(jnp.bfloat16)
    edge = rim.shape[0]
    rim_copy = push(gated.at[pl.ds(rows - edge, edge)], rim, rim_send, rim_recv, ahead)

    @pl.when(me < seats - 1)
    def _():
        rim_copy.start()

    loads[4].wait()
    loads[5].wait()
    query_scale = row_scale * (math.log2(math.e) / math.sqrt(NOPE_DIM + ROT_DIM))
    plain = (project(qw) * query_scale).T.astype(jnp.bfloat16)
    turned = (project(qrw) * query_scale).T
    for head in range(2 * pairs):
        side = head % 2
        cols = slice(side * rows, (side + 1) * rows)
        q2[head // 2, side * NOPE_DIM : (side + 1) * NOPE_DIM, cols] = plain[
            head * NOPE_DIM : (head + 1) * NOPE_DIM
        ]
        q2[head // 2, 2 * NOPE_DIM : 2 * NOPE_DIM + ROT_DIM, cols] = rotate(
            turned[head * ROT_DIM : (head + 1) * ROT_DIM]
        ).astype(jnp.bfloat16)

    relay(1)

    @pl.when(me > 0)
    def _():
        rim_copy.wait_recv()

    @pl.when(me == 0)
    def _():
        rim[...] = jnp.zeros(rim.shape, jnp.bfloat16)

    taps = taps_ref.shape[0]
    chunk = 64
    for slab in range(conv.shape[1] // 128):
        cols = slice(slab * 128, (slab + 1) * 128)
        wide[slab, :edge, :] = rim[:, cols].astype(jnp.float32)
        wide[slab, edge:, :] = gated[:, cols].astype(jnp.float32)
        coeff = taps_ref[:, cols]

        def band_step(step, carry, slab=slab, cols=cols, coeff=coeff):
            base = step * chunk
            total = jnp.zeros((chunk, 128), jnp.float32)
            for tap in range(taps):
                total = total + coeff[tap : tap + 1, :] * wide[
                    slab, pl.ds(base + (edge - taps + 1 + tap), chunk), :
                ]
            conv[pl.ds(pl.multiple_of(base, chunk), chunk), cols] = total
            return carry

        lax.fori_loop(0, rows // chunk, band_step, 0)

    values = conv[...]
    for slot, total in enumerate((values, values * values)):
        sq_mine[:, slot * 128 : (slot + 1) * 128] = jnp.broadcast_to(
            jnp.sum(total, axis=1, keepdims=True), (rows, 128)
        )
    sums = push(sq_mine, sq_other, sq_send, sq_recv, other)
    sums.start()
    hand_over(0)
    sums.wait()
    moments = (sq_mine[...] + sq_other[...]) / CONV_CH
    mean_val = moments[:, :1]
    spread_val = moments[:, 128:129] - mean_val * mean_val
    normed = (values - mean_val) * lax.rsqrt(spread_val + norm_eps)
    swished = jax.nn.silu(normed * ln_gain_ref[...] + ln_bias_ref[...])
    conv[...] = swished
    end_mine[0] = jnp.broadcast_to(
        jnp.sum(swished * swished, axis=1, keepdims=True), (rows, 128)
    )
    conv_sum = push(end_mine.at[0], end_other.at[0], csq_send, csq_recv, other)
    conv_sum.start()
    relay(2)

    def gathered(step):
        for d in range(1, PLANE):
            core_copy((layer - step) * PLANE + spot_at(d)).wait_recv()

    span = 2 * rows

    def expand(group):
        for index in range(PLANE // 2):
            blk = group * PLANE + 2 * index
            cols = slice(index * span, (index + 1) * span)
            lat = jnp.concatenate([lat_ref[blk, :rows, :], lat_ref[blk + 1, :rows, :]], axis=0)
            kn[cols, :] = jnp.dot(
                lat, kup[...], preferred_element_type=jnp.float32
            ).astype(jnp.bfloat16)
            values = lax.dot_general(
                vup_t[...], lat, (((1,), (1,)), ((), ())), preferred_element_type=jnp.float32
            ).astype(jnp.bfloat16)
            for pair in range(pairs):
                low = 2 * VALUE_DIM * pair
                vt[pair, :ones_low, cols] = values[low : low + VALUE_DIM]
                vt[pair, ones_high:, cols] = values[low + VALUE_DIM : low + 2 * VALUE_DIM]
            for part_id in range(2):
                pieces = []
                for piece in range(rows // 128):
                    band = rows + piece // across * ROT_DIM
                    lanes = slice(piece % across * 128, piece % across * 128 + 128)
                    pieces.append(lat_ref[blk + part_id, band : band + ROT_DIM, lanes])
                rot = jnp.concatenate(pieces, axis=1).astype(jnp.float32)
                rot = jnp.concatenate(
                    [rot, jnp.zeros((128 - ROT_DIM, rows), jnp.float32)], axis=0
                )
                low = index * span + part_id * rows
                kr[low : low + rows, :] = rot.T.astype(jnp.bfloat16)

    strip = 256
    strips = keys_wide // strip
    tiles = both // 256
    tile_rows = tuple(
        (
            0 if 256 * tile < rows else ones_low,
            ones_high if 256 * (tile + 1) <= rows else vt.shape[1],
        )
        for tile in range(tiles)
    )

    def attend(first, hidden, middle):
        def score(pair, index):
            cut = slice(index * strip, (index + 1) * strip)
            keys = jnp.concatenate([kn[cut, 128 * pair : 128 * pair + 128], kr[cut, :]], axis=1)
            scores = jnp.dot(keys, q2[pair], preferred_element_type=jnp.float32)
            if hidden is not None:
                scores = jnp.where(hidden(index), far_below, scores)
            s_ref[pair % 2, cut, :] = scores
            return jnp.max(scores, axis=0, keepdims=True)

        tops = [score(0, index) for index in range(strips)]
        for pair in range(pairs):
            if pair == pairs // 2:
                middle()
            top = tops[0]
            for value in tops[1:]:
                top = jnp.maximum(top, value)
            if not first:
                old = run_max[pair : pair + 1, :]
                top = jnp.maximum(old, top)
                fade = jnp.exp2(old - top)
            run_max[pair : pair + 1, :] = top
            tops = []
            sums = [None] * tiles
            for index in range(strips):
                cut = slice(index * strip, (index + 1) * strip)
                if pair + 1 < pairs:
                    tops.append(score(pair + 1, index))
                weights = jnp.exp2(s_ref[pair % 2, cut, :] - top).astype(jnp.bfloat16)
                for tile, (low, high) in enumerate(tile_rows):
                    new = jnp.dot(
                        vt[pair, low:high, cut],
                        weights[:, 256 * tile : 256 * (tile + 1)],
                        preferred_element_type=jnp.float32,
                    )
                    sums[tile] = new if sums[tile] is None else sums[tile] + new
            for tile, (low, high) in enumerate(tile_rows):
                new = sums[tile]
                if not first:
                    new = new + acc[pair, tile, : high - low, :] * fade[
                        :, 256 * tile : 256 * (tile + 1)
                    ]
                acc[pair, tile, : high - low, :] = new

    def hidden(index):
        key = layer * keys_wide + index * strip + lax.broadcasted_iota(
            jnp.int32, (strip, both), 0
        )
        query = lax.broadcasted_iota(jnp.int32, (strip, both), 1)
        return key > me * rows + jnp.where(query >= rows, query - rows, query)

    loads[6].wait()
    gathered(0)
    expand(layer)

    def first_middle():
        hand_over(1)

    attend(True, hidden, first_middle)

    def far(step, carry):
        for d in range(PLANE):
            core_copy((layer - step) * PLANE + spot_at(d)).wait_recv()
        expand(layer - step)

        def middle():
            hand_over(step + 1)
            relay(step + 2)

        attend(False, None, middle)
        return carry

    lax.fori_loop(1, layer + 1, far, 0)

    for pair in range(pairs):
        for side in range(2):
            pieces = []
            for tile, (low, high) in enumerate(tile_rows):
                start = max(side * rows, 256 * tile)
                stop = min((side + 1) * rows, 256 * (tile + 1))
                if start >= stop:
                    continue
                total = acc[pair, tile, : high - low, start - 256 * tile : stop - 256 * tile]
                base = 0 if side == 0 else ones_high - low
                pieces.append(
                    total[base : base + VALUE_DIM] / total[ones_low - low : ones_low - low + 1]
                )
            low = (2 * pair + side) * VALUE_DIM
            att_t[low : low + VALUE_DIM, :] = jnp.concatenate(pieces, axis=1)
    attended = att_t[...].T.astype(jnp.bfloat16).astype(jnp.float32)
    end_mine[1] = jnp.broadcast_to(
        jnp.sum(attended * attended, axis=1, keepdims=True), (rows, 128)
    )
    att_sum = push(end_mine.at[1], end_other.at[1], asq_send, asq_recv, other)
    att_sum.start()
    conv_sum.wait()
    conv_scale = lax.rsqrt((end_mine[0] + end_other[0])[:, :1] / CONV_CH + norm_eps)
    conv_mixed = (conv[...] * conv_scale * conv_gain_ref[...]).astype(jnp.bfloat16)
    att_mixed = (attended * att_gain_ref[...]).astype(jnp.bfloat16)
    loads[8].wait()
    loads[9].wait()
    pieces = part.shape[0]
    piece = part.shape[2]

    def products(owner, index):
        cols = pl.ds(pl.multiple_of(owner * width + index * piece, 128), piece)
        return (
            jnp.dot(att_mixed, att_w[:, cols], preferred_element_type=jnp.float32),
            jnp.dot(conv_mixed, conv_w[:, cols], preferred_element_type=jnp.float32),
        )

    waiting = [products(1 - mine, index) for index in range(pieces)]
    att_sum.wait()
    att_scale = lax.rsqrt((end_mine[1] + end_other[1])[:, :1] / ATT_WIDTH + norm_eps)
    copies = []
    for index, (from_att, from_conv) in enumerate(waiting):
        part[index] = (from_att * att_scale + from_conv).astype(jnp.bfloat16)
        copy = push(
            part.at[index], arrived.at[index], part_send.at[index], part_recv.at[index], other
        )
        copy.start()
        copies.append(copy)
    for index in range(pieces):
        from_att, from_conv = products(mine, index)
        own = (from_att * att_scale + from_conv).astype(jnp.bfloat16).astype(jnp.float32)
        copies[index].wait()
        out_ref[:, index * piece : (index + 1) * piece] = (
            own + arrived[index].astype(jnp.float32)
        ).astype(jnp.bfloat16)

    @pl.when(me < seats - 1)
    def _():
        rim_copy.wait_send()

    for d in range(1, layers):

        @pl.when(layer + d < layers)
        def _(d=d):
            column_copy(d).wait_send()

    def settle(step, carry):
        base = (layer - step) * PLANE
        for d in range(1, PLANE):
            plane_copy(base + spot, d).wait_send()
            core_copy(base + spot_at(d)).wait_send()

        @pl.when(step > 0)
        def _():
            core_copy(base + spot).wait_send()

        return carry

    lax.fori_loop(0, layer + 1, settle, 0)


def angle_tables(seats, rows):
    frequency = rope_base ** (-np.arange(ROT_DIM // 2) / (ROT_DIM // 2))

    def table(positions):
        angles = frequency[:, None] * positions[None, :]
        return jnp.asarray(
            np.concatenate([np.cos(angles), np.sin(angles)], axis=0), jnp.float32
        )

    return table(np.arange(rows)), table(rows * np.arange(-(-seats // 128) * 128))


def fused(tokens, gains, matrices, taps, seats):
    rows, width = tokens.shape
    chans = taps.shape[1]
    rank = matrices[0].shape[1]
    heads = matrices[4].shape[1] // NOPE_DIM
    pairs = heads // 2
    keys_wide = PLANE * rows
    layers = seats // PLANE
    across = rank // 128
    height = rows + -(-(rows // 128) // across) * ROT_DIM
    vmem = pl.BlockSpec(memory_space=pltpu.VMEM)
    anywhere = pl.BlockSpec(memory_space=pltpu.HBM)
    dma = pltpu.SemaphoreType.DMA
    edge = 32
    pieces = 4
    bf16 = jnp.bfloat16
    f32 = jnp.float32
    value_rows = 2 * VALUE_DIM + 16
    base, seat = angle_tables(seats, rows)
    input_gain, kv_gain, ln_gain, ln_bias, att_gain, conv_gain = gains
    return pl.pallas_call(
        layer_kernel,
        out_shape=jax.ShapeDtypeStruct((rows, width), bf16),
        in_specs=[anywhere] + [vmem] * 9 + [anywhere] * 10,
        out_specs=vmem,
        scratch_shapes=[pltpu.VMEM(matrix.shape, bf16) for matrix in matrices]
        + [
            pltpu.VMEM(matrices[7].shape[::-1], bf16),
            pltpu.VMEM((rows, width), bf16),
            pltpu.VMEM((rows, width), bf16),
            pltpu.VMEM((rows, 2 * width), bf16),
            pltpu.VMEM((rows, 128), f32),
            pltpu.VMEM((rows, chans), bf16),
            pltpu.VMEM((edge, chans), bf16),
            pltpu.VMEM((chans // 128, rows + edge, 128), f32),
            pltpu.VMEM((rows, chans), f32),
            pltpu.VMEM((rows, 256), f32),
            pltpu.VMEM((rows, 256), f32),
            pltpu.VMEM((seats, height, rank), bf16),
            pltpu.VMEM((pairs, 256, 2 * rows), bf16),
            pltpu.VMEM((keys_wide, heads * NOPE_DIM), bf16),
            pltpu.VMEM((keys_wide, 128), bf16),
            pltpu.VMEM((pairs, value_rows, keys_wide), bf16),
            pltpu.VMEM((max(pairs, 8), 2 * rows), f32),
            pltpu.VMEM((pairs, 2 * rows // 256, value_rows, 256), f32),
            pltpu.VMEM((2, keys_wide, 2 * rows), f32),
            pltpu.VMEM((heads * VALUE_DIM, rows), f32),
            pltpu.VMEM((2, rows, 128), f32),
            pltpu.VMEM((2, rows, 128), f32),
            pltpu.VMEM((pieces, rows, width // pieces), bf16),
            pltpu.VMEM((pieces, rows, width // pieces), bf16),
            dma((len(matrices),)),
        ]
        + [dma] * 11
        + [
            dma((pieces,)),
            dma((pieces,)),
            dma((max(layers - 1, 1),)),
            dma((layers, PLANE - 1)),
            dma((seats,)),
            dma((seats,)),
            dma((seats,)),
        ],
        compiler_params=pltpu.CompilerParams(
            vmem_limit_bytes=60 << 20, collective_id=0, has_side_effects=True
        ),
        name="layer",
    )(tokens, input_gain, kv_gain, base, seat, taps, ln_gain, ln_bias, att_gain, conv_gain, *matrices)


def gathered_kernel(q_ref, lat_ref, kup_ref, vup_ref, o_ref, kt, vt, run_max, acc):
    heads, rows, lanes = q_ref.shape
    blocks = lat_ref.shape[0]
    rank = kup_ref.shape[1]
    nope = kup_ref.shape[0] // heads
    vdim = vup_ref.shape[0] // heads
    rot = lat_ref.shape[1] - rank
    wide = kt.shape[2]
    group = wide // rows
    me = lax.axis_index("sp")
    last = me // group
    kt[:, nope + rot :, :] = jnp.zeros((heads, lanes - nope - rot, wide), jnp.bfloat16)
    vt[:, vdim:, :] = jnp.ones((heads, lanes - vdim, wide), jnp.bfloat16)

    def expand(block):
        for part in range(group):
            src = jnp.minimum(block * group + part, blocks - 1)
            lat = lat_ref[src, :rank, :]
            turned = lat_ref[src, rank:, :]
            cols = slice(part * rows, (part + 1) * rows)
            keys = jnp.dot(kup_ref[...], lat, preferred_element_type=jnp.float32)
            values = jnp.dot(vup_ref[...], lat, preferred_element_type=jnp.float32)
            for head in range(heads):
                kt[head, :nope, cols] = keys[head * nope : (head + 1) * nope].astype(jnp.bfloat16)
                kt[head, nope : nope + rot, cols] = turned
                vt[head, :vdim, cols] = values[head * vdim : (head + 1) * vdim].astype(
                    jnp.bfloat16
                )

    def weigh(head, scores, top):
        weights = jnp.exp2(scores - top).astype(jnp.bfloat16)
        return lax.dot_general(
            weights, vt[head], (((1,), (1,)), ((), ())), preferred_element_type=jnp.float32
        )

    expand(last)
    key_pos = last * wide + lax.broadcasted_iota(jnp.int32, (rows, wide), 1)
    query_pos = me * rows + lax.broadcasted_iota(jnp.int32, (rows, wide), 0)
    hidden = key_pos > query_pos
    for head in range(heads):
        scores = jnp.dot(q_ref[head], kt[head], preferred_element_type=jnp.float32)
        scores = jnp.where(hidden, far_below, scores)
        top = jnp.max(scores, axis=1, keepdims=True)
        run_max[head] = jnp.broadcast_to(top, (rows, lanes))
        acc[head] = weigh(head, scores, top)

    def visit(step, carry):
        expand(step)
        for head in range(heads):
            scores = jnp.dot(q_ref[head], kt[head], preferred_element_type=jnp.float32)
            old = run_max[head]
            top = jnp.maximum(old[:, :1], jnp.max(scores, axis=1, keepdims=True))
            wide_top = jnp.broadcast_to(top, (rows, lanes))
            run_max[head] = wide_top
            acc[head] = acc[head] * jnp.exp2(old - wide_top) + weigh(head, scores, top)
        return carry

    lax.fori_loop(0, last, visit, 0)
    lane = lax.broadcasted_iota(jnp.int32, (rows, lanes), 1)
    for pair in range(heads // 2):
        halves = []
        for head in (2 * pair, 2 * pair + 1):
            total = acc[head]
            halves.append(total / pltpu.roll(total, vdim, axis=1))
        both = jnp.where(lane < vdim, halves[0], pltpu.roll(halves[1], vdim, axis=1))
        o_ref[:, pair * lanes : (pair + 1) * lanes] = both.astype(jnp.bfloat16)


def gathered_attention(q_heads, lat_all, key_up_t, value_up_t):
    heads, rows, lanes = q_heads.shape
    blocks = lat_all.shape[0]
    wide = 2 * rows if blocks % 2 == 0 else rows
    vmem = pl.BlockSpec(memory_space=pltpu.VMEM)
    return pl.pallas_call(
        gathered_kernel,
        out_shape=jax.ShapeDtypeStruct((rows, value_up_t.shape[0]), jnp.bfloat16),
        in_specs=[vmem] * 4,
        out_specs=vmem,
        scratch_shapes=[
            pltpu.VMEM((heads, lanes, wide), jnp.bfloat16),
            pltpu.VMEM((heads, lanes, wide), jnp.bfloat16),
            pltpu.VMEM((heads, rows, lanes), jnp.float32),
            pltpu.VMEM((heads, rows, lanes), jnp.float32),
        ],
        compiler_params=pltpu.CompilerParams(vmem_limit_bytes=48 << 20),
        cost_estimate=pl.CostEstimate(
            flops=20_000_000_000, bytes_accessed=8 << 20, transcendentals=20_000_000
        ),
        name="gathered_attention",
    )(q_heads, lat_all, key_up_t, value_up_t)


def conv_kernel(gated_ref, rim_ref, taps_ref, out_ref, wide):
    rows, chans = gated_ref.shape
    rim = rim_ref.shape[0]
    taps = taps_ref.shape[0]
    chunk = 64
    for part in range(chans // 128):
        cols = slice(part * 128, (part + 1) * 128)
        wide[part, :rim, :] = rim_ref[:, cols].astype(jnp.float32)
        wide[part, rim:, :] = gated_ref[:, cols].astype(jnp.float32)
        coeff = taps_ref[:, cols]

        def band(step, carry):
            base = step * chunk
            total = jnp.zeros((chunk, 128), jnp.float32)
            for tap in range(taps):
                total = total + coeff[tap : tap + 1, :] * wide[
                    part, pl.ds(base + (rim - taps + 1 + tap), chunk), :
                ]
            out_ref[pl.ds(pl.multiple_of(base, chunk), chunk), cols] = total
            return carry

        lax.fori_loop(0, rows // chunk, band, 0)


def convolve(gated, rim, taps):
    rows, chans = gated.shape
    vmem = pl.BlockSpec(memory_space=pltpu.VMEM)
    return pl.pallas_call(
        conv_kernel,
        out_shape=jax.ShapeDtypeStruct((rows, chans), jnp.float32),
        in_specs=[vmem] * 3,
        out_specs=vmem,
        scratch_shapes=[pltpu.VMEM((chans // 128, rows + rim.shape[0], 128), jnp.float32)],
        cost_estimate=pl.CostEstimate(
            flops=2 * rows * chans * 31, bytes_accessed=2 << 20, transcendentals=0
        ),
        name="depthwise",
    )(gated, rim, taps)


def shards(
    tokens,
    input_gain,
    query_weight,
    query_rot_weight,
    kv_down,
    rot_down,
    kv_gain,
    key_up,
    value_up,
    conv_value_weight,
    conv_gate_weight,
    conv_taps,
    conv_ln_gain,
    conv_ln_bias,
    att_out_gain,
    conv_out_gain,
    att_out_weight,
    conv_out_weight,
):
    tok_rows = tokens.shape[0]
    heads_here = key_up.shape[1] // NOPE_DIM
    chan_here = conv_taps.shape[1]
    weight_list = (
        query_weight,
        query_rot_weight,
        kv_down,
        rot_down,
        conv_value_weight,
        conv_gate_weight,
    )
    seats = lax.axis_size("sp")
    if (
        lax.axis_size("tp") == 2
        and seats % PLANE == 0
        and tok_rows % 128 == 0
        and heads_here % 2 == 0
    ):
        gains = (
            input_gain, kv_gain, conv_ln_gain, conv_ln_bias, att_out_gain, conv_out_gain
        )
        return fused(
            tokens,
            tuple(gain[None, :] for gain in gains),
            (
                kv_down, rot_down.T, conv_gate_weight, conv_value_weight, query_weight,
                query_rot_weight, key_up, value_up, att_out_weight, conv_out_weight,
            ),
            conv_taps,
            seats,
        )
    whole_rows = lax.all_gather(tokens, "tp", axis=1, tiled=True).astype(jnp.float32)
    scaled = (whole_rows * input_gain[None, :]).astype(jnp.bfloat16)
    row_scale = lax.rsqrt(jnp.mean(whole_rows * whole_rows, axis=1, keepdims=True) + norm_eps)

    def add_product(weight):
        return jnp.dot(scaled, weight, preferred_element_type=jnp.float32)

    summed = tuple((add_product(weight) for weight in weight_list))
    q_acc, qrot_acc, latent_raw, rot_acc, value_acc, gate_acc = summed
    positions = lax.axis_index("sp") * tok_rows + jnp.arange(tok_rows, dtype=jnp.int32)
    cos_table, sine_table = rotary_tables(positions, ROT_DIM // 2)
    fold = math.log2(math.e) / math.sqrt(NOPE_DIM + ROT_DIM)
    query_scale = row_scale * fold
    plain_q = (q_acc * query_scale).reshape(tok_rows, heads_here, NOPE_DIM)
    turned_q = rotate_half(
        (qrot_acc * query_scale).reshape(tok_rows, heads_here, ROT_DIM),
        cos_table[:, None, :],
        sine_table[:, None, :],
    )
    blank = jnp.zeros((tok_rows, heads_here, 128 - NOPE_DIM - ROT_DIM), jnp.float32)
    q_heads = jnp.transpose(
        jnp.concatenate([plain_q, turned_q, blank], axis=2).astype(jnp.bfloat16), (1, 0, 2)
    )
    latent = (
        latent_raw
        * lax.rsqrt(jnp.mean(latent_raw * latent_raw, axis=1, keepdims=True) + norm_eps)
        * kv_gain[None, :]
    ).astype(jnp.bfloat16)
    key_rot = rotate_half(rot_acc * row_scale, cos_table, sine_table).astype(jnp.bfloat16)
    gated_input = (value_acc * row_scale * jax.nn.sigmoid(gate_acc * row_scale)).astype(
        jnp.bfloat16
    )
    packed = jnp.concatenate([latent.T, key_rot.T], axis=0)
    rim_rows = shifted(gated_input[tok_rows - (KERNEL + 1) :], "sp", 1)
    conv_out = convolve(gated_input, rim_rows, conv_taps)
    moment_one, moment_two = lax.psum(
        (jnp.sum(conv_out, axis=1), jnp.sum(conv_out * conv_out, axis=1)), "tp"
    )
    mean_val = moment_one / CONV_CH
    spread = moment_two / CONV_CH - mean_val * mean_val
    normed = (conv_out - mean_val[:, None]) * lax.rsqrt(spread + norm_eps)[:, None]
    swished = jax.nn.silu(normed * conv_ln_gain[None, :] + conv_ln_bias[None, :])
    lat_all = lax.all_gather(packed, "sp", axis=0)
    attended = gathered_attention(q_heads, lat_all, key_up.T, value_up.T).astype(jnp.float32)
    att_sq, conv_sq = lax.psum(
        (
            jnp.sum(attended * attended, axis=1, keepdims=True),
            jnp.sum(swished * swished, axis=1, keepdims=True),
        ),
        "tp",
    )
    att_mixed = (
        attended * lax.rsqrt(att_sq / ATT_WIDTH + norm_eps) * att_out_gain[None, :]
    ).astype(jnp.bfloat16)
    conv_mixed = (
        swished * lax.rsqrt(conv_sq / CONV_CH + norm_eps) * conv_out_gain[None, :]
    ).astype(jnp.bfloat16)
    share = (
        jnp.dot(att_mixed, att_out_weight, preferred_element_type=jnp.float32)
        + jnp.dot(conv_mixed, conv_out_weight, preferred_element_type=jnp.float32)
    ).astype(jnp.bfloat16)
    return lax.psum_scatter(share, "tp", scatter_dimension=1, tiled=True)


def solution(mesh):
    return jax.shard_map(
        shards,
        mesh=mesh,
        in_specs=(
            P("sp", "tp"),
            P(),
            P(None, "tp"),
            P(None, "tp"),
            P(),
            P(),
            P(),
            P(None, "tp"),
            P(None, "tp"),
            P(None, "tp"),
            P(None, "tp"),
            P(None, "tp"),
            P("tp"),
            P("tp"),
            P("tp"),
            P("tp"),
            P("tp", None),
            P("tp", None),
        ),
        out_specs=P("sp", "tp"),
        check_vma=False,
    )
```

```python
import math

import jax
import jax.numpy as jnp
import numpy as np
from jax import lax
from jax.experimental import pallas as pl
from jax.experimental.pallas import tpu as pltpu
from jax.sharding import PartitionSpec as P

D_MODEL = 2048
NOPE_DIM = 64
ROT_DIM = 32
VALUE_DIM = 64
CONV_CH = 1024
KERNEL = 31
ATT_WIDTH = 1024


norm_eps = 1e-06
far_below = -1e30
rope_base = 10000.0


def shifted(block, axis, distance):
    devices = range(lax.axis_size(axis))
    route = [(i - distance, i) for i in devices if i - distance in devices]
    return lax.ppermute(block, axis, route)


def rotary_tables(positions, half_dim):
    frequency = rope_base ** (-jnp.arange(half_dim, dtype=jnp.float32) / half_dim)
    angles = positions.astype(jnp.float32)[:, None] * frequency[None, :]
    return (jnp.cos(angles), jnp.sin(angles))


def rotate_half(values, cos_table, sine_table):
    half_dim = cos_table.shape[-1]
    front_half = values[..., :half_dim]
    back_half = values[..., half_dim:]
    return jnp.concatenate(
        [
            front_half * cos_table - back_half * sine_table,
            back_half * cos_table + front_half * sine_table,
        ],
        axis=-1,
    )


MESH = pl.DeviceIdType.MESH


def push(src, dst, send, recv, target):
    return pltpu.make_async_remote_copy(
        src_ref=src,
        dst_ref=dst,
        send_sem=send,
        recv_sem=recv,
        device_id=target,
        device_id_type=MESH,
    )


def other_core():
    return {"sp": lax.axis_index("sp"), "tp": 1 - lax.axis_index("tp")}


PLANE = 4


def layer_kernel(
    tok_hbm, gain_ref, kv_gain_ref, base_ref, seat_ref, taps_ref, ln_gain_ref, ln_bias_ref,
    att_gain_ref, conv_gain_ref,
    kvd_hbm, rotw_hbm, cgw_hbm, cvw_hbm, qw_hbm, qrw_hbm, kup_hbm, vup_hbm, att_hbm, conv_hbm,
    out_ref,
    kvd, rotw, cgw, cvw, qw, qrw, kup, vup, att_w, conv_w, vup_t,
    tok, landed, scaled, narrow, gated, rim, wide, conv, sq_mine, sq_other,
    lat_ref, q2, kn, kr, vt, run_max, acc, s_ref, att_t, end_mine, end_other,
    att_sq, att_sq_other, att_act, conv_act,
    w_sem, w_send, w_recv, tok_load, tok_send, tok_recv, rim_send, rim_recv, sq_send, sq_recv,
    csq_send, csq_recv, asq_send, asq_recv, conv_send, conv_recv, att_send, att_recv,
    col_send, plane_send, core_send, link_recv, core_recv,
):
    mine = lax.axis_index("tp")
    me = lax.axis_index("sp")
    seats = lax.axis_size("sp")
    rows, width = tok.shape
    blocks = lat_ref.shape[0]
    rank = kvd.shape[1]
    layers = blocks // PLANE
    layer = me // PLANE
    spot = me % PLANE
    height = lat_ref.shape[1] // 2
    half = pl.ds(pl.multiple_of(mine * height, 16), height)
    other = other_core()
    ahead = {"sp": (me + 1) % seats, "tp": mine}
    behind = {"sp": (me + seats - 1) % seats, "tp": mine}

    def columns(owner):
        return pl.ds(pl.multiple_of(owner * width, 128), width)

    loads = [
        pltpu.make_async_copy(src, dst, w_sem.at[index])
        for index, (src, dst) in enumerate(
            (
                (kvd_hbm, kvd), (rotw_hbm, rotw), (cgw_hbm, cgw), (cvw_hbm, cvw),
                (qw_hbm, qw), (qrw_hbm, qrw), (kup_hbm, kup), (vup_hbm, vup),
                (att_hbm.at[:, columns(mine)], att_w.at[0]),
                (conv_hbm.at[:, columns(mine)], conv_w.at[0]),
            )
        )
    ]
    fetch = pltpu.make_async_copy(tok_hbm, tok, tok_load)
    fetch.start()
    for load in loads[:2]:
        load.start()
    gifts = [
        push(src.at[:, columns(1 - mine)], dst.at[1], w_send.at[index], w_recv.at[index], other)
        for index, (src, dst) in enumerate(((att_hbm, att_w), (conv_hbm, conv_w)))
    ]

    def spot_at(distance):
        return (spot + distance) % PLANE

    def at(layer_id, spot_id):
        return {"sp": layer_id * PLANE + spot_id, "tp": mine}

    barrier = pltpu.get_barrier_semaphore()
    peers = [at(layer, spot_at(d)) for d in range(1, PLANE)] + [other]
    for peer in peers:
        pl.semaphore_signal(barrier, inc=1, device_id=peer, device_id_type=MESH)
    above = at(jnp.minimum(layer + 1, layers - 1), spot)
    below = at(jnp.maximum(layer - 1, 0), spot)
    for condition, peer in (
        (layer < layers - 1, above), (layer > 0, below), (me < seats - 1, ahead), (me > 0, behind),
    ):

        @pl.when(condition)
        def _(peer=peer):
            pl.semaphore_signal(barrier, inc=1, device_id=peer, device_id_type=MESH)

    q2[...] = jnp.zeros(q2.shape, jnp.bfloat16)
    pairs, _, both = q2.shape
    keys_wide = kn.shape[0]
    ones_low = VALUE_DIM
    ones_high = vt.shape[1] - VALUE_DIM
    vt[:, ones_low:ones_high, :] = jnp.ones((pairs, ones_high - ones_low, keys_wide), jnp.bfloat16)
    pl.semaphore_wait(
        barrier,
        len(peers)
        + jnp.minimum(me, 1)
        + jnp.minimum(seats - 1 - me, 1)
        + jnp.minimum(layer, 1)
        + jnp.minimum(layers - 1 - layer, 1),
    )
    fetch.wait()
    tok_copy = push(tok, landed, tok_send, tok_recv, other)
    tok_copy.start()
    for load in loads[2:]:
        load.start()

    def place(block, index):
        cols = pl.ds(pl.multiple_of(index * width, 128), width)
        full = block[...].astype(jnp.float32)
        scaled[:, cols] = (full * gain_ref[:, cols]).astype(jnp.bfloat16)
        return jnp.sum(full * full, axis=1, keepdims=True)

    squares = place(tok, mine)
    column = lax.broadcasted_iota(jnp.int32, seat_ref.shape, 1)
    seat_turn = jnp.sum(
        jnp.where(column == me, seat_ref[...], 0.0), axis=1, keepdims=True
    )
    turn = ROT_DIM // 2
    seat_cos, seat_sin = seat_turn[:turn], seat_turn[turn:]
    base_cos, base_sin = base_ref[:turn], base_ref[turn:]
    cos_table = seat_cos * base_cos - seat_sin * base_sin
    sin_table = seat_sin * base_cos + seat_cos * base_sin

    def rotate(block):
        front = block[:turn]
        back = block[turn : 2 * turn]
        return jnp.concatenate(
            [front * cos_table - back * sin_table, back * cos_table + front * sin_table], axis=0
        )

    tok_copy.wait()
    squares = squares + place(landed, 1 - mine)
    row_scale = lax.rsqrt(squares / (2 * width) + norm_eps)

    def project(weight):
        return jnp.dot(scaled[...], weight[...], preferred_element_type=jnp.float32)

    loads[0].wait()
    loads[1].wait()
    raw = project(kvd)
    latent = (
        raw
        * lax.rsqrt(jnp.mean(raw * raw, axis=1, keepdims=True) + norm_eps)
        * kv_gain_ref[...]
    )
    lat_ref[me, :rows, :] = latent.astype(jnp.bfloat16)
    narrow[...] = jnp.broadcast_to(row_scale, narrow.shape)
    key_turn = lax.dot_general(
        rotw[...], scaled[...], (((1,), (1,)), ((), ())), preferred_element_type=jnp.float32
    )
    key_rot = rotate(key_turn * narrow[...].T[:ROT_DIM]).astype(jnp.bfloat16)
    across = rank // 128
    for piece in range(across * ((rows // 128 + across - 1) // across)):
        band = rows + piece // across * ROT_DIM
        lanes = slice(piece % across * 128, piece % across * 128 + 128)
        lat_ref[me, band : band + ROT_DIM, lanes] = (
            key_rot[:, piece * 128 : piece * 128 + 128]
            if piece < rows // 128
            else jnp.zeros((ROT_DIM, 128), jnp.bfloat16)
        )

    def column_copy(block):
        spread = lat_ref.at[block, half]
        return push(spread, spread, col_send.at[block // PLANE], link_recv.at[block], above)

    def rise(block):
        @pl.when(layer + 1 < layers)
        def _():
            column_copy(block).start()

    def plane_copy(block, distance):
        return push(
            lat_ref.at[block, half],
            lat_ref.at[block, half],
            plane_send.at[block // PLANE, distance - 1],
            link_recv.at[block],
            at(layer, spot_at(distance)),
        )

    def core_copy(block):
        spread = lat_ref.at[block, half]
        return push(spread, spread, core_send.at[block], core_recv.at[block], other)

    rise(me)
    for d in range(1, PLANE):
        plane_copy(me, d).start()
    for gift in gifts:
        gift.start()

    def arrive(block):
        spread = lat_ref.at[block, half]
        push(spread, spread, core_send.at[block], link_recv.at[block], other).wait_recv()

    def relay(step):
        @pl.when(step <= layer)
        def _():
            block = (layer - step) * PLANE + spot
            arrive(block)
            rise(block)
            for d in range(1, PLANE):
                plane_copy(block, d).start()
            core_copy(block).start()

    def hand_over(step):
        @pl.when(step <= layer)
        def _():
            for d in range(1, PLANE):
                block = (layer - step) * PLANE + spot_at(d)
                arrive(block)
                core_copy(block).start()

    loads[2].wait()
    loads[3].wait()
    gate = project(cgw) * row_scale
    gated[...] = (project(cvw) * row_scale * jax.nn.sigmoid(gate)).astype(jnp.bfloat16)
    edge = rim.shape[0]
    rim_copy = push(gated.at[pl.ds(rows - edge, edge)], rim, rim_send, rim_recv, ahead)

    @pl.when(me < seats - 1)
    def _():
        rim_copy.start()

    loads[4].wait()
    loads[5].wait()
    query_scale = row_scale * (math.log2(math.e) / math.sqrt(NOPE_DIM + ROT_DIM))
    plain = (project(qw) * query_scale).T.astype(jnp.bfloat16)
    turned = (project(qrw) * query_scale).T
    for head in range(2 * pairs):
        side = head % 2
        cols = slice(side * rows, (side + 1) * rows)
        q2[head // 2, side * NOPE_DIM : (side + 1) * NOPE_DIM, cols] = plain[
            head * NOPE_DIM : (head + 1) * NOPE_DIM
        ]
        q2[head // 2, 2 * NOPE_DIM : 2 * NOPE_DIM + ROT_DIM, cols] = rotate(
            turned[head * ROT_DIM : (head + 1) * ROT_DIM]
        ).astype(jnp.bfloat16)

    loads[7].wait()
    vup_t[...] = vup[...].astype(jnp.float32).T.astype(jnp.bfloat16)

    @pl.when(me > 0)
    def _():
        rim_copy.wait_recv()

    @pl.when(me == 0)
    def _():
        rim[...] = jnp.zeros(rim.shape, jnp.bfloat16)

    taps = taps_ref.shape[0]
    chunk = 64
    for slab in range(conv.shape[1] // 128):
        cols = slice(slab * 128, (slab + 1) * 128)
        wide[slab, :edge, :] = rim[:, cols].astype(jnp.float32)
        wide[slab, edge:, :] = gated[:, cols].astype(jnp.float32)
        coeff = taps_ref[:, cols]

        def band_step(step, carry, slab=slab, cols=cols, coeff=coeff):
            base = step * chunk
            total = jnp.zeros((chunk, 128), jnp.float32)
            for tap in range(taps):
                total = total + coeff[tap : tap + 1, :] * wide[
                    slab, pl.ds(base + (edge - taps + 1 + tap), chunk), :
                ]
            conv[pl.ds(pl.multiple_of(base, chunk), chunk), cols] = total
            return carry

        lax.fori_loop(0, rows // chunk, band_step, 0)
        if slab == 1:
            relay(1)

    values = conv[...]
    for slot, total in enumerate((values, values * values)):
        sq_mine[:, slot * 128 : (slot + 1) * 128] = jnp.broadcast_to(
            jnp.sum(total, axis=1, keepdims=True), (rows, 128)
        )
    sums = push(sq_mine, sq_other, sq_send, sq_recv, other)
    sums.start()
    hand_over(0)

    def activate():
        sums.wait()
        values = conv[...]
        moments = (sq_mine[...] + sq_other[...]) / CONV_CH
        mean_val = moments[:, :1]
        spread_val = moments[:, 128:129] - mean_val * mean_val
        normed = (values - mean_val) * lax.rsqrt(spread_val + norm_eps)
        swished = jax.nn.silu(normed * ln_gain_ref[...] + ln_bias_ref[...])
        conv_act[0] = (swished * conv_gain_ref[...]).astype(jnp.bfloat16)
        end_mine[...] = jnp.broadcast_to(
            jnp.sum(swished * swished, axis=1, keepdims=True), (rows, 128)
        )
        conv_sum.start()
        conv_copy.start()

    conv_sum = push(end_mine, end_other, csq_send, csq_recv, other)
    conv_copy = push(conv_act.at[0], conv_act.at[1], conv_send, conv_recv, other)

    def gathered(step):
        for d in range(1, PLANE):
            core_copy((layer - step) * PLANE + spot_at(d)).wait_recv()

    span = 2 * rows

    def expand(group):
        for index in range(PLANE // 2):
            blk = group * PLANE + 2 * index
            cols = slice(index * span, (index + 1) * span)
            lat = jnp.concatenate([lat_ref[blk, :rows, :], lat_ref[blk + 1, :rows, :]], axis=0)
            kn[cols, :] = jnp.dot(
                lat, kup[...], preferred_element_type=jnp.float32
            ).astype(jnp.bfloat16)
            values = lax.dot_general(
                vup_t[...], lat, (((1,), (1,)), ((), ())), preferred_element_type=jnp.float32
            ).astype(jnp.bfloat16)
            for pair in range(pairs):
                low = 2 * VALUE_DIM * pair
                vt[pair, :ones_low, cols] = values[low : low + VALUE_DIM]
                vt[pair, ones_high:, cols] = values[low + VALUE_DIM : low + 2 * VALUE_DIM]
            for part_id in range(2):
                pieces = []
                for piece in range(rows // 128):
                    band = rows + piece // across * ROT_DIM
                    lanes = slice(piece % across * 128, piece % across * 128 + 128)
                    pieces.append(lat_ref[blk + part_id, band : band + ROT_DIM, lanes])
                rot = jnp.concatenate(pieces, axis=1).astype(jnp.float32)
                rot = jnp.concatenate(
                    [rot, jnp.zeros((128 - ROT_DIM, rows), jnp.float32)], axis=0
                )
                low = index * span + part_id * rows
                kr[low : low + rows, :] = rot.T.astype(jnp.bfloat16)

    strip = 256
    strips = keys_wide // strip
    tiles = both // 256
    tile_rows = tuple(
        (
            0 if 256 * tile < rows else ones_low,
            ones_high if 256 * (tile + 1) <= rows else vt.shape[1],
        )
        for tile in range(tiles)
    )

    def attend(first, hidden, middle):
        def score(pair, index):
            cut = slice(index * strip, (index + 1) * strip)
            keys = jnp.concatenate([kn[cut, 128 * pair : 128 * pair + 128], kr[cut, :]], axis=1)
            scores = jnp.dot(keys, q2[pair], preferred_element_type=jnp.float32)
            if hidden is not None:
                scores = jnp.where(hidden(index), far_below, scores)
            s_ref[pair % 2, cut, :] = scores
            return jnp.max(scores, axis=0, keepdims=True)

        tops = [score(0, index) for index in range(strips)]
        for pair in range(pairs):
            middle(pair)
            top = tops[0]
            for value in tops[1:]:
                top = jnp.maximum(top, value)
            if not first:
                old = run_max[pair : pair + 1, :]
                top = jnp.maximum(old, top)
                fade = jnp.exp2(old - top)
            run_max[pair : pair + 1, :] = top
            tops = []
            sums = [None] * tiles
            for index in range(strips):
                cut = slice(index * strip, (index + 1) * strip)
                if pair + 1 < pairs:
                    tops.append(score(pair + 1, index))
                weights = jnp.exp2(s_ref[pair % 2, cut, :] - top).astype(jnp.bfloat16)
                for tile, (low, high) in enumerate(tile_rows):
                    new = jnp.dot(
                        vt[pair, low:high, cut],
                        weights[:, 256 * tile : 256 * (tile + 1)],
                        preferred_element_type=jnp.float32,
                    )
                    sums[tile] = new if sums[tile] is None else sums[tile] + new
            for tile, (low, high) in enumerate(tile_rows):
                new = sums[tile]
                if not first:
                    new = new + acc[pair, tile, : high - low, :] * fade[
                        :, 256 * tile : 256 * (tile + 1)
                    ]
                acc[pair, tile, : high - low, :] = new

    def hidden(index):
        key = layer * keys_wide + index * strip + lax.broadcasted_iota(
            jnp.int32, (strip, both), 0
        )
        query = lax.broadcasted_iota(jnp.int32, (strip, both), 1)
        return key > me * rows + jnp.where(query >= rows, query - rows, query)

    loads[6].wait()
    gathered(0)
    expand(layer)

    def first_middle(pair):
        if pair == 1:
            relay(2)
            activate()
        if pair == pairs - 1:
            hand_over(1)

    attend(True, hidden, first_middle)

    def far(step, carry):
        for d in range(PLANE):
            core_copy((layer - step) * PLANE + spot_at(d)).wait_recv()
        expand(layer - step)

        def middle(pair):
            if pair == 1:
                relay(step + 2)
            if pair == pairs - 1:
                hand_over(step + 1)

        attend(False, None, middle)
        return carry

    lax.fori_loop(1, layer + 1, far, 0)

    for pair in range(pairs):
        for side in range(2):
            pieces = []
            for tile, (low, high) in enumerate(tile_rows):
                start = max(side * rows, 256 * tile)
                stop = min((side + 1) * rows, 256 * (tile + 1))
                if start >= stop:
                    continue
                total = acc[pair, tile, : high - low, start - 256 * tile : stop - 256 * tile]
                base = 0 if side == 0 else ones_high - low
                pieces.append(
                    total[base : base + VALUE_DIM] / total[ones_low - low : ones_low - low + 1]
                )
            low = (2 * pair + side) * VALUE_DIM
            att_t[low : low + VALUE_DIM, :] = (
                jnp.concatenate(pieces, axis=1).astype(jnp.bfloat16).astype(jnp.float32)
            )
    attended = att_t[...]
    att_sq[...] = jnp.broadcast_to(
        jnp.sum(attended * attended, axis=0, keepdims=True), att_sq.shape
    )
    att_act[0] = (attended.T * att_gain_ref[...]).astype(jnp.bfloat16)
    att_sum = push(att_sq, att_sq_other, asq_send, asq_recv, other)
    att_sum.start()
    att_copy = push(att_act.at[0], att_act.at[1], att_send, att_recv, other)
    att_copy.start()
    for index in (8, 9):
        loads[index].wait()
    for gift in gifts:
        gift.wait()
    conv_sum.wait()
    conv_copy.wait()
    conv_scale = lax.rsqrt((end_mine[...] + end_other[...])[:, :1] / CONV_CH + norm_eps)

    def product(activations, weight):
        return jnp.dot(activations, weight, preferred_element_type=jnp.float32)

    base_part = (
        product(conv_act[0], conv_w[0]) + product(conv_act[1], conv_w[1])
    ) * conv_scale
    own_part = product(att_act[0], att_w[0])
    att_sum.wait()
    squares_t = jnp.broadcast_to(att_sq[:1] + att_sq_other[:1], (128, rows)).T
    att_scale = lax.rsqrt(squares_t[:, :1] / ATT_WIDTH + norm_eps)
    att_copy.wait()
    out_ref[...] = (
        (own_part + product(att_act[1], att_w[1])) * att_scale + base_part
    ).astype(jnp.bfloat16)

    @pl.when(me < seats - 1)
    def _():
        rim_copy.wait_send()

    def settle(step, carry):
        base = (layer - step) * PLANE
        for d in range(1, PLANE):
            plane_copy(base + spot, d).wait_send()
            core_copy(base + spot_at(d)).wait_send()

        @pl.when(layer + 1 < layers)
        def _():
            column_copy(base + spot).wait_send()

        @pl.when(step > 0)
        def _():
            core_copy(base + spot).wait_send()

        return carry

    lax.fori_loop(0, layer + 1, settle, 0)


def angle_tables(seats, rows):
    frequency = rope_base ** (-np.arange(ROT_DIM // 2) / (ROT_DIM // 2))

    def table(positions):
        angles = frequency[:, None] * positions[None, :]
        return jnp.asarray(
            np.concatenate([np.cos(angles), np.sin(angles)], axis=0), jnp.float32
        )

    return table(np.arange(rows)), table(rows * np.arange(-(-seats // 128) * 128))


def fused(tokens, gains, matrices, taps, seats):
    rows, width = tokens.shape
    chans = taps.shape[1]
    rank = matrices[0].shape[1]
    heads = matrices[4].shape[1] // NOPE_DIM
    pairs = heads // 2
    keys_wide = PLANE * rows
    layers = seats // PLANE
    across = rank // 128
    height = rows + -(-(rows // 128) // across) * ROT_DIM
    vmem = pl.BlockSpec(memory_space=pltpu.VMEM)
    anywhere = pl.BlockSpec(memory_space=pltpu.HBM)
    dma = pltpu.SemaphoreType.DMA
    edge = 32
    bf16 = jnp.bfloat16
    f32 = jnp.float32
    value_rows = 2 * VALUE_DIM + 16
    base, seat = angle_tables(seats, rows)
    input_gain, kv_gain, ln_gain, ln_bias, att_gain, conv_gain = gains
    return pl.pallas_call(
        layer_kernel,
        out_shape=jax.ShapeDtypeStruct((rows, width), bf16),
        in_specs=[anywhere] + [vmem] * 9 + [anywhere] * 10,
        out_specs=vmem,
        scratch_shapes=[pltpu.VMEM(matrix.shape, bf16) for matrix in matrices[:8]]
        + [
            pltpu.VMEM((2, matrix.shape[0], width), bf16) for matrix in matrices[8:]
        ]
        + [
            pltpu.VMEM(matrices[7].shape[::-1], bf16),
            pltpu.VMEM((rows, width), bf16),
            pltpu.VMEM((rows, width), bf16),
            pltpu.VMEM((rows, 2 * width), bf16),
            pltpu.VMEM((rows, 128), f32),
            pltpu.VMEM((rows, chans), bf16),
            pltpu.VMEM((edge, chans), bf16),
            pltpu.VMEM((chans // 128, rows + edge, 128), f32),
            pltpu.VMEM((rows, chans), f32),
            pltpu.VMEM((rows, 256), f32),
            pltpu.VMEM((rows, 256), f32),
            pltpu.VMEM((seats, height, rank), bf16),
            pltpu.VMEM((pairs, 256, 2 * rows), bf16),
            pltpu.VMEM((keys_wide, heads * NOPE_DIM), bf16),
            pltpu.VMEM((keys_wide, 128), bf16),
            pltpu.VMEM((pairs, value_rows, keys_wide), bf16),
            pltpu.VMEM((max(pairs, 8), 2 * rows), f32),
            pltpu.VMEM((pairs, 2 * rows // 256, value_rows, 256), f32),
            pltpu.VMEM((2, keys_wide, 2 * rows), f32),
            pltpu.VMEM((heads * VALUE_DIM, rows), f32),
            pltpu.VMEM((rows, 128), f32),
            pltpu.VMEM((rows, 128), f32),
            pltpu.VMEM((8, rows), f32),
            pltpu.VMEM((8, rows), f32),
            pltpu.VMEM((2, rows, heads * VALUE_DIM), bf16),
            pltpu.VMEM((2, rows, chans), bf16),
            dma((len(matrices),)),
            dma((2,)),
            dma((2,)),
        ]
        + [dma] * 15
        + [
            dma((layers,)),
            dma((layers, PLANE - 1)),
            dma((seats,)),
            dma((seats,)),
            dma((seats,)),
        ],
        compiler_params=pltpu.CompilerParams(
            vmem_limit_bytes=60 << 20, collective_id=0, has_side_effects=True
        ),
        name="layer",
    )(tokens, input_gain, kv_gain, base, seat, taps, ln_gain, ln_bias, att_gain, conv_gain, *matrices)


def gathered_kernel(q_ref, lat_ref, kup_ref, vup_ref, o_ref, kt, vt, run_max, acc):
    heads, rows, lanes = q_ref.shape
    blocks = lat_ref.shape[0]
    rank = kup_ref.shape[1]
    nope = kup_ref.shape[0] // heads
    vdim = vup_ref.shape[0] // heads
    rot = lat_ref.shape[1] - rank
    wide = kt.shape[2]
    group = wide // rows
    me = lax.axis_index("sp")
    last = me // group
    kt[:, nope + rot :, :] = jnp.zeros((heads, lanes - nope - rot, wide), jnp.bfloat16)
    vt[:, vdim:, :] = jnp.ones((heads, lanes - vdim, wide), jnp.bfloat16)

    def expand(block):
        for part in range(group):
            src = jnp.minimum(block * group + part, blocks - 1)
            lat = lat_ref[src, :rank, :]
            turned = lat_ref[src, rank:, :]
            cols = slice(part * rows, (part + 1) * rows)
            keys = jnp.dot(kup_ref[...], lat, preferred_element_type=jnp.float32)
            values = jnp.dot(vup_ref[...], lat, preferred_element_type=jnp.float32)
            for head in range(heads):
                kt[head, :nope, cols] = keys[head * nope : (head + 1) * nope].astype(jnp.bfloat16)
                kt[head, nope : nope + rot, cols] = turned
                vt[head, :vdim, cols] = values[head * vdim : (head + 1) * vdim].astype(
                    jnp.bfloat16
                )

    def weigh(head, scores, top):
        weights = jnp.exp2(scores - top).astype(jnp.bfloat16)
        return lax.dot_general(
            weights, vt[head], (((1,), (1,)), ((), ())), preferred_element_type=jnp.float32
        )

    expand(last)
    key_pos = last * wide + lax.broadcasted_iota(jnp.int32, (rows, wide), 1)
    query_pos = me * rows + lax.broadcasted_iota(jnp.int32, (rows, wide), 0)
    hidden = key_pos > query_pos
    for head in range(heads):
        scores = jnp.dot(q_ref[head], kt[head], preferred_element_type=jnp.float32)
        scores = jnp.where(hidden, far_below, scores)
        top = jnp.max(scores, axis=1, keepdims=True)
        run_max[head] = jnp.broadcast_to(top, (rows, lanes))
        acc[head] = weigh(head, scores, top)

    def visit(step, carry):
        expand(step)
        for head in range(heads):
            scores = jnp.dot(q_ref[head], kt[head], preferred_element_type=jnp.float32)
            old = run_max[head]
            top = jnp.maximum(old[:, :1], jnp.max(scores, axis=1, keepdims=True))
            wide_top = jnp.broadcast_to(top, (rows, lanes))
            run_max[head] = wide_top
            acc[head] = acc[head] * jnp.exp2(old - wide_top) + weigh(head, scores, top)
        return carry

    lax.fori_loop(0, last, visit, 0)
    lane = lax.broadcasted_iota(jnp.int32, (rows, lanes), 1)
    for pair in range(heads // 2):
        halves = []
        for head in (2 * pair, 2 * pair + 1):
            total = acc[head]
            halves.append(total / pltpu.roll(total, vdim, axis=1))
        both = jnp.where(lane < vdim, halves[0], pltpu.roll(halves[1], vdim, axis=1))
        o_ref[:, pair * lanes : (pair + 1) * lanes] = both.astype(jnp.bfloat16)


def gathered_attention(q_heads, lat_all, key_up_t, value_up_t):
    heads, rows, lanes = q_heads.shape
    blocks = lat_all.shape[0]
    wide = 2 * rows if blocks % 2 == 0 else rows
    vmem = pl.BlockSpec(memory_space=pltpu.VMEM)
    return pl.pallas_call(
        gathered_kernel,
        out_shape=jax.ShapeDtypeStruct((rows, value_up_t.shape[0]), jnp.bfloat16),
        in_specs=[vmem] * 4,
        out_specs=vmem,
        scratch_shapes=[
            pltpu.VMEM((heads, lanes, wide), jnp.bfloat16),
            pltpu.VMEM((heads, lanes, wide), jnp.bfloat16),
            pltpu.VMEM((heads, rows, lanes), jnp.float32),
            pltpu.VMEM((heads, rows, lanes), jnp.float32),
        ],
        compiler_params=pltpu.CompilerParams(vmem_limit_bytes=48 << 20),
        cost_estimate=pl.CostEstimate(
            flops=20_000_000_000, bytes_accessed=8 << 20, transcendentals=20_000_000
        ),
        name="gathered_attention",
    )(q_heads, lat_all, key_up_t, value_up_t)


def conv_kernel(gated_ref, rim_ref, taps_ref, out_ref, wide):
    rows, chans = gated_ref.shape
    rim = rim_ref.shape[0]
    taps = taps_ref.shape[0]
    chunk = 64
    for part in range(chans // 128):
        cols = slice(part * 128, (part + 1) * 128)
        wide[part, :rim, :] = rim_ref[:, cols].astype(jnp.float32)
        wide[part, rim:, :] = gated_ref[:, cols].astype(jnp.float32)
        coeff = taps_ref[:, cols]

        def band(step, carry):
            base = step * chunk
            total = jnp.zeros((chunk, 128), jnp.float32)
            for tap in range(taps):
                total = total + coeff[tap : tap + 1, :] * wide[
                    part, pl.ds(base + (rim - taps + 1 + tap), chunk), :
                ]
            out_ref[pl.ds(pl.multiple_of(base, chunk), chunk), cols] = total
            return carry

        lax.fori_loop(0, rows // chunk, band, 0)


def convolve(gated, rim, taps):
    rows, chans = gated.shape
    vmem = pl.BlockSpec(memory_space=pltpu.VMEM)
    return pl.pallas_call(
        conv_kernel,
        out_shape=jax.ShapeDtypeStruct((rows, chans), jnp.float32),
        in_specs=[vmem] * 3,
        out_specs=vmem,
        scratch_shapes=[pltpu.VMEM((chans // 128, rows + rim.shape[0], 128), jnp.float32)],
        cost_estimate=pl.CostEstimate(
            flops=2 * rows * chans * 31, bytes_accessed=2 << 20, transcendentals=0
        ),
        name="depthwise",
    )(gated, rim, taps)


def shards(
    tokens,
    input_gain,
    query_weight,
    query_rot_weight,
    kv_down,
    rot_down,
    kv_gain,
    key_up,
    value_up,
    conv_value_weight,
    conv_gate_weight,
    conv_taps,
    conv_ln_gain,
    conv_ln_bias,
    att_out_gain,
    conv_out_gain,
    att_out_weight,
    conv_out_weight,
):
    tok_rows = tokens.shape[0]
    heads_here = key_up.shape[1] // NOPE_DIM
    chan_here = conv_taps.shape[1]
    weight_list = (
        query_weight,
        query_rot_weight,
        kv_down,
        rot_down,
        conv_value_weight,
        conv_gate_weight,
    )
    seats = lax.axis_size("sp")
    if (
        lax.axis_size("tp") == 2
        and seats % PLANE == 0
        and tok_rows % 128 == 0
        and heads_here % 2 == 0
    ):
        gains = (
            input_gain, kv_gain, conv_ln_gain, conv_ln_bias, att_out_gain, conv_out_gain
        )
        return fused(
            tokens,
            tuple(gain[None, :] for gain in gains),
            (
                kv_down, rot_down.T, conv_gate_weight, conv_value_weight, query_weight,
                query_rot_weight, key_up, value_up, att_out_weight, conv_out_weight,
            ),
            conv_taps,
            seats,
        )
    whole_rows = lax.all_gather(tokens, "tp", axis=1, tiled=True).astype(jnp.float32)
    scaled = (whole_rows * input_gain[None, :]).astype(jnp.bfloat16)
    row_scale = lax.rsqrt(jnp.mean(whole_rows * whole_rows, axis=1, keepdims=True) + norm_eps)

    def add_product(weight):
        return jnp.dot(scaled, weight, preferred_element_type=jnp.float32)

    summed = tuple((add_product(weight) for weight in weight_list))
    q_acc, qrot_acc, latent_raw, rot_acc, value_acc, gate_acc = summed
    positions = lax.axis_index("sp") * tok_rows + jnp.arange(tok_rows, dtype=jnp.int32)
    cos_table, sine_table = rotary_tables(positions, ROT_DIM // 2)
    fold = math.log2(math.e) / math.sqrt(NOPE_DIM + ROT_DIM)
    query_scale = row_scale * fold
    plain_q = (q_acc * query_scale).reshape(tok_rows, heads_here, NOPE_DIM)
    turned_q = rotate_half(
        (qrot_acc * query_scale).reshape(tok_rows, heads_here, ROT_DIM),
        cos_table[:, None, :],
        sine_table[:, None, :],
    )
    blank = jnp.zeros((tok_rows, heads_here, 128 - NOPE_DIM - ROT_DIM), jnp.float32)
    q_heads = jnp.transpose(
        jnp.concatenate([plain_q, turned_q, blank], axis=2).astype(jnp.bfloat16), (1, 0, 2)
    )
    latent = (
        latent_raw
        * lax.rsqrt(jnp.mean(latent_raw * latent_raw, axis=1, keepdims=True) + norm_eps)
        * kv_gain[None, :]
    ).astype(jnp.bfloat16)
    key_rot = rotate_half(rot_acc * row_scale, cos_table, sine_table).astype(jnp.bfloat16)
    gated_input = (value_acc * row_scale * jax.nn.sigmoid(gate_acc * row_scale)).astype(
        jnp.bfloat16
    )
    packed = jnp.concatenate([latent.T, key_rot.T], axis=0)
    rim_rows = shifted(gated_input[tok_rows - (KERNEL + 1) :], "sp", 1)
    conv_out = convolve(gated_input, rim_rows, conv_taps)
    moment_one, moment_two = lax.psum(
        (jnp.sum(conv_out, axis=1), jnp.sum(conv_out * conv_out, axis=1)), "tp"
    )
    mean_val = moment_one / CONV_CH
    spread = moment_two / CONV_CH - mean_val * mean_val
    normed = (conv_out - mean_val[:, None]) * lax.rsqrt(spread + norm_eps)[:, None]
    swished = jax.nn.silu(normed * conv_ln_gain[None, :] + conv_ln_bias[None, :])
    lat_all = lax.all_gather(packed, "sp", axis=0)
    attended = gathered_attention(q_heads, lat_all, key_up.T, value_up.T).astype(jnp.float32)
    att_sq, conv_sq = lax.psum(
        (
            jnp.sum(attended * attended, axis=1, keepdims=True),
            jnp.sum(swished * swished, axis=1, keepdims=True),
        ),
        "tp",
    )
    att_mixed = (
        attended * lax.rsqrt(att_sq / ATT_WIDTH + norm_eps) * att_out_gain[None, :]
    ).astype(jnp.bfloat16)
    conv_mixed = (
        swished * lax.rsqrt(conv_sq / CONV_CH + norm_eps) * conv_out_gain[None, :]
    ).astype(jnp.bfloat16)
    share = (
        jnp.dot(att_mixed, att_out_weight, preferred_element_type=jnp.float32)
        + jnp.dot(conv_mixed, conv_out_weight, preferred_element_type=jnp.float32)
    ).astype(jnp.bfloat16)
    return lax.psum_scatter(share, "tp", scatter_dimension=1, tiled=True)


def solution(mesh):
    return jax.shard_map(
        shards,
        mesh=mesh,
        in_specs=(
            P("sp", "tp"),
            P(),
            P(None, "tp"),
            P(None, "tp"),
            P(),
            P(),
            P(),
            P(None, "tp"),
            P(None, "tp"),
            P(None, "tp"),
            P(None, "tp"),
            P(None, "tp"),
            P("tp"),
            P("tp"),
            P("tp"),
            P("tp"),
            P("tp", None),
            P("tp", None),
        ),
        out_specs=P("sp", "tp"),
        check_vma=False,
    )
```

```python
import functools
import math

import jax
import jax.numpy as jnp
import numpy as np
from jax import lax
from jax.experimental import pallas as pl
from jax.experimental.pallas import tpu as pltpu
from jax.sharding import PartitionSpec as P

D_MODEL = 2048
NOPE_DIM = 64
ROT_DIM = 32
VALUE_DIM = 64
CONV_CH = 1024
KERNEL = 31
ATT_WIDTH = 1024


norm_eps = 1e-06
far_below = -1e30
rope_base = 10000.0


def shifted(block, axis, distance):
    devices = range(lax.axis_size(axis))
    route = [(i - distance, i) for i in devices if i - distance in devices]
    return lax.ppermute(block, axis, route)


def rotary_tables(positions, half_dim):
    frequency = rope_base ** (-jnp.arange(half_dim, dtype=jnp.float32) / half_dim)
    angles = positions.astype(jnp.float32)[:, None] * frequency[None, :]
    return (jnp.cos(angles), jnp.sin(angles))


def rotate_half(values, cos_table, sine_table):
    half_dim = cos_table.shape[-1]
    front_half = values[..., :half_dim]
    back_half = values[..., half_dim:]
    return jnp.concatenate(
        [
            front_half * cos_table - back_half * sine_table,
            back_half * cos_table + front_half * sine_table,
        ],
        axis=-1,
    )


MESH = pl.DeviceIdType.MESH


def push(src, dst, send, recv, target):
    return pltpu.make_async_remote_copy(
        src_ref=src,
        dst_ref=dst,
        send_sem=send,
        recv_sem=recv,
        device_id=target,
        device_id_type=MESH,
    )


def other_core():
    return {"sp": lax.axis_index("sp"), "tp": 1 - lax.axis_index("tp")}


PLANE = 4


def layer_kernel(
    tok_hbm, gain_ref, kv_gain_ref, base_ref, seat_ref, taps_ref, ln_gain_ref, ln_bias_ref,
    att_gain_ref, conv_gain_ref,
    kvd_hbm, rotw_hbm, cgw_hbm, cvw_hbm, qw_hbm, qrw_hbm, kup_hbm, vup_hbm, att_hbm, conv_hbm,
    out_ref,
    kvd, rotw, cgw, cvw, qw, qrw, kup, vup, att_w, conv_w, vup_t,
    tok, landed, scaled, narrow, gated, rim, wide, conv, sq_mine, sq_other,
    lat_ref, q2, kn, kr, vt, run_max, acc, s_ref, att_t, end_mine, end_other,
    att_sq, att_sq_other, att_act, conv_act, out_stage,
    w_sem, w_send, w_recv, tok_load, tok_send, tok_recv, rim_send, rim_recv, sq_send, sq_recv,
    csq_send, csq_recv, asq_send, asq_recv, conv_send, conv_recv, att_send, att_recv,
    col_send, plane_send, core_send, link_recv, core_recv, out_sem,
):
    mine = lax.axis_index("tp")
    me = lax.axis_index("sp")
    seats = lax.axis_size("sp")
    rows, width = tok.shape
    blocks = lat_ref.shape[0]
    rank = kvd.shape[1]
    layers = blocks // PLANE
    layer = me // PLANE
    spot = me % PLANE
    height = lat_ref.shape[1] // 2
    half = pl.ds(pl.multiple_of(mine * height, 16), height)
    other = other_core()
    ahead = {"sp": (me + 1) % seats, "tp": mine}
    behind = {"sp": (me + seats - 1) % seats, "tp": mine}

    def columns(owner):
        return pl.ds(pl.multiple_of(owner * width, 128), width)

    loads = [
        pltpu.make_async_copy(src, dst, w_sem.at[index])
        for index, (src, dst) in enumerate(
            (
                (kvd_hbm, kvd), (rotw_hbm, rotw), (cgw_hbm, cgw), (cvw_hbm, cvw),
                (qw_hbm, qw), (qrw_hbm, qrw), (kup_hbm, kup), (vup_hbm, vup),
                (att_hbm.at[:, columns(mine)], att_w.at[0]),
                (conv_hbm.at[:, columns(mine)], conv_w.at[0]),
            )
        )
    ]
    fetch = pltpu.make_async_copy(tok_hbm, tok, tok_load)
    fetch.start()
    for load in loads[:2]:
        load.start()
    gifts = [
        push(src.at[:, columns(1 - mine)], dst.at[1], w_send.at[index], w_recv.at[index], other)
        for index, (src, dst) in enumerate(((att_hbm, att_w), (conv_hbm, conv_w)))
    ]

    def spot_at(distance):
        return (spot + distance) % PLANE

    def at(layer_id, spot_id):
        return {"sp": layer_id * PLANE + spot_id, "tp": mine}

    barrier = pltpu.get_barrier_semaphore()
    peers = [at(layer, spot_at(d)) for d in range(1, PLANE)] + [other]
    for peer in peers:
        pl.semaphore_signal(barrier, inc=1, device_id=peer, device_id_type=MESH)
    above = at(jnp.minimum(layer + 1, layers - 1), spot)
    below = at(jnp.maximum(layer - 1, 0), spot)
    for condition, peer in (
        (layer < layers - 1, above), (layer > 0, below), (me < seats - 1, ahead), (me > 0, behind),
    ):

        @pl.when(condition)
        def _(peer=peer):
            pl.semaphore_signal(barrier, inc=1, device_id=peer, device_id_type=MESH)

    q2[...] = jnp.zeros(q2.shape, jnp.bfloat16)
    pairs, _, both = q2.shape
    keys_wide = kn.shape[1]
    ones_low = VALUE_DIM
    ones_high = vt.shape[2] - VALUE_DIM
    vt[:, :, ones_low:ones_high, :] = jnp.ones(
        (2, pairs, ones_high - ones_low, keys_wide), jnp.bfloat16
    )
    pl.semaphore_wait(
        barrier,
        len(peers)
        + jnp.minimum(me, 1)
        + jnp.minimum(seats - 1 - me, 1)
        + jnp.minimum(layer, 1)
        + jnp.minimum(layers - 1 - layer, 1),
    )
    fetch.wait()
    tok_copy = push(tok, landed, tok_send, tok_recv, other)
    tok_copy.start()
    for load in loads[2:]:
        load.start()

    def place(block, index):
        cols = pl.ds(pl.multiple_of(index * width, 128), width)
        full = block[...].astype(jnp.float32)
        scaled[:, cols] = (full * gain_ref[:, cols]).astype(jnp.bfloat16)
        return jnp.sum(full * full, axis=1, keepdims=True)

    squares = place(tok, mine)
    column = lax.broadcasted_iota(jnp.int32, seat_ref.shape, 1)
    seat_turn = jnp.sum(
        jnp.where(column == me, seat_ref[...], 0.0), axis=1, keepdims=True
    )
    turn = ROT_DIM // 2
    seat_cos, seat_sin = seat_turn[:turn], seat_turn[turn:]
    base_cos, base_sin = base_ref[:turn], base_ref[turn:]
    cos_table = seat_cos * base_cos - seat_sin * base_sin
    sin_table = seat_sin * base_cos + seat_cos * base_sin

    def rotate(block):
        front = block[:turn]
        back = block[turn : 2 * turn]
        return jnp.concatenate(
            [front * cos_table - back * sin_table, back * cos_table + front * sin_table], axis=0
        )

    tok_copy.wait()
    squares = squares + place(landed, 1 - mine)
    row_scale = lax.rsqrt(squares / (2 * width) + norm_eps)

    def project(weight):
        return jnp.dot(scaled[...], weight[...], preferred_element_type=jnp.float32)

    loads[0].wait()
    loads[1].wait()
    raw = project(kvd)
    latent = (
        raw
        * lax.rsqrt(jnp.mean(raw * raw, axis=1, keepdims=True) + norm_eps)
        * kv_gain_ref[...]
    )
    lat_ref[me, :rows, :] = latent.astype(jnp.bfloat16)
    narrow[...] = jnp.broadcast_to(row_scale, narrow.shape)
    key_turn = lax.dot_general(
        rotw[...], scaled[...], (((1,), (1,)), ((), ())), preferred_element_type=jnp.float32
    )
    key_rot = rotate(key_turn * narrow[...].T[:ROT_DIM]).astype(jnp.bfloat16)
    across = rank // 128
    for piece in range(across * ((rows // 128 + across - 1) // across)):
        band = rows + piece // across * ROT_DIM
        lanes = slice(piece % across * 128, piece % across * 128 + 128)
        lat_ref[me, band : band + ROT_DIM, lanes] = (
            key_rot[:, piece * 128 : piece * 128 + 128]
            if piece < rows // 128
            else jnp.zeros((ROT_DIM, 128), jnp.bfloat16)
        )

    def column_copy(block):
        spread = lat_ref.at[block, half]
        return push(spread, spread, col_send.at[block // PLANE], link_recv.at[block], above)

    def rise(block):
        @pl.when(layer + 1 < layers)
        def _():
            column_copy(block).start()

    def plane_copy(block, distance):
        return push(
            lat_ref.at[block, half],
            lat_ref.at[block, half],
            plane_send.at[block // PLANE, distance - 1],
            link_recv.at[block],
            at(layer, spot_at(distance)),
        )

    def core_copy(block):
        spread = lat_ref.at[block, half]
        return push(spread, spread, core_send.at[block], core_recv.at[block], other)

    rise(me)
    for d in range(1, PLANE):
        plane_copy(me, d).start()
    for gift in gifts:
        gift.start()

    def arrive(block):
        spread = lat_ref.at[block, half]
        push(spread, spread, core_send.at[block], link_recv.at[block], other).wait_recv()

    def relay(step):
        @pl.when(step <= layer)
        def _():
            block = (layer - step) * PLANE + spot
            arrive(block)
            rise(block)
            for d in range(1, PLANE):
                plane_copy(block, d).start()
            core_copy(block).start()

    def hand_over(step):
        @pl.when(step <= layer)
        def _():
            for d in range(1, PLANE):
                block = (layer - step) * PLANE + spot_at(d)
                arrive(block)
                core_copy(block).start()

    loads[2].wait()
    loads[3].wait()
    gate = project(cgw) * row_scale
    gated[...] = (project(cvw) * row_scale * jax.nn.sigmoid(gate)).astype(jnp.bfloat16)
    edge = rim.shape[0]
    rim_copy = push(gated.at[pl.ds(rows - edge, edge)], rim, rim_send, rim_recv, ahead)

    @pl.when(me < seats - 1)
    def _():
        rim_copy.start()

    loads[4].wait()
    loads[5].wait()
    query_scale = row_scale * (math.log2(math.e) / math.sqrt(NOPE_DIM + ROT_DIM))
    plain = (project(qw) * query_scale).T.astype(jnp.bfloat16)
    turned = (project(qrw) * query_scale).T
    for head in range(2 * pairs):
        side = head % 2
        cols = slice(side * rows, (side + 1) * rows)
        q2[head // 2, side * NOPE_DIM : (side + 1) * NOPE_DIM, cols] = plain[
            head * NOPE_DIM : (head + 1) * NOPE_DIM
        ]
        q2[head // 2, 2 * NOPE_DIM : 2 * NOPE_DIM + ROT_DIM, cols] = rotate(
            turned[head * ROT_DIM : (head + 1) * ROT_DIM]
        ).astype(jnp.bfloat16)

    loads[7].wait()
    vup_t[...] = vup[...].astype(jnp.float32).T.astype(jnp.bfloat16)

    taps = taps_ref.shape[0]
    chunk = 64

    def band_step(step, carry, slab):
        cols = slice(slab * 128, (slab + 1) * 128)
        coeff = taps_ref[:, cols]
        base = step * chunk
        total = jnp.zeros((chunk, 128), jnp.float32)
        for tap in range(taps):
            total = total + coeff[tap : tap + 1, :] * wide[
                slab, pl.ds(base + (edge - taps + 1 + tap), chunk), :
            ]
        conv[pl.ds(pl.multiple_of(base, chunk), chunk), cols] = total
        return carry

    slabs = conv.shape[1] // 128
    for slab in range(slabs):
        wide[slab, edge:, :] = gated[:, slab * 128 : (slab + 1) * 128].astype(jnp.float32)
        lax.fori_loop(1, rows // chunk, functools.partial(band_step, slab=slab), 0)
        if slab == slabs // 2:
            relay(1)
    hand_over(0)

    @pl.when(me > 0)
    def _():
        rim_copy.wait_recv()

    @pl.when(me == 0)
    def _():
        rim[...] = jnp.zeros(rim.shape, jnp.bfloat16)

    for slab in range(slabs):
        wide[slab, :edge, :] = rim[:, slab * 128 : (slab + 1) * 128].astype(jnp.float32)
        band_step(0, 0, slab)

    values = conv[...]
    for slot, total in enumerate((values, values * values)):
        sq_mine[:, slot * 128 : (slot + 1) * 128] = jnp.broadcast_to(
            jnp.sum(total, axis=1, keepdims=True), (rows, 128)
        )
    sums = push(sq_mine, sq_other, sq_send, sq_recv, other)
    sums.start()

    def activate():
        sums.wait()
        values = conv[...]
        moments = (sq_mine[...] + sq_other[...]) / CONV_CH
        mean_val = moments[:, :1]
        spread_val = moments[:, 128:129] - mean_val * mean_val
        normed = (values - mean_val) * lax.rsqrt(spread_val + norm_eps)
        swished = jax.nn.silu(normed * ln_gain_ref[...] + ln_bias_ref[...])
        conv_act[0] = (swished * conv_gain_ref[...]).astype(jnp.bfloat16)
        end_mine[...] = jnp.broadcast_to(
            jnp.sum(swished * swished, axis=1, keepdims=True), (rows, 128)
        )
        conv_sum.start()
        conv_copy.start()

    conv_sum = push(end_mine, end_other, csq_send, csq_recv, other)
    conv_copy = push(conv_act.at[0], conv_act.at[1], conv_send, conv_recv, other)

    def gathered(step):
        for d in range(1, PLANE):
            core_copy((layer - step) * PLANE + spot_at(d)).wait_recv()

    strip = 256
    strips = keys_wide // strip

    def expand(group, slot, index):
        pieces = []
        low, left = index * strip, strip
        while left > 0:
            take = min(rows - low % rows, left)
            pieces.append(
                lat_ref[group * PLANE + low // rows, low % rows : low % rows + take, :]
            )
            low, left = low + take, left - take
        lat = pieces[0] if len(pieces) == 1 else jnp.concatenate(pieces, axis=0)
        cut = slice(index * strip, (index + 1) * strip)
        kn[slot, cut, :] = jnp.dot(
            lat, kup[...], preferred_element_type=jnp.float32
        ).astype(jnp.bfloat16)
        values = lax.dot_general(
            vup_t[...], lat, (((1,), (1,)), ((), ())), preferred_element_type=jnp.float32
        ).astype(jnp.bfloat16)
        for pair in range(pairs):
            low = 2 * VALUE_DIM * pair
            vt[slot, pair, :ones_low, cut] = values[low : low + VALUE_DIM]
            vt[slot, pair, ones_high:, cut] = values[low + VALUE_DIM : low + 2 * VALUE_DIM]
        for blk in range(index, PLANE, strips):
            pieces = []
            for piece in range(rows // 128):
                band = rows + piece // across * ROT_DIM
                lanes = slice(piece % across * 128, piece % across * 128 + 128)
                pieces.append(lat_ref[group * PLANE + blk, band : band + ROT_DIM, lanes])
            rot = jnp.concatenate(pieces, axis=1).astype(jnp.float32)
            rot = jnp.concatenate([rot, jnp.zeros((128 - ROT_DIM, rows), jnp.float32)], axis=0)
            kr[slot, blk * rows : (blk + 1) * rows, :] = rot.T.astype(jnp.bfloat16)

    tiles = both // 256
    tile_rows = tuple(
        (
            0 if 256 * tile < rows else ones_low,
            ones_high if 256 * (tile + 1) <= rows else vt.shape[2],
        )
        for tile in range(tiles)
    )

    def attend(slot, first, hidden, middle, following):
        def score(pair, index):
            cut = slice(index * strip, (index + 1) * strip)
            keys = jnp.concatenate(
                [kn[slot, cut, 128 * pair : 128 * pair + 128], kr[slot, cut, :]], axis=1
            )
            scores = jnp.dot(keys, q2[pair], preferred_element_type=jnp.float32)
            if hidden is not None:
                scores = jnp.where(hidden(index), far_below, scores)
            s_ref[pair % 2, cut, :] = scores
            return jnp.max(scores, axis=0, keepdims=True)

        tops = [score(0, index) for index in range(strips)]
        for pair in range(pairs):
            middle(pair)
            top = tops[0]
            for value in tops[1:]:
                top = jnp.maximum(top, value)
            if not first:
                old = run_max[pair : pair + 1, :]
                top = jnp.maximum(old, top)
                fade = jnp.exp2(old - top)
            run_max[pair : pair + 1, :] = top
            tops = []
            sums = [None] * tiles
            for index in range(strips):
                cut = slice(index * strip, (index + 1) * strip)
                if pair + 1 < pairs:
                    tops.append(score(pair + 1, index))
                weights = jnp.exp2(s_ref[pair % 2, cut, :] - top).astype(jnp.bfloat16)
                for tile, (low, high) in enumerate(tile_rows):
                    new = jnp.dot(
                        vt[slot, pair, low:high, cut],
                        weights[:, 256 * tile : 256 * (tile + 1)],
                        preferred_element_type=jnp.float32,
                    )
                    sums[tile] = new if sums[tile] is None else sums[tile] + new
                if pair + 1 == pairs:
                    expand(following, 1 - slot, index)
            for tile, (low, high) in enumerate(tile_rows):
                new = sums[tile]
                if not first:
                    new = new + acc[pair, tile, : high - low, :] * fade[
                        :, 256 * tile : 256 * (tile + 1)
                    ]
                acc[pair, tile, : high - low, :] = new

    def hidden(index):
        key = layer * keys_wide + index * strip + lax.broadcasted_iota(
            jnp.int32, (strip, both), 0
        )
        query = lax.broadcasted_iota(jnp.int32, (strip, both), 1)
        return key > me * rows + jnp.where(query >= rows, query - rows, query)

    loads[6].wait()
    gathered(0)
    for index in range(strips):
        expand(layer, 0, index)

    def ready(step):
        @pl.when(step <= layer)
        def _():
            for d in range(PLANE):
                core_copy((layer - step) * PLANE + spot_at(d)).wait_recv()

    def first_middle(pair):
        if pair == pairs // 2:
            relay(2)
            hand_over(1)
            activate()
        if pair == pairs - 1:
            ready(1)

    attend(0, True, hidden, first_middle, jnp.maximum(layer - 1, 0))

    def far(step, carry):
        def middle(pair):
            if pair == pairs // 2:
                relay(step + 2)
                hand_over(step + 1)
            if pair == pairs - 1:
                ready(step + 1)

        attend(step % 2, False, None, middle, jnp.maximum(layer - step - 1, 0))
        return carry

    lax.fori_loop(1, layer + 1, far, 0)

    for pair in range(pairs):
        for side in range(2):
            pieces = []
            for tile, (low, high) in enumerate(tile_rows):
                start = max(side * rows, 256 * tile)
                stop = min((side + 1) * rows, 256 * (tile + 1))
                if start >= stop:
                    continue
                total = acc[pair, tile, : high - low, start - 256 * tile : stop - 256 * tile]
                base = 0 if side == 0 else ones_high - low
                pieces.append(
                    total[base : base + VALUE_DIM] / total[ones_low - low : ones_low - low + 1]
                )
            low = (2 * pair + side) * VALUE_DIM
            att_t[low : low + VALUE_DIM, :] = (
                jnp.concatenate(pieces, axis=1).astype(jnp.bfloat16).astype(jnp.float32)
            )
    attended = att_t[...]
    att_sq[...] = jnp.broadcast_to(
        jnp.sum(attended * attended, axis=0, keepdims=True), att_sq.shape
    )
    att_act[0] = (attended.T * att_gain_ref[...]).astype(jnp.bfloat16)
    att_sum = push(att_sq, att_sq_other, asq_send, asq_recv, other)
    att_sum.start()
    att_copy = push(att_act.at[0], att_act.at[1], att_send, att_recv, other)
    att_copy.start()
    for index in (8, 9):
        loads[index].wait()
    for gift in gifts:
        gift.wait()
    conv_sum.wait()
    conv_copy.wait()
    conv_scale = lax.rsqrt((end_mine[...] + end_other[...])[:, :1] / CONV_CH + norm_eps)

    def product(activations, weight):
        return jnp.dot(activations, weight, preferred_element_type=jnp.float32)

    base_part = (
        product(conv_act[0], conv_w[0]) + product(conv_act[1], conv_w[1])
    ) * conv_scale
    own_part = product(att_act[0], att_w[0])
    att_sum.wait()
    squares_t = jnp.broadcast_to(att_sq[:1] + att_sq_other[:1], (128, rows)).T
    att_scale = lax.rsqrt(squares_t[:, :1] / ATT_WIDTH + norm_eps)
    att_copy.wait()
    leaves = []
    for index in range(width // 256):
        cols = slice(index * 256, (index + 1) * 256)
        out_stage[:, cols] = (
            (own_part[:, cols] + product(att_act[1], att_w[1, :, cols])) * att_scale
            + base_part[:, cols]
        ).astype(jnp.bfloat16)
        leave = pltpu.make_async_copy(
            out_stage.at[:, cols], out_ref.at[:, cols], out_sem.at[index]
        )
        leave.start()
        leaves.append(leave)

    @pl.when(me < seats - 1)
    def _():
        rim_copy.wait_send()

    def settle(step, carry):
        base = (layer - step) * PLANE
        for d in range(1, PLANE):
            plane_copy(base + spot, d).wait_send()
            core_copy(base + spot_at(d)).wait_send()

        @pl.when(layer + 1 < layers)
        def _():
            column_copy(base + spot).wait_send()

        @pl.when(step > 0)
        def _():
            core_copy(base + spot).wait_send()

        return carry

    lax.fori_loop(0, layer + 1, settle, 0)
    for leave in leaves:
        leave.wait()


def angle_tables(seats, rows):
    frequency = rope_base ** (-np.arange(ROT_DIM // 2) / (ROT_DIM // 2))

    def table(positions):
        angles = frequency[:, None] * positions[None, :]
        return jnp.asarray(
            np.concatenate([np.cos(angles), np.sin(angles)], axis=0), jnp.float32
        )

    return table(np.arange(rows)), table(rows * np.arange(-(-seats // 128) * 128))


def fused(tokens, gains, matrices, taps, seats):
    rows, width = tokens.shape
    chans = taps.shape[1]
    rank = matrices[0].shape[1]
    heads = matrices[4].shape[1] // NOPE_DIM
    pairs = heads // 2
    keys_wide = PLANE * rows
    layers = seats // PLANE
    across = rank // 128
    height = rows + -(-(rows // 128) // across) * ROT_DIM
    vmem = pl.BlockSpec(memory_space=pltpu.VMEM)
    anywhere = pl.BlockSpec(memory_space=pltpu.HBM)
    dma = pltpu.SemaphoreType.DMA
    edge = 32
    bf16 = jnp.bfloat16
    f32 = jnp.float32
    value_rows = 2 * VALUE_DIM + 16
    base, seat = angle_tables(seats, rows)
    input_gain, kv_gain, ln_gain, ln_bias, att_gain, conv_gain = gains
    return pl.pallas_call(
        layer_kernel,
        out_shape=jax.ShapeDtypeStruct((rows, width), bf16),
        in_specs=[anywhere] + [vmem] * 9 + [anywhere] * 10,
        out_specs=anywhere,
        scratch_shapes=[pltpu.VMEM(matrix.shape, bf16) for matrix in matrices[:8]]
        + [
            pltpu.VMEM((2, matrix.shape[0], width), bf16) for matrix in matrices[8:]
        ]
        + [
            pltpu.VMEM(matrices[7].shape[::-1], bf16),
            pltpu.VMEM((rows, width), bf16),
            pltpu.VMEM((rows, width), bf16),
            pltpu.VMEM((rows, 2 * width), bf16),
            pltpu.VMEM((rows, 128), f32),
            pltpu.VMEM((rows, chans), bf16),
            pltpu.VMEM((edge, chans), bf16),
            pltpu.VMEM((chans // 128, rows + edge, 128), f32),
            pltpu.VMEM((rows, chans), f32),
            pltpu.VMEM((rows, 256), f32),
            pltpu.VMEM((rows, 256), f32),
            pltpu.VMEM((seats, height, rank), bf16),
            pltpu.VMEM((pairs, 256, 2 * rows), bf16),
            pltpu.VMEM((2, keys_wide, heads * NOPE_DIM), bf16),
            pltpu.VMEM((2, keys_wide, 128), bf16),
            pltpu.VMEM((2, pairs, value_rows, keys_wide), bf16),
            pltpu.VMEM((max(pairs, 8), 2 * rows), f32),
            pltpu.VMEM((pairs, 2 * rows // 256, value_rows, 256), f32),
            pltpu.VMEM((2, keys_wide, 2 * rows), f32),
            pltpu.VMEM((heads * VALUE_DIM, rows), f32),
            pltpu.VMEM((rows, 128), f32),
            pltpu.VMEM((rows, 128), f32),
            pltpu.VMEM((8, rows), f32),
            pltpu.VMEM((8, rows), f32),
            pltpu.VMEM((2, rows, heads * VALUE_DIM), bf16),
            pltpu.VMEM((2, rows, chans), bf16),
            pltpu.VMEM((rows, width), bf16),
            dma((len(matrices),)),
            dma((2,)),
            dma((2,)),
        ]
        + [dma] * 15
        + [
            dma((layers,)),
            dma((layers, PLANE - 1)),
            dma((seats,)),
            dma((seats,)),
            dma((seats,)),
            dma((width // 256,)),
        ],
        compiler_params=pltpu.CompilerParams(
            vmem_limit_bytes=60 << 20, collective_id=0, has_side_effects=True
        ),
        name="layer",
    )(tokens, input_gain, kv_gain, base, seat, taps, ln_gain, ln_bias, att_gain, conv_gain, *matrices)


def gathered_kernel(q_ref, lat_ref, kup_ref, vup_ref, o_ref, kt, vt, run_max, acc):
    heads, rows, lanes = q_ref.shape
    blocks = lat_ref.shape[0]
    rank = kup_ref.shape[1]
    nope = kup_ref.shape[0] // heads
    vdim = vup_ref.shape[0] // heads
    rot = lat_ref.shape[1] - rank
    wide = kt.shape[2]
    group = wide // rows
    me = lax.axis_index("sp")
    last = me // group
    kt[:, nope + rot :, :] = jnp.zeros((heads, lanes - nope - rot, wide), jnp.bfloat16)
    vt[:, vdim:, :] = jnp.ones((heads, lanes - vdim, wide), jnp.bfloat16)

    def expand(block):
        for part in range(group):
            src = jnp.minimum(block * group + part, blocks - 1)
            lat = lat_ref[src, :rank, :]
            turned = lat_ref[src, rank:, :]
            cols = slice(part * rows, (part + 1) * rows)
            keys = jnp.dot(kup_ref[...], lat, preferred_element_type=jnp.float32)
            values = jnp.dot(vup_ref[...], lat, preferred_element_type=jnp.float32)
            for head in range(heads):
                kt[head, :nope, cols] = keys[head * nope : (head + 1) * nope].astype(jnp.bfloat16)
                kt[head, nope : nope + rot, cols] = turned
                vt[head, :vdim, cols] = values[head * vdim : (head + 1) * vdim].astype(
                    jnp.bfloat16
                )

    def weigh(head, scores, top):
        weights = jnp.exp2(scores - top).astype(jnp.bfloat16)
        return lax.dot_general(
            weights, vt[head], (((1,), (1,)), ((), ())), preferred_element_type=jnp.float32
        )

    expand(last)
    key_pos = last * wide + lax.broadcasted_iota(jnp.int32, (rows, wide), 1)
    query_pos = me * rows + lax.broadcasted_iota(jnp.int32, (rows, wide), 0)
    hidden = key_pos > query_pos
    for head in range(heads):
        scores = jnp.dot(q_ref[head], kt[head], preferred_element_type=jnp.float32)
        scores = jnp.where(hidden, far_below, scores)
        top = jnp.max(scores, axis=1, keepdims=True)
        run_max[head] = jnp.broadcast_to(top, (rows, lanes))
        acc[head] = weigh(head, scores, top)

    def visit(step, carry):
        expand(step)
        for head in range(heads):
            scores = jnp.dot(q_ref[head], kt[head], preferred_element_type=jnp.float32)
            old = run_max[head]
            top = jnp.maximum(old[:, :1], jnp.max(scores, axis=1, keepdims=True))
            wide_top = jnp.broadcast_to(top, (rows, lanes))
            run_max[head] = wide_top
            acc[head] = acc[head] * jnp.exp2(old - wide_top) + weigh(head, scores, top)
        return carry

    lax.fori_loop(0, last, visit, 0)
    lane = lax.broadcasted_iota(jnp.int32, (rows, lanes), 1)
    for pair in range(heads // 2):
        halves = []
        for head in (2 * pair, 2 * pair + 1):
            total = acc[head]
            halves.append(total / pltpu.roll(total, vdim, axis=1))
        both = jnp.where(lane < vdim, halves[0], pltpu.roll(halves[1], vdim, axis=1))
        o_ref[:, pair * lanes : (pair + 1) * lanes] = both.astype(jnp.bfloat16)


def gathered_attention(q_heads, lat_all, key_up_t, value_up_t):
    heads, rows, lanes = q_heads.shape
    blocks = lat_all.shape[0]
    wide = 2 * rows if blocks % 2 == 0 else rows
    vmem = pl.BlockSpec(memory_space=pltpu.VMEM)
    return pl.pallas_call(
        gathered_kernel,
        out_shape=jax.ShapeDtypeStruct((rows, value_up_t.shape[0]), jnp.bfloat16),
        in_specs=[vmem] * 4,
        out_specs=vmem,
        scratch_shapes=[
            pltpu.VMEM((heads, lanes, wide), jnp.bfloat16),
            pltpu.VMEM((heads, lanes, wide), jnp.bfloat16),
            pltpu.VMEM((heads, rows, lanes), jnp.float32),
            pltpu.VMEM((heads, rows, lanes), jnp.float32),
        ],
        compiler_params=pltpu.CompilerParams(vmem_limit_bytes=48 << 20),
        cost_estimate=pl.CostEstimate(
            flops=20_000_000_000, bytes_accessed=8 << 20, transcendentals=20_000_000
        ),
        name="gathered_attention",
    )(q_heads, lat_all, key_up_t, value_up_t)


def conv_kernel(gated_ref, rim_ref, taps_ref, out_ref, wide):
    rows, chans = gated_ref.shape
    rim = rim_ref.shape[0]
    taps = taps_ref.shape[0]
    chunk = 64
    for part in range(chans // 128):
        cols = slice(part * 128, (part + 1) * 128)
        wide[part, :rim, :] = rim_ref[:, cols].astype(jnp.float32)
        wide[part, rim:, :] = gated_ref[:, cols].astype(jnp.float32)
        coeff = taps_ref[:, cols]

        def band(step, carry):
            base = step * chunk
            total = jnp.zeros((chunk, 128), jnp.float32)
            for tap in range(taps):
                total = total + coeff[tap : tap + 1, :] * wide[
                    part, pl.ds(base + (rim - taps + 1 + tap), chunk), :
                ]
            out_ref[pl.ds(pl.multiple_of(base, chunk), chunk), cols] = total
            return carry

        lax.fori_loop(0, rows // chunk, band, 0)


def convolve(gated, rim, taps):
    rows, chans = gated.shape
    vmem = pl.BlockSpec(memory_space=pltpu.VMEM)
    return pl.pallas_call(
        conv_kernel,
        out_shape=jax.ShapeDtypeStruct((rows, chans), jnp.float32),
        in_specs=[vmem] * 3,
        out_specs=vmem,
        scratch_shapes=[pltpu.VMEM((chans // 128, rows + rim.shape[0], 128), jnp.float32)],
        cost_estimate=pl.CostEstimate(
            flops=2 * rows * chans * 31, bytes_accessed=2 << 20, transcendentals=0
        ),
        name="depthwise",
    )(gated, rim, taps)


def shards(
    tokens,
    input_gain,
    query_weight,
    query_rot_weight,
    kv_down,
    rot_down,
    kv_gain,
    key_up,
    value_up,
    conv_value_weight,
    conv_gate_weight,
    conv_taps,
    conv_ln_gain,
    conv_ln_bias,
    att_out_gain,
    conv_out_gain,
    att_out_weight,
    conv_out_weight,
):
    tok_rows = tokens.shape[0]
    heads_here = key_up.shape[1] // NOPE_DIM
    chan_here = conv_taps.shape[1]
    weight_list = (
        query_weight,
        query_rot_weight,
        kv_down,
        rot_down,
        conv_value_weight,
        conv_gate_weight,
    )
    seats = lax.axis_size("sp")
    if (
        lax.axis_size("tp") == 2
        and seats % PLANE == 0
        and tok_rows % 128 == 0
        and heads_here % 2 == 0
    ):
        gains = (
            input_gain, kv_gain, conv_ln_gain, conv_ln_bias, att_out_gain, conv_out_gain
        )
        return fused(
            tokens,
            tuple(gain[None, :] for gain in gains),
            (
                kv_down, rot_down.T, conv_gate_weight, conv_value_weight, query_weight,
                query_rot_weight, key_up, value_up, att_out_weight, conv_out_weight,
            ),
            conv_taps,
            seats,
        )
    whole_rows = lax.all_gather(tokens, "tp", axis=1, tiled=True).astype(jnp.float32)
    scaled = (whole_rows * input_gain[None, :]).astype(jnp.bfloat16)
    row_scale = lax.rsqrt(jnp.mean(whole_rows * whole_rows, axis=1, keepdims=True) + norm_eps)

    def add_product(weight):
        return jnp.dot(scaled, weight, preferred_element_type=jnp.float32)

    summed = tuple((add_product(weight) for weight in weight_list))
    q_acc, qrot_acc, latent_raw, rot_acc, value_acc, gate_acc = summed
    positions = lax.axis_index("sp") * tok_rows + jnp.arange(tok_rows, dtype=jnp.int32)
    cos_table, sine_table = rotary_tables(positions, ROT_DIM // 2)
    fold = math.log2(math.e) / math.sqrt(NOPE_DIM + ROT_DIM)
    query_scale = row_scale * fold
    plain_q = (q_acc * query_scale).reshape(tok_rows, heads_here, NOPE_DIM)
    turned_q = rotate_half(
        (qrot_acc * query_scale).reshape(tok_rows, heads_here, ROT_DIM),
        cos_table[:, None, :],
        sine_table[:, None, :],
    )
    blank = jnp.zeros((tok_rows, heads_here, 128 - NOPE_DIM - ROT_DIM), jnp.float32)
    q_heads = jnp.transpose(
        jnp.concatenate([plain_q, turned_q, blank], axis=2).astype(jnp.bfloat16), (1, 0, 2)
    )
    latent = (
        latent_raw
        * lax.rsqrt(jnp.mean(latent_raw * latent_raw, axis=1, keepdims=True) + norm_eps)
        * kv_gain[None, :]
    ).astype(jnp.bfloat16)
    key_rot = rotate_half(rot_acc * row_scale, cos_table, sine_table).astype(jnp.bfloat16)
    gated_input = (value_acc * row_scale * jax.nn.sigmoid(gate_acc * row_scale)).astype(
        jnp.bfloat16
    )
    packed = jnp.concatenate([latent.T, key_rot.T], axis=0)
    rim_rows = shifted(gated_input[tok_rows - (KERNEL + 1) :], "sp", 1)
    conv_out = convolve(gated_input, rim_rows, conv_taps)
    moment_one, moment_two = lax.psum(
        (jnp.sum(conv_out, axis=1), jnp.sum(conv_out * conv_out, axis=1)), "tp"
    )
    mean_val = moment_one / CONV_CH
    spread = moment_two / CONV_CH - mean_val * mean_val
    normed = (conv_out - mean_val[:, None]) * lax.rsqrt(spread + norm_eps)[:, None]
    swished = jax.nn.silu(normed * conv_ln_gain[None, :] + conv_ln_bias[None, :])
    lat_all = lax.all_gather(packed, "sp", axis=0)
    attended = gathered_attention(q_heads, lat_all, key_up.T, value_up.T).astype(jnp.float32)
    att_sq, conv_sq = lax.psum(
        (
            jnp.sum(attended * attended, axis=1, keepdims=True),
            jnp.sum(swished * swished, axis=1, keepdims=True),
        ),
        "tp",
    )
    att_mixed = (
        attended * lax.rsqrt(att_sq / ATT_WIDTH + norm_eps) * att_out_gain[None, :]
    ).astype(jnp.bfloat16)
    conv_mixed = (
        swished * lax.rsqrt(conv_sq / CONV_CH + norm_eps) * conv_out_gain[None, :]
    ).astype(jnp.bfloat16)
    share = (
        jnp.dot(att_mixed, att_out_weight, preferred_element_type=jnp.float32)
        + jnp.dot(conv_mixed, conv_out_weight, preferred_element_type=jnp.float32)
    ).astype(jnp.bfloat16)
    return lax.psum_scatter(share, "tp", scatter_dimension=1, tiled=True)


def solution(mesh):
    return jax.shard_map(
        shards,
        mesh=mesh,
        in_specs=(
            P("sp", "tp"),
            P(),
            P(None, "tp"),
            P(None, "tp"),
            P(),
            P(),
            P(),
            P(None, "tp"),
            P(None, "tp"),
            P(None, "tp"),
            P(None, "tp"),
            P(None, "tp"),
            P("tp"),
            P("tp"),
            P("tp"),
            P("tp"),
            P("tp", None),
            P("tp", None),
        ),
        out_specs=P("sp", "tp"),
        check_vma=False,
    )
```

```python
import functools
import math

import jax
import jax.numpy as jnp
import numpy as np
from jax import lax
from jax.experimental import pallas as pl
from jax.experimental.pallas import tpu as pltpu
from jax.sharding import PartitionSpec as P

D_MODEL = 2048
NOPE_DIM = 64
ROT_DIM = 32
VALUE_DIM = 64
CONV_CH = 1024
KERNEL = 31
ATT_WIDTH = 1024


norm_eps = 1e-06
far_below = -1e30
rope_base = 10000.0


def shifted(block, axis, distance):
    devices = range(lax.axis_size(axis))
    route = [(i - distance, i) for i in devices if i - distance in devices]
    return lax.ppermute(block, axis, route)


def rotary_tables(positions, half_dim):
    frequency = rope_base ** (-jnp.arange(half_dim, dtype=jnp.float32) / half_dim)
    angles = positions.astype(jnp.float32)[:, None] * frequency[None, :]
    return (jnp.cos(angles), jnp.sin(angles))


def rotate_half(values, cos_table, sine_table):
    half_dim = cos_table.shape[-1]
    front_half = values[..., :half_dim]
    back_half = values[..., half_dim:]
    return jnp.concatenate(
        [
            front_half * cos_table - back_half * sine_table,
            back_half * cos_table + front_half * sine_table,
        ],
        axis=-1,
    )


MESH = pl.DeviceIdType.MESH


def push(src, dst, send, recv, target):
    return pltpu.make_async_remote_copy(
        src_ref=src,
        dst_ref=dst,
        send_sem=send,
        recv_sem=recv,
        device_id=target,
        device_id_type=MESH,
    )


def other_core():
    return {"sp": lax.axis_index("sp"), "tp": 1 - lax.axis_index("tp")}


PLANE = 4


def layer_kernel(
    tok_hbm, gain_ref, kv_gain_ref, base_ref, seat_ref, taps_ref, ln_gain_ref, ln_bias_ref,
    att_gain_ref, conv_gain_ref,
    kvd_hbm, rotw_hbm, cgw_hbm, cvw_hbm, qw_hbm, qrw_hbm, kup_hbm, vup_hbm, att_hbm, conv_hbm,
    out_ref,
    kvd, rotw, cgw, cvw, qw, qrw, kup, vup, att_w, conv_w, vup_t,
    tok, landed, scaled, narrow, gated, rim, wide, conv, sq_mine, sq_other,
    lat_ref, q2, kn, kr, vt, run_max, acc, s_ref, att_t, end_mine, end_other,
    att_sq, att_sq_other, att_act, conv_act, out_stage,
    w_sem, w_send, w_recv, tok_load, tok_send, tok_recv, rim_send, rim_recv, sq_send, sq_recv,
    csq_send, csq_recv, asq_send, asq_recv, conv_send, conv_recv, att_send, att_recv,
    col_send, down_send, plane_send, core_send, link_recv, core_recv, out_sem,
    q_help, help_out, help_in, qh_send, qh_recv, help_send, help_recv,
):
    mine = lax.axis_index("tp")
    me = lax.axis_index("sp")
    seats = lax.axis_size("sp")
    rows, width = tok.shape
    blocks = lat_ref.shape[0]
    rank = kvd.shape[1]
    layers = blocks // PLANE
    layer = me // PLANE
    spot = me % PLANE
    height = lat_ref.shape[1] // 2
    half = pl.ds(pl.multiple_of(mine * height, 16), height)
    other = other_core()
    ahead = {"sp": (me + 1) % seats, "tp": mine}
    behind = {"sp": (me + seats - 1) % seats, "tp": mine}

    def columns(owner):
        return pl.ds(pl.multiple_of(owner * width, 128), width)

    loads = [
        pltpu.make_async_copy(src, dst, w_sem.at[index])
        for index, (src, dst) in enumerate(
            (
                (kvd_hbm, kvd), (rotw_hbm, rotw), (cgw_hbm, cgw), (cvw_hbm, cvw),
                (qw_hbm, qw), (qrw_hbm, qrw), (kup_hbm, kup), (vup_hbm, vup),
                (att_hbm.at[:, columns(mine)], att_w.at[0]),
                (conv_hbm.at[:, columns(mine)], conv_w.at[0]),
            )
        )
    ]
    fetch = pltpu.make_async_copy(tok_hbm, tok, tok_load)
    fetch.start()
    for load in loads[:2]:
        load.start()
    gifts = [
        push(src.at[:, columns(1 - mine)], dst.at[1], w_send.at[index], w_recv.at[index], other)
        for index, (src, dst) in enumerate(((att_hbm, att_w), (conv_hbm, conv_w)))
    ]

    def spot_at(distance):
        return (spot + distance) % PLANE

    def at(layer_id, spot_id):
        return {"sp": layer_id * PLANE + spot_id, "tp": mine}

    q_help[...] = jnp.zeros(q_help.shape, jnp.bfloat16)
    barrier = pltpu.get_barrier_semaphore()
    peers = [at(layer, spot_at(d)) for d in range(1, PLANE)] + [other]
    for peer in peers:
        pl.semaphore_signal(barrier, inc=1, device_id=peer, device_id_type=MESH)
    above = at(jnp.minimum(layer + 1, layers - 1), spot)
    below = at(jnp.maximum(layer - 1, 0), spot)
    top_layer = layers - 1
    opposite = at(top_layer - layer, spot)
    outer = jnp.where((layer == 0) | (layer == top_layer), 1, 0)
    for condition, peer in (
        (outer == 1, opposite), (layer < layers - 1, above), (layer > 0, below), (me < seats - 1, ahead), (me > 0, behind),
    ):

        @pl.when(condition)
        def _(peer=peer):
            pl.semaphore_signal(barrier, inc=1, device_id=peer, device_id_type=MESH)

    pairs, _, both = q2.shape
    keys_wide = kn.shape[1]
    q2[...] = jnp.zeros(q2.shape, jnp.bfloat16)
    ones_low = VALUE_DIM
    ones_high = vt.shape[2] - VALUE_DIM
    vt[:, :, ones_low:ones_high, :] = jnp.ones(
        (2, pairs, ones_high - ones_low, keys_wide), jnp.bfloat16
    )
    pl.semaphore_wait(
        barrier,
        len(peers)
        + jnp.minimum(me, 1)
        + jnp.minimum(seats - 1 - me, 1)
        + jnp.minimum(layer, 1)
        + jnp.minimum(layers - 1 - layer, 1)
        + outer,
    )
    fetch.wait()
    tok_copy = push(tok, landed, tok_send, tok_recv, other)
    tok_copy.start()
    for load in loads[2:]:
        load.start()

    def place(block, index):
        cols = pl.ds(pl.multiple_of(index * width, 128), width)
        full = block[...].astype(jnp.float32)
        scaled[:, cols] = (full * gain_ref[:, cols]).astype(jnp.bfloat16)
        return jnp.sum(full * full, axis=1, keepdims=True)

    squares = place(tok, mine)
    column = lax.broadcasted_iota(jnp.int32, seat_ref.shape, 1)
    seat_turn = jnp.sum(
        jnp.where(column == me, seat_ref[...], 0.0), axis=1, keepdims=True
    )
    turn = ROT_DIM // 2
    seat_cos, seat_sin = seat_turn[:turn], seat_turn[turn:]
    base_cos, base_sin = base_ref[:turn], base_ref[turn:]
    cos_table = seat_cos * base_cos - seat_sin * base_sin
    sin_table = seat_sin * base_cos + seat_cos * base_sin

    def rotate(block):
        front = block[:turn]
        back = block[turn : 2 * turn]
        return jnp.concatenate(
            [front * cos_table - back * sin_table, back * cos_table + front * sin_table], axis=0
        )

    tok_copy.wait()
    squares = squares + place(landed, 1 - mine)
    row_scale = lax.rsqrt(squares / (2 * width) + norm_eps)

    def project(weight):
        return jnp.dot(scaled[...], weight[...], preferred_element_type=jnp.float32)

    loads[0].wait()
    loads[1].wait()
    raw = project(kvd)
    latent = (
        raw
        * lax.rsqrt(jnp.mean(raw * raw, axis=1, keepdims=True) + norm_eps)
        * kv_gain_ref[...]
    )
    lat_ref[me, :rows, :] = latent.astype(jnp.bfloat16)
    narrow[...] = jnp.broadcast_to(row_scale, narrow.shape)
    key_turn = lax.dot_general(
        rotw[...], scaled[...], (((1,), (1,)), ((), ())), preferred_element_type=jnp.float32
    )
    key_rot = rotate(key_turn * narrow[...].T[:ROT_DIM]).astype(jnp.bfloat16)
    across = rank // 128
    for piece in range(across * ((rows // 128 + across - 1) // across)):
        band = rows + piece // across * ROT_DIM
        lanes = slice(piece % across * 128, piece % across * 128 + 128)
        lat_ref[me, band : band + ROT_DIM, lanes] = (
            key_rot[:, piece * 128 : piece * 128 + 128]
            if piece < rows // 128
            else jnp.zeros((ROT_DIM, 128), jnp.bfloat16)
        )

    def column_copy(block):
        spread = lat_ref.at[block, half]
        return push(spread, spread, col_send.at[block // PLANE], link_recv.at[block], above)

    def down_copy(block):
        spread = lat_ref.at[block, half]
        return push(spread, spread, down_send.at[block // PLANE], link_recv.at[block], below)

    def rise(block):
        @pl.when(layer + 1 < layers)
        def _():
            column_copy(block).start()

    def plane_copy(block, distance):
        return push(
            lat_ref.at[block, half],
            lat_ref.at[block, half],
            plane_send.at[block // PLANE, distance - 1],
            link_recv.at[block],
            at(layer, spot_at(distance)),
        )

    def core_copy(block):
        spread = lat_ref.at[block, half]
        return push(spread, spread, core_send.at[block], core_recv.at[block], other)

    rise(me)

    @pl.when(layer > 0)
    def _():
        down_copy(me).start()

    for d in range(1, PLANE):
        plane_copy(me, d).start()
    for gift in gifts:
        gift.start()

    def arrive(block):
        spread = lat_ref.at[block, half]
        push(spread, spread, core_send.at[block], link_recv.at[block], other).wait_recv()

    def spread_layer(which, upward):
        block = which * PLANE + spot
        arrive(block)
        if upward:
            rise(block)
        for d in range(1, PLANE):
            plane_copy(block, d).start()
        core_copy(block).start()

    def hand_layer(which):
        for d in range(1, PLANE):
            block = which * PLANE + spot_at(d)
            arrive(block)
            core_copy(block).start()

    def relay(step):
        @pl.when(step <= layer)
        def _():
            spread_layer(layer - step, True)

    def hand_over(step):
        @pl.when(step <= layer)
        def _():
            hand_layer(layer - step)

    def descend(distance):
        @pl.when((layer > 0) & (layer + distance < layers))
        def _():
            block = (layer + distance) * PLANE + spot
            arrive(block)
            down_copy(block).start()

        @pl.when((layer == 0) & (distance < layers))
        def _():
            spread_layer(distance, False)

    loads[2].wait()
    loads[3].wait()
    gate = project(cgw) * row_scale
    gated[...] = (project(cvw) * row_scale * jax.nn.sigmoid(gate)).astype(jnp.bfloat16)
    edge = rim.shape[0]
    rim_copy = push(gated.at[pl.ds(rows - edge, edge)], rim, rim_send, rim_recv, ahead)

    @pl.when(me < seats - 1)
    def _():
        rim_copy.start()

    loads[4].wait()
    loads[5].wait()
    query_scale = row_scale * (math.log2(math.e) / math.sqrt(NOPE_DIM + ROT_DIM))
    plain = (project(qw) * query_scale).T.astype(jnp.bfloat16)
    turned = (project(qrw) * query_scale).T
    for head in range(2 * pairs):
        side = head % 2
        cols = slice(side * rows, (side + 1) * rows)
        q2[head // 2, side * NOPE_DIM : (side + 1) * NOPE_DIM, cols] = plain[
            head * NOPE_DIM : (head + 1) * NOPE_DIM
        ]
        q2[head // 2, 2 * NOPE_DIM : 2 * NOPE_DIM + ROT_DIM, cols] = rotate(
            turned[head * ROT_DIM : (head + 1) * ROT_DIM]
        ).astype(jnp.bfloat16)

    lent = pairs - 1
    q_parts = tuple(
        (pl.ds(low, count), pl.ds(first_col, cols))
        for low, count, first_col, cols in (
            (0, NOPE_DIM, 0, rows),
            (NOPE_DIM, NOPE_DIM, rows, rows),
            (2 * NOPE_DIM, ROT_DIM, 0, 2 * rows),
        )
    )
    q_copies = [
        push(
            q2.at[lent, part_rows, part_cols],
            q_help.at[part_rows, part_cols],
            qh_send.at[index],
            qh_recv.at[index],
            opposite,
        )
        for index, (part_rows, part_cols) in enumerate(q_parts)
    ]

    @pl.when(layer == top_layer)
    def _():
        for copy in q_copies:
            copy.start()

    loads[7].wait()
    vup_t[...] = vup[...].astype(jnp.float32).T.astype(jnp.bfloat16)

    taps = taps_ref.shape[0]
    chunk = 64

    def band_step(step, carry, slab):
        cols = slice(slab * 128, (slab + 1) * 128)
        coeff = taps_ref[:, cols]
        base = step * chunk
        total = jnp.zeros((chunk, 128), jnp.float32)
        for tap in range(taps):
            total = total + coeff[tap : tap + 1, :] * wide[
                slab, pl.ds(base + (edge - taps + 1 + tap), chunk), :
            ]
        conv[pl.ds(pl.multiple_of(base, chunk), chunk), cols] = total
        return carry

    slabs = conv.shape[1] // 128
    for slab in range(slabs):
        wide[slab, edge:, :] = gated[:, slab * 128 : (slab + 1) * 128].astype(jnp.float32)
        lax.fori_loop(1, rows // chunk, functools.partial(band_step, slab=slab), 0)
        if slab == slabs // 2:
            relay(1)
            descend(1)
    hand_over(0)

    @pl.when(me > 0)
    def _():
        rim_copy.wait_recv()

    @pl.when(me == 0)
    def _():
        rim[...] = jnp.zeros(rim.shape, jnp.bfloat16)

    for slab in range(slabs):
        wide[slab, :edge, :] = rim[:, slab * 128 : (slab + 1) * 128].astype(jnp.float32)
        band_step(0, 0, slab)

    values = conv[...]
    for slot, total in enumerate((values, values * values)):
        sq_mine[:, slot * 128 : (slot + 1) * 128] = jnp.broadcast_to(
            jnp.sum(total, axis=1, keepdims=True), (rows, 128)
        )
    sums = push(sq_mine, sq_other, sq_send, sq_recv, other)
    sums.start()

    def activate():
        sums.wait()
        values = conv[...]
        moments = (sq_mine[...] + sq_other[...]) / CONV_CH
        mean_val = moments[:, :1]
        spread_val = moments[:, 128:129] - mean_val * mean_val
        normed = (values - mean_val) * lax.rsqrt(spread_val + norm_eps)
        swished = jax.nn.silu(normed * ln_gain_ref[...] + ln_bias_ref[...])
        conv_act[0] = (swished * conv_gain_ref[...]).astype(jnp.bfloat16)
        end_mine[...] = jnp.broadcast_to(
            jnp.sum(swished * swished, axis=1, keepdims=True), (rows, 128)
        )
        conv_sum.start()
        conv_copy.start()

    conv_sum = push(end_mine, end_other, csq_send, csq_recv, other)
    conv_copy = push(conv_act.at[0], conv_act.at[1], conv_send, conv_recv, other)

    def gathered(step):
        for d in range(1, PLANE):
            core_copy((layer - step) * PLANE + spot_at(d)).wait_recv()

    strip = 256
    strips = keys_wide // strip

    def expand(group, slot, index, only=None):
        pieces = []
        low, left = index * strip, strip
        while left > 0:
            take = min(rows - low % rows, left)
            pieces.append(
                lat_ref[group * PLANE + low // rows, low % rows : low % rows + take, :]
            )
            low, left = low + take, left - take
        lat = pieces[0] if len(pieces) == 1 else jnp.concatenate(pieces, axis=0)
        cut = slice(index * strip, (index + 1) * strip)
        some = range(pairs) if only is None else range(only, only + 1)
        key_cols = slice(2 * NOPE_DIM * some[0], 2 * NOPE_DIM * (some[-1] + 1))
        value_cols = slice(2 * VALUE_DIM * some[0], 2 * VALUE_DIM * (some[-1] + 1))
        kn[slot, cut, : 2 * NOPE_DIM * len(some)] = jnp.dot(
            lat, kup[:, key_cols], preferred_element_type=jnp.float32
        ).astype(jnp.bfloat16)
        values = lax.dot_general(
            vup_t[value_cols, :],
            lat,
            (((1,), (1,)), ((), ())),
            preferred_element_type=jnp.float32,
        ).astype(jnp.bfloat16)
        for pair in range(len(some)):
            low = 2 * VALUE_DIM * pair
            vt[slot, pair, :ones_low, cut] = values[low : low + VALUE_DIM]
            vt[slot, pair, ones_high:, cut] = values[low + VALUE_DIM : low + 2 * VALUE_DIM]
        for blk in range(index, PLANE, strips):
            pieces = []
            for piece in range(rows // 128):
                band = rows + piece // across * ROT_DIM
                lanes = slice(piece % across * 128, piece % across * 128 + 128)
                pieces.append(lat_ref[group * PLANE + blk, band : band + ROT_DIM, lanes])
            rot = jnp.concatenate(pieces, axis=1).astype(jnp.float32)
            rot = jnp.concatenate([rot, jnp.zeros((128 - ROT_DIM, rows), jnp.float32)], axis=0)
            kr[slot, blk * rows : (blk + 1) * rows, :] = rot.T.astype(jnp.bfloat16)

    tiles = both // 256
    tile_rows = tuple(
        (
            0 if 256 * tile < rows else ones_low,
            ones_high if 256 * (tile + 1) <= rows else vt.shape[2],
        )
        for tile in range(tiles)
    )

    def hidden_keys(first_key, first_query):
        key = first_key + lax.broadcasted_iota(jnp.int32, (strip, both), 0)
        query = lax.broadcasted_iota(jnp.int32, (strip, both), 1)
        return key > first_query + jnp.where(query >= rows, query - rows, query)

    def weigh(slot, place_id, index, weights, sums):
        cut = slice(index * strip, (index + 1) * strip)
        for tile, (low, high) in enumerate(tile_rows):
            new = jnp.dot(
                vt[slot, place_id, low:high, cut],
                weights[:, 256 * tile : 256 * (tile + 1)],
                preferred_element_type=jnp.float32,
            )
            sums[tile] = new if sums[tile] is None else sums[tile] + new

    def attend(slot, first, hidden, middle, following):
        def score(pair, index):
            cut = slice(index * strip, (index + 1) * strip)
            keys = jnp.concatenate(
                [kn[slot, cut, 128 * pair : 128 * pair + 128], kr[slot, cut, :]], axis=1
            )
            scores = jnp.dot(keys, q2[pair], preferred_element_type=jnp.float32)
            if hidden is not None:
                scores = jnp.where(hidden(index), far_below, scores)
            s_ref[pair % 2, cut, :] = scores
            return jnp.max(scores, axis=0, keepdims=True)

        def settle_top(pair, tops):
            top = functools.reduce(jnp.maximum, tops)
            fade = None
            if not first:
                old = run_max[pair : pair + 1, :]
                top = jnp.maximum(old, top)
                fade = jnp.exp2(old - top)
            run_max[pair : pair + 1, :] = top
            return top, fade

        def weights_of(pair, index, top):
            cut = slice(index * strip, (index + 1) * strip)
            return jnp.exp2(s_ref[pair % 2, cut, :] - top).astype(jnp.bfloat16)

        def close(pair, sums, fade):
            for tile, (low, high) in enumerate(tile_rows):
                new = sums[tile]
                if not first:
                    new = new + acc[pair, tile, : high - low, :] * fade[
                        :, 256 * tile : 256 * (tile + 1)
                    ]
                acc[pair, tile, : high - low, :] = new

        tops = [score(0, index) for index in range(strips)]
        for pair in range(lent):
            middle(pair)
            top, fade = settle_top(pair, tops)
            tops = []
            sums = [None] * tiles
            for index in range(strips):
                if pair + 1 < lent:
                    tops.append(score(pair + 1, index))
                weigh(slot, pair, index, weights_of(pair, index, top), sums)
                if pair + 1 == lent and following is not None:
                    expand(following, 1 - slot, index)
            close(pair, sums, fade)

        @pl.when(layer < top_layer)
        def _():
            top, fade = settle_top(lent, [score(lent, index) for index in range(strips)])
            sums = [None] * tiles
            for index in range(strips):
                weigh(slot, lent, index, weights_of(lent, index, top), sums)
            close(lent, sums, fade)

    def hidden(index):
        return hidden_keys(layer * keys_wide + index * strip, me * rows)

    loads[6].wait()
    gathered(0)
    for index in range(strips):
        expand(layer, 0, index)
    for distance in range(2, layers):

        @pl.when(layer > 0)
        def _(distance=distance):
            descend(distance)


    def ready_layer(which):
        for d in range(PLANE):
            core_copy(which * PLANE + spot_at(d)).wait_recv()

    def ready(step):
        @pl.when(step <= layer)
        def _():
            ready_layer(layer - step)

    def first_middle(pair):
        if pair == 1:
            relay(2)
            hand_over(1)

            @pl.when(layer == 0)
            def _():
                descend(2)

            activate()
        if pair == lent - 1:
            ready(1)

    attend(0, True, hidden, first_middle, jnp.maximum(layer - 1, 0))

    def far(step, carry):
        def middle(pair):
            if pair == 1:
                relay(step + 2)
                hand_over(step + 1)
            if pair == lent - 1:
                ready(step + 1)

        attend(step % 2, False, None, middle, layer - step - 1)
        return carry

    lax.fori_loop(1, layer, far, 0)

    @pl.when(layer > 0)
    def _():
        attend(layer % 2, False, None, lambda pair: None, None)

    def finish(pair, keep):
        for side in range(2):
            pieces = []
            for tile, (low, high) in enumerate(tile_rows):
                start = max(side * rows, 256 * tile)
                stop = min((side + 1) * rows, 256 * (tile + 1))
                if start >= stop:
                    continue
                total = acc[pair, tile, : high - low, start - 256 * tile : stop - 256 * tile]
                base = 0 if side == 0 else ones_high - low
                pieces.append(
                    total[base : base + VALUE_DIM] / total[ones_low - low : ones_low - low + 1]
                )
            keep(side, jnp.concatenate(pieces, axis=1).astype(jnp.bfloat16))

    def keep_local(pair):
        def keep(side, block):
            low = (2 * pair + side) * VALUE_DIM
            att_t[low : low + VALUE_DIM, :] = block.astype(jnp.float32)

        return keep

    for pair in range(lent):
        finish(pair, keep_local(pair))

    @pl.when(layer < top_layer)
    def _():
        finish(lent, keep_local(lent))

    help_copy = push(help_out, help_in, help_send, help_recv, opposite)

    @pl.when(layer == 0)
    def _():
        for distance in range(3, layers):
            descend(distance)
        for copy in q_copies:
            copy.wait_recv()
        run_max[0:1, :] = jnp.full((1, both), far_below, jnp.float32)
        acc[0] = jnp.zeros(acc.shape[1:], jnp.float32)
        guest = top_layer * PLANE + spot

        def lend(which, carry):
            @pl.when(which + 1 < layers)
            def _():
                hand_layer(which + 1)

            @pl.when(which > 0)
            def _():
                ready_layer(which)

            tops = []
            for index in range(strips):
                expand(which, 0, index, lent)
            for index in range(strips):
                cut = slice(index * strip, (index + 1) * strip)
                keys = jnp.concatenate([kn[0, cut, :128], kr[0, cut, :]], axis=1)
                scores = jnp.dot(keys, q_help[...], preferred_element_type=jnp.float32)
                scores = jnp.where(
                    hidden_keys(which * keys_wide + index * strip, guest * rows), far_below, scores
                )
                s_ref[0, cut, :] = scores
                tops.append(jnp.max(scores, axis=0, keepdims=True))
            old = run_max[0:1, :]
            top = jnp.maximum(old, functools.reduce(jnp.maximum, tops))
            fade = jnp.exp2(old - top)
            run_max[0:1, :] = top
            sums = [None] * tiles
            for index in range(strips):
                cut = slice(index * strip, (index + 1) * strip)
                weights = jnp.exp2(s_ref[0, cut, :] - top).astype(jnp.bfloat16)
                weigh(0, 0, index, weights, sums)
            for tile, (low, high) in enumerate(tile_rows):
                acc[0, tile, : high - low, :] = sums[tile] + acc[0, tile, : high - low, :] * fade[
                    :, 256 * tile : 256 * (tile + 1)
                ]
            return carry

        lax.fori_loop(0, layers, lend, 0)

        def keep(side, block):
            help_out[side * VALUE_DIM : (side + 1) * VALUE_DIM, :] = block

        finish(0, keep)
        help_copy.start()

    @pl.when(layer == top_layer)
    def _():
        help_copy.wait_recv()
        low = 2 * lent * VALUE_DIM
        att_t[low : low + 2 * VALUE_DIM, :] = help_in[...].astype(jnp.float32)

    attended = att_t[...]
    att_sq[...] = jnp.broadcast_to(
        jnp.sum(attended * attended, axis=0, keepdims=True), att_sq.shape
    )
    att_act[0] = (attended.T * att_gain_ref[...]).astype(jnp.bfloat16)
    att_sum = push(att_sq, att_sq_other, asq_send, asq_recv, other)
    att_sum.start()
    att_copy = push(att_act.at[0], att_act.at[1], att_send, att_recv, other)
    att_copy.start()
    for index in (8, 9):
        loads[index].wait()
    for gift in gifts:
        gift.wait()
    conv_sum.wait()
    conv_copy.wait()
    conv_scale = lax.rsqrt((end_mine[...] + end_other[...])[:, :1] / CONV_CH + norm_eps)

    def product(activations, weight):
        return jnp.dot(activations, weight, preferred_element_type=jnp.float32)

    base_part = (
        product(conv_act[0], conv_w[0]) + product(conv_act[1], conv_w[1])
    ) * conv_scale
    own_part = product(att_act[0], att_w[0])
    att_sum.wait()
    squares_t = jnp.broadcast_to(att_sq[:1] + att_sq_other[:1], (128, rows)).T
    att_scale = lax.rsqrt(squares_t[:, :1] / ATT_WIDTH + norm_eps)
    att_copy.wait()
    leaves = []
    for index in range(width // 256):
        cols = slice(index * 256, (index + 1) * 256)
        out_stage[:, cols] = (
            (own_part[:, cols] + product(att_act[1], att_w[1, :, cols])) * att_scale
            + base_part[:, cols]
        ).astype(jnp.bfloat16)
        leave = pltpu.make_async_copy(
            out_stage.at[:, cols], out_ref.at[:, cols], out_sem.at[index]
        )
        leave.start()
        leaves.append(leave)

    @pl.when(me < seats - 1)
    def _():
        rim_copy.wait_send()

    def settle(step, carry):
        base = (layer - step) * PLANE
        for d in range(1, PLANE):
            plane_copy(base + spot, d).wait_send()
            core_copy(base + spot_at(d)).wait_send()

        @pl.when(layer + 1 < layers)
        def _():
            column_copy(base + spot).wait_send()

        @pl.when(step > 0)
        def _():
            core_copy(base + spot).wait_send()

        return carry

    lax.fori_loop(0, layer + 1, settle, 0)

    def settle_down(which, carry):
        down_copy(which * PLANE + spot).wait_send()
        return carry

    @pl.when(layer > 0)
    def _():
        lax.fori_loop(layer, layers, settle_down, 0)

    def settle_guest(which, carry):
        for d in range(1, PLANE):
            plane_copy(which * PLANE + spot, d).wait_send()
        for d in range(PLANE):
            core_copy(which * PLANE + spot_at(d)).wait_send()
        return carry

    @pl.when(layer == 0)
    def _():
        lax.fori_loop(1, layers, settle_guest, 0)
        help_copy.wait_send()

    @pl.when(layer == top_layer)
    def _():
        for copy in q_copies:
            copy.wait_send()

    for leave in leaves:
        leave.wait()


def angle_tables(seats, rows):
    frequency = rope_base ** (-np.arange(ROT_DIM // 2) / (ROT_DIM // 2))

    def table(positions):
        angles = frequency[:, None] * positions[None, :]
        return jnp.asarray(
            np.concatenate([np.cos(angles), np.sin(angles)], axis=0), jnp.float32
        )

    return table(np.arange(rows)), table(rows * np.arange(-(-seats // 128) * 128))


def fused(tokens, gains, matrices, taps, seats):
    rows, width = tokens.shape
    chans = taps.shape[1]
    rank = matrices[0].shape[1]
    heads = matrices[4].shape[1] // NOPE_DIM
    pairs = heads // 2
    keys_wide = PLANE * rows
    layers = seats // PLANE
    across = rank // 128
    height = rows + -(-(rows // 128) // across) * ROT_DIM
    vmem = pl.BlockSpec(memory_space=pltpu.VMEM)
    anywhere = pl.BlockSpec(memory_space=pltpu.HBM)
    dma = pltpu.SemaphoreType.DMA
    edge = 32
    bf16 = jnp.bfloat16
    f32 = jnp.float32
    value_rows = 2 * VALUE_DIM + 16
    base, seat = angle_tables(seats, rows)
    input_gain, kv_gain, ln_gain, ln_bias, att_gain, conv_gain = gains
    return pl.pallas_call(
        layer_kernel,
        out_shape=jax.ShapeDtypeStruct((rows, width), bf16),
        in_specs=[anywhere] + [vmem] * 9 + [anywhere] * 10,
        out_specs=anywhere,
        scratch_shapes=[pltpu.VMEM(matrix.shape, bf16) for matrix in matrices[:8]]
        + [
            pltpu.VMEM((2, matrix.shape[0], width), bf16) for matrix in matrices[8:]
        ]
        + [
            pltpu.VMEM(matrices[7].shape[::-1], bf16),
            pltpu.VMEM((rows, width), bf16),
            pltpu.VMEM((rows, width), bf16),
            pltpu.VMEM((rows, 2 * width), bf16),
            pltpu.VMEM((rows, 128), f32),
            pltpu.VMEM((rows, chans), bf16),
            pltpu.VMEM((edge, chans), bf16),
            pltpu.VMEM((chans // 128, rows + edge, 128), f32),
            pltpu.VMEM((rows, chans), f32),
            pltpu.VMEM((rows, 256), f32),
            pltpu.VMEM((rows, 256), f32),
            pltpu.VMEM((seats, height, rank), bf16),
            pltpu.VMEM((pairs, 256, 2 * rows), bf16),
            pltpu.VMEM((2, keys_wide, heads * NOPE_DIM), bf16),
            pltpu.VMEM((2, keys_wide, 128), bf16),
            pltpu.VMEM((2, pairs, value_rows, keys_wide), bf16),
            pltpu.VMEM((max(pairs, 8), 2 * rows), f32),
            pltpu.VMEM((pairs, 2 * rows // 256, value_rows, 256), f32),
            pltpu.VMEM((2, keys_wide, 2 * rows), f32),
            pltpu.VMEM((heads * VALUE_DIM, rows), f32),
            pltpu.VMEM((rows, 128), f32),
            pltpu.VMEM((rows, 128), f32),
            pltpu.VMEM((8, rows), f32),
            pltpu.VMEM((8, rows), f32),
            pltpu.VMEM((2, rows, heads * VALUE_DIM), bf16),
            pltpu.VMEM((2, rows, chans), bf16),
            pltpu.VMEM((rows, width), bf16),
            dma((len(matrices),)),
            dma((2,)),
            dma((2,)),
        ]
        + [dma] * 15
        + [
            dma((layers,)),
            dma((layers,)),
            dma((layers, PLANE - 1)),
            dma((seats,)),
            dma((seats,)),
            dma((seats,)),
            dma((width // 256,)),
            pltpu.VMEM((256, 2 * rows), bf16),
            pltpu.VMEM((2 * VALUE_DIM, rows), bf16),
            pltpu.VMEM((2 * VALUE_DIM, rows), bf16),
            dma((3,)),
            dma((3,)),
            dma,
            dma,
        ],
        compiler_params=pltpu.CompilerParams(
            vmem_limit_bytes=60 << 20, collective_id=0, has_side_effects=True
        ),
        name="layer",
    )(tokens, input_gain, kv_gain, base, seat, taps, ln_gain, ln_bias, att_gain, conv_gain, *matrices)


def gathered_kernel(q_ref, lat_ref, kup_ref, vup_ref, o_ref, kt, vt, run_max, acc):
    heads, rows, lanes = q_ref.shape
    blocks = lat_ref.shape[0]
    rank = kup_ref.shape[1]
    nope = kup_ref.shape[0] // heads
    vdim = vup_ref.shape[0] // heads
    rot = lat_ref.shape[1] - rank
    wide = kt.shape[2]
    group = wide // rows
    me = lax.axis_index("sp")
    last = me // group
    kt[:, nope + rot :, :] = jnp.zeros((heads, lanes - nope - rot, wide), jnp.bfloat16)
    vt[:, vdim:, :] = jnp.ones((heads, lanes - vdim, wide), jnp.bfloat16)

    def expand(block):
        for part in range(group):
            src = jnp.minimum(block * group + part, blocks - 1)
            lat = lat_ref[src, :rank, :]
            turned = lat_ref[src, rank:, :]
            cols = slice(part * rows, (part + 1) * rows)
            keys = jnp.dot(kup_ref[...], lat, preferred_element_type=jnp.float32)
            values = jnp.dot(vup_ref[...], lat, preferred_element_type=jnp.float32)
            for head in range(heads):
                kt[head, :nope, cols] = keys[head * nope : (head + 1) * nope].astype(jnp.bfloat16)
                kt[head, nope : nope + rot, cols] = turned
                vt[head, :vdim, cols] = values[head * vdim : (head + 1) * vdim].astype(
                    jnp.bfloat16
                )

    def weigh(head, scores, top):
        weights = jnp.exp2(scores - top).astype(jnp.bfloat16)
        return lax.dot_general(
            weights, vt[head], (((1,), (1,)), ((), ())), preferred_element_type=jnp.float32
        )

    expand(last)
    key_pos = last * wide + lax.broadcasted_iota(jnp.int32, (rows, wide), 1)
    query_pos = me * rows + lax.broadcasted_iota(jnp.int32, (rows, wide), 0)
    hidden = key_pos > query_pos
    for head in range(heads):
        scores = jnp.dot(q_ref[head], kt[head], preferred_element_type=jnp.float32)
        scores = jnp.where(hidden, far_below, scores)
        top = jnp.max(scores, axis=1, keepdims=True)
        run_max[head] = jnp.broadcast_to(top, (rows, lanes))
        acc[head] = weigh(head, scores, top)

    def visit(step, carry):
        expand(step)
        for head in range(heads):
            scores = jnp.dot(q_ref[head], kt[head], preferred_element_type=jnp.float32)
            old = run_max[head]
            top = jnp.maximum(old[:, :1], jnp.max(scores, axis=1, keepdims=True))
            wide_top = jnp.broadcast_to(top, (rows, lanes))
            run_max[head] = wide_top
            acc[head] = acc[head] * jnp.exp2(old - wide_top) + weigh(head, scores, top)
        return carry

    lax.fori_loop(0, last, visit, 0)
    lane = lax.broadcasted_iota(jnp.int32, (rows, lanes), 1)
    for pair in range(heads // 2):
        halves = []
        for head in (2 * pair, 2 * pair + 1):
            total = acc[head]
            halves.append(total / pltpu.roll(total, vdim, axis=1))
        both = jnp.where(lane < vdim, halves[0], pltpu.roll(halves[1], vdim, axis=1))
        o_ref[:, pair * lanes : (pair + 1) * lanes] = both.astype(jnp.bfloat16)


def gathered_attention(q_heads, lat_all, key_up_t, value_up_t):
    heads, rows, lanes = q_heads.shape
    blocks = lat_all.shape[0]
    wide = 2 * rows if blocks % 2 == 0 else rows
    vmem = pl.BlockSpec(memory_space=pltpu.VMEM)
    return pl.pallas_call(
        gathered_kernel,
        out_shape=jax.ShapeDtypeStruct((rows, value_up_t.shape[0]), jnp.bfloat16),
        in_specs=[vmem] * 4,
        out_specs=vmem,
        scratch_shapes=[
            pltpu.VMEM((heads, lanes, wide), jnp.bfloat16),
            pltpu.VMEM((heads, lanes, wide), jnp.bfloat16),
            pltpu.VMEM((heads, rows, lanes), jnp.float32),
            pltpu.VMEM((heads, rows, lanes), jnp.float32),
        ],
        compiler_params=pltpu.CompilerParams(vmem_limit_bytes=48 << 20),
        cost_estimate=pl.CostEstimate(
            flops=20_000_000_000, bytes_accessed=8 << 20, transcendentals=20_000_000
        ),
        name="gathered_attention",
    )(q_heads, lat_all, key_up_t, value_up_t)


def conv_kernel(gated_ref, rim_ref, taps_ref, out_ref, wide):
    rows, chans = gated_ref.shape
    rim = rim_ref.shape[0]
    taps = taps_ref.shape[0]
    chunk = 64
    for part in range(chans // 128):
        cols = slice(part * 128, (part + 1) * 128)
        wide[part, :rim, :] = rim_ref[:, cols].astype(jnp.float32)
        wide[part, rim:, :] = gated_ref[:, cols].astype(jnp.float32)
        coeff = taps_ref[:, cols]

        def band(step, carry):
            base = step * chunk
            total = jnp.zeros((chunk, 128), jnp.float32)
            for tap in range(taps):
                total = total + coeff[tap : tap + 1, :] * wide[
                    part, pl.ds(base + (rim - taps + 1 + tap), chunk), :
                ]
            out_ref[pl.ds(pl.multiple_of(base, chunk), chunk), cols] = total
            return carry

        lax.fori_loop(0, rows // chunk, band, 0)


def convolve(gated, rim, taps):
    rows, chans = gated.shape
    vmem = pl.BlockSpec(memory_space=pltpu.VMEM)
    return pl.pallas_call(
        conv_kernel,
        out_shape=jax.ShapeDtypeStruct((rows, chans), jnp.float32),
        in_specs=[vmem] * 3,
        out_specs=vmem,
        scratch_shapes=[pltpu.VMEM((chans // 128, rows + rim.shape[0], 128), jnp.float32)],
        cost_estimate=pl.CostEstimate(
            flops=2 * rows * chans * 31, bytes_accessed=2 << 20, transcendentals=0
        ),
        name="depthwise",
    )(gated, rim, taps)


def shards(
    tokens,
    input_gain,
    query_weight,
    query_rot_weight,
    kv_down,
    rot_down,
    kv_gain,
    key_up,
    value_up,
    conv_value_weight,
    conv_gate_weight,
    conv_taps,
    conv_ln_gain,
    conv_ln_bias,
    att_out_gain,
    conv_out_gain,
    att_out_weight,
    conv_out_weight,
):
    tok_rows = tokens.shape[0]
    heads_here = key_up.shape[1] // NOPE_DIM
    chan_here = conv_taps.shape[1]
    weight_list = (
        query_weight,
        query_rot_weight,
        kv_down,
        rot_down,
        conv_value_weight,
        conv_gate_weight,
    )
    seats = lax.axis_size("sp")
    if (
        lax.axis_size("tp") == 2
        and seats % PLANE == 0
        and tok_rows % 128 == 0
        and heads_here % 2 == 0
        and heads_here > 2
        and seats > PLANE
    ):
        gains = (
            input_gain, kv_gain, conv_ln_gain, conv_ln_bias, att_out_gain, conv_out_gain
        )
        return fused(
            tokens,
            tuple(gain[None, :] for gain in gains),
            (
                kv_down, rot_down.T, conv_gate_weight, conv_value_weight, query_weight,
                query_rot_weight, key_up, value_up, att_out_weight, conv_out_weight,
            ),
            conv_taps,
            seats,
        )
    whole_rows = lax.all_gather(tokens, "tp", axis=1, tiled=True).astype(jnp.float32)
    scaled = (whole_rows * input_gain[None, :]).astype(jnp.bfloat16)
    row_scale = lax.rsqrt(jnp.mean(whole_rows * whole_rows, axis=1, keepdims=True) + norm_eps)

    def add_product(weight):
        return jnp.dot(scaled, weight, preferred_element_type=jnp.float32)

    summed = tuple((add_product(weight) for weight in weight_list))
    q_acc, qrot_acc, latent_raw, rot_acc, value_acc, gate_acc = summed
    positions = lax.axis_index("sp") * tok_rows + jnp.arange(tok_rows, dtype=jnp.int32)
    cos_table, sine_table = rotary_tables(positions, ROT_DIM // 2)
    fold = math.log2(math.e) / math.sqrt(NOPE_DIM + ROT_DIM)
    query_scale = row_scale * fold
    plain_q = (q_acc * query_scale).reshape(tok_rows, heads_here, NOPE_DIM)
    turned_q = rotate_half(
        (qrot_acc * query_scale).reshape(tok_rows, heads_here, ROT_DIM),
        cos_table[:, None, :],
        sine_table[:, None, :],
    )
    blank = jnp.zeros((tok_rows, heads_here, 128 - NOPE_DIM - ROT_DIM), jnp.float32)
    q_heads = jnp.transpose(
        jnp.concatenate([plain_q, turned_q, blank], axis=2).astype(jnp.bfloat16), (1, 0, 2)
    )
    latent = (
        latent_raw
        * lax.rsqrt(jnp.mean(latent_raw * latent_raw, axis=1, keepdims=True) + norm_eps)
        * kv_gain[None, :]
    ).astype(jnp.bfloat16)
    key_rot = rotate_half(rot_acc * row_scale, cos_table, sine_table).astype(jnp.bfloat16)
    gated_input = (value_acc * row_scale * jax.nn.sigmoid(gate_acc * row_scale)).astype(
        jnp.bfloat16
    )
    packed = jnp.concatenate([latent.T, key_rot.T], axis=0)
    rim_rows = shifted(gated_input[tok_rows - (KERNEL + 1) :], "sp", 1)
    conv_out = convolve(gated_input, rim_rows, conv_taps)
    moment_one, moment_two = lax.psum(
        (jnp.sum(conv_out, axis=1), jnp.sum(conv_out * conv_out, axis=1)), "tp"
    )
    mean_val = moment_one / CONV_CH
    spread = moment_two / CONV_CH - mean_val * mean_val
    normed = (conv_out - mean_val[:, None]) * lax.rsqrt(spread + norm_eps)[:, None]
    swished = jax.nn.silu(normed * conv_ln_gain[None, :] + conv_ln_bias[None, :])
    lat_all = lax.all_gather(packed, "sp", axis=0)
    attended = gathered_attention(q_heads, lat_all, key_up.T, value_up.T).astype(jnp.float32)
    att_sq, conv_sq = lax.psum(
        (
            jnp.sum(attended * attended, axis=1, keepdims=True),
            jnp.sum(swished * swished, axis=1, keepdims=True),
        ),
        "tp",
    )
    att_mixed = (
        attended * lax.rsqrt(att_sq / ATT_WIDTH + norm_eps) * att_out_gain[None, :]
    ).astype(jnp.bfloat16)
    conv_mixed = (
        swished * lax.rsqrt(conv_sq / CONV_CH + norm_eps) * conv_out_gain[None, :]
    ).astype(jnp.bfloat16)
    share = (
        jnp.dot(att_mixed, att_out_weight, preferred_element_type=jnp.float32)
        + jnp.dot(conv_mixed, conv_out_weight, preferred_element_type=jnp.float32)
    ).astype(jnp.bfloat16)
    return lax.psum_scatter(share, "tp", scatter_dimension=1, tiled=True)


def solution(mesh):
    return jax.shard_map(
        shards,
        mesh=mesh,
        in_specs=(
            P("sp", "tp"),
            P(),
            P(None, "tp"),
            P(None, "tp"),
            P(),
            P(),
            P(),
            P(None, "tp"),
            P(None, "tp"),
            P(None, "tp"),
            P(None, "tp"),
            P(None, "tp"),
            P("tp"),
            P("tp"),
            P("tp"),
            P("tp"),
            P("tp", None),
            P("tp", None),
        ),
        out_specs=P("sp", "tp"),
        check_vma=False,
    )
```

```python
import functools
import math

import jax
import jax.numpy as jnp
import numpy as np
from jax import lax
from jax.experimental import pallas as pl
from jax.experimental.pallas import tpu as pltpu
from jax.sharding import PartitionSpec as P

D_MODEL = 2048
NOPE_DIM = 64
ROT_DIM = 32
VALUE_DIM = 64
CONV_CH = 1024
KERNEL = 31
ATT_WIDTH = 1024


norm_eps = 1e-06
far_below = -1e30
rope_base = 10000.0


def shifted(block, axis, distance):
    devices = range(lax.axis_size(axis))
    route = [(i - distance, i) for i in devices if i - distance in devices]
    return lax.ppermute(block, axis, route)


def rotary_tables(positions, half_dim):
    frequency = rope_base ** (-jnp.arange(half_dim, dtype=jnp.float32) / half_dim)
    angles = positions.astype(jnp.float32)[:, None] * frequency[None, :]
    return (jnp.cos(angles), jnp.sin(angles))


def rotate_half(values, cos_table, sine_table):
    half_dim = cos_table.shape[-1]
    front_half = values[..., :half_dim]
    back_half = values[..., half_dim:]
    return jnp.concatenate(
        [
            front_half * cos_table - back_half * sine_table,
            back_half * cos_table + front_half * sine_table,
        ],
        axis=-1,
    )


MESH = pl.DeviceIdType.MESH


def push(src, dst, send, recv, target):
    return pltpu.make_async_remote_copy(
        src_ref=src,
        dst_ref=dst,
        send_sem=send,
        recv_sem=recv,
        device_id=target,
        device_id_type=MESH,
    )


def other_core():
    return {"sp": lax.axis_index("sp"), "tp": 1 - lax.axis_index("tp")}


PLANE = 4


FAR_FIRST = (3, 1, 2)


def layer_kernel(
    tok_hbm, gain_ref, kv_gain_ref, base_ref, seat_ref, taps_ref, ln_gain_ref, ln_bias_ref,
    att_gain_ref, conv_gain_ref,
    kvd_hbm, rotw_hbm, cgw_hbm, cvw_hbm, qw_hbm, qrw_hbm, kup_hbm, vup_hbm, att_hbm, conv_hbm,
    out_ref,
    kvd, rotw, cgw, cvw, qw, qrw, kup, vup, att_w, conv_w, vup_t,
    tok, landed, scaled, own_raw, narrow, gated, rim, wide, conv, sq_mine, sq_other,
    lat_ref, q2, kn, kr, vt, run_max, acc, s_ref, att_t, end_mine, end_other,
    att_sq, att_sq_other, att_act, conv_act, out_stage, base_part, own_part,
    w_sem, w_send, w_recv, tok_load, tok_send, tok_recv, rim_send, rim_recv, sq_send, sq_recv,
    csq_send, csq_recv, asq_send, asq_recv, conv_send, conv_recv, att_send, att_recv,
    col_send, down_send, plane_send, core_send, link_recv, core_recv, out_sem,
    q_help, help_out, help_in, qh_send, qh_recv, help_send, help_recv,
):
    mine = lax.axis_index("tp")
    me = lax.axis_index("sp")
    seats = lax.axis_size("sp")
    rows, width = tok.shape
    blocks = lat_ref.shape[0]
    rank = kvd.shape[1]
    layers = blocks // PLANE
    layer = me // PLANE
    spot = me % PLANE
    height = lat_ref.shape[1] // 2
    half = pl.ds(pl.multiple_of(mine * height, 16), height)
    other = other_core()
    ahead = {"sp": (me + 1) % seats, "tp": mine}
    behind = {"sp": (me + seats - 1) % seats, "tp": mine}

    def columns(owner):
        return pl.ds(pl.multiple_of(owner * width, 128), width)

    loads = [
        pltpu.make_async_copy(src, dst, w_sem.at[index])
        for index, (src, dst) in enumerate(
            (
                (kvd_hbm, kvd), (rotw_hbm, rotw), (cgw_hbm, cgw), (cvw_hbm, cvw),
                (qw_hbm, qw), (qrw_hbm, qrw), (kup_hbm, kup), (vup_hbm, vup),
                (att_hbm.at[:, columns(mine)], att_w.at[0]),
                (conv_hbm.at[:, columns(mine)], conv_w.at[0]),
            )
        )
    ]
    fetch = pltpu.make_async_copy(tok_hbm, tok, tok_load)
    fetch.start()
    for load in loads[:2]:
        load.start()
    gifts = [
        push(src.at[:, columns(1 - mine)], dst.at[1], w_send.at[index], w_recv.at[index], other)
        for index, (src, dst) in enumerate(((att_hbm, att_w), (conv_hbm, conv_w)))
    ]

    def spot_at(step):
        return (spot % 2 + step % 2) % 2 + 2 * ((spot // 2 + step // 2) % 2)

    def at(layer_id, spot_id):
        return {"sp": layer_id * PLANE + spot_id, "tp": mine}

    q_help[...] = jnp.zeros(q_help.shape, jnp.bfloat16)
    barrier = pltpu.get_barrier_semaphore()
    peers = [at(layer, spot_at(d)) for d in range(1, PLANE)] + [other]
    for peer in peers:
        pl.semaphore_signal(barrier, inc=1, device_id=peer, device_id_type=MESH)
    above = at(jnp.minimum(layer + 1, layers - 1), spot)
    below = at(jnp.maximum(layer - 1, 0), spot)
    top_layer = layers - 1
    opposite = at(top_layer - layer, spot)
    root = at(0, spot)
    for condition, peer in [
        (layer == 0, at(other_layer, spot)) for other_layer in range(2, layers)
    ] + [
        (layer > 1, root), (layer < layers - 1, above), (layer > 0, below), (me < seats - 1, ahead), (me > 0, behind),
    ]:

        @pl.when(condition)
        def _(peer=peer):
            pl.semaphore_signal(barrier, inc=1, device_id=peer, device_id_type=MESH)

    pairs, _, both = q2.shape
    keys_wide = kn.shape[1]
    q2[...] = jnp.zeros(q2.shape, jnp.bfloat16)
    ones_low = VALUE_DIM
    ones_high = vt.shape[2] - VALUE_DIM
    vt[:, :, ones_low:ones_high, :] = jnp.ones(
        (2, pairs, ones_high - ones_low, keys_wide), jnp.bfloat16
    )
    pl.semaphore_wait(
        barrier,
        len(peers)
        + jnp.minimum(me, 1)
        + jnp.minimum(seats - 1 - me, 1)
        + jnp.minimum(layer, 1)
        + jnp.minimum(layers - 1 - layer, 1)
        + jnp.where(layer == 0, layers - 2, jnp.where(layer > 1, 1, 0)),
    )
    fetch.wait()
    tok_copy = push(tok, landed, tok_send, tok_recv, other)
    tok_copy.start()
    for load in loads[2:]:
        load.start()

    def place(block, index):
        cols = pl.ds(pl.multiple_of(index * width, 128), width)
        full = block[...].astype(jnp.float32)
        scaled[:, cols] = (full * gain_ref[:, cols]).astype(jnp.bfloat16)
        return jnp.sum(full * full, axis=1, keepdims=True)

    squares = place(tok, mine)
    column = lax.broadcasted_iota(jnp.int32, seat_ref.shape, 1)
    seat_turn = jnp.sum(
        jnp.where(column == me, seat_ref[...], 0.0), axis=1, keepdims=True
    )
    turn = ROT_DIM // 2
    seat_cos, seat_sin = seat_turn[:turn], seat_turn[turn:]
    base_cos, base_sin = base_ref[:turn], base_ref[turn:]
    cos_table = seat_cos * base_cos - seat_sin * base_sin
    sin_table = seat_sin * base_cos + seat_cos * base_sin

    def rotate(block):
        front = block[:turn]
        back = block[turn : 2 * turn]
        return jnp.concatenate(
            [front * cos_table - back * sin_table, back * cos_table + front * sin_table], axis=0
        )

    loads[0].wait()
    own_raw[...] = jnp.dot(
        scaled[:, columns(mine)], kvd[columns(mine), :], preferred_element_type=jnp.float32
    )
    tok_copy.wait()
    squares = squares + place(landed, 1 - mine)
    row_scale = lax.rsqrt(squares / (2 * width) + norm_eps)

    def project(weight):
        return jnp.dot(scaled[...], weight[...], preferred_element_type=jnp.float32)

    loads[1].wait()
    raw = own_raw[...] + jnp.dot(
        scaled[:, columns(1 - mine)], kvd[columns(1 - mine), :], preferred_element_type=jnp.float32
    )
    latent = (
        raw
        * lax.rsqrt(jnp.mean(raw * raw, axis=1, keepdims=True) + norm_eps)
        * kv_gain_ref[...]
    )
    lat_ref[me, :rows, :] = latent.astype(jnp.bfloat16)
    narrow[...] = jnp.broadcast_to(row_scale, narrow.shape)
    key_turn = lax.dot_general(
        rotw[...], scaled[...], (((1,), (1,)), ((), ())), preferred_element_type=jnp.float32
    )
    key_rot = rotate(key_turn * narrow[...].T[:ROT_DIM]).astype(jnp.bfloat16)
    across = rank // 128
    for piece in range(across * ((rows // 128 + across - 1) // across)):
        band = rows + piece // across * ROT_DIM
        lanes = slice(piece % across * 128, piece % across * 128 + 128)
        lat_ref[me, band : band + ROT_DIM, lanes] = (
            key_rot[:, piece * 128 : piece * 128 + 128]
            if piece < rows // 128
            else jnp.zeros((ROT_DIM, 128), jnp.bfloat16)
        )

    def column_copy(block):
        spread = lat_ref.at[block, half]
        return push(spread, spread, col_send.at[block // PLANE], link_recv.at[block], above)

    down_copy = push(
        lat_ref.at[me, half], lat_ref.at[me, half], down_send, link_recv.at[me], root
    )

    def rise(block):
        @pl.when(layer + 1 < layers)
        def _():
            column_copy(block).start()

    def plane_copy(block, distance):
        return push(
            lat_ref.at[block, half],
            lat_ref.at[block, half],
            plane_send.at[block // PLANE, distance - 1],
            link_recv.at[block],
            at(layer, spot_at(distance)),
        )

    def core_copy(block):
        spread = lat_ref.at[block, half]
        return push(spread, spread, core_send.at[block], core_recv.at[block], other)

    rise(me)

    @pl.when(layer > 0)
    def _():
        down_copy.start()

    for d in FAR_FIRST:
        plane_copy(me, d).start()
    for gift in gifts:
        gift.start()

    def arrive(block):
        spread = lat_ref.at[block, half]
        push(spread, spread, core_send.at[block], link_recv.at[block], other).wait_recv()

    def spread_layer(which, upward):
        block = which * PLANE + spot
        arrive(block)
        if upward:
            rise(block)
        for d in FAR_FIRST:
            plane_copy(block, d).start()
        core_copy(block).start()

    def hand_layer(which):
        for d in range(1, PLANE):
            block = which * PLANE + spot_at(d)
            arrive(block)
            core_copy(block).start()

    def relay(step):
        @pl.when(step <= layer)
        def _():
            spread_layer(layer - step, True)

    def hand_over(step):
        @pl.when(step <= layer)
        def _():
            hand_layer(layer - step)

    def descend(distance):
        @pl.when((layer == 0) & (distance < layers))
        def _():
            spread_layer(distance, False)

    loads[2].wait()
    loads[3].wait()
    gate = project(cgw) * row_scale
    gated[...] = (project(cvw) * row_scale * jax.nn.sigmoid(gate)).astype(jnp.bfloat16)
    edge = rim.shape[0]
    rim_copy = push(gated.at[pl.ds(rows - edge, edge)], rim, rim_send, rim_recv, ahead)

    @pl.when(me < seats - 1)
    def _():
        rim_copy.start()

    loads[4].wait()
    loads[5].wait()
    query_scale = row_scale * (math.log2(math.e) / math.sqrt(NOPE_DIM + ROT_DIM))
    plain = (project(qw) * query_scale).T.astype(jnp.bfloat16)
    turned = (project(qrw) * query_scale).T
    for head in range(2 * pairs):
        side = head % 2
        cols = slice(side * rows, (side + 1) * rows)
        q2[head // 2, side * NOPE_DIM : (side + 1) * NOPE_DIM, cols] = plain[
            head * NOPE_DIM : (head + 1) * NOPE_DIM
        ]
        q2[head // 2, 2 * NOPE_DIM : 2 * NOPE_DIM + ROT_DIM, cols] = rotate(
            turned[head * ROT_DIM : (head + 1) * ROT_DIM]
        ).astype(jnp.bfloat16)

    lent = pairs - 1
    q_parts = tuple(
        (pl.ds(low, count), pl.ds(first_col, cols))
        for low, count, first_col, cols in (
            (0, NOPE_DIM, 0, rows),
            (NOPE_DIM, NOPE_DIM, rows, rows),
            (2 * NOPE_DIM, ROT_DIM, 0, 2 * rows),
        )
    )
    q_copies = [
        push(
            q2.at[lent, part_rows, part_cols],
            q_help.at[part_rows, part_cols],
            qh_send.at[index],
            qh_recv.at[index],
            opposite,
        )
        for index, (part_rows, part_cols) in enumerate(q_parts)
    ]

    @pl.when(layer == top_layer)
    def _():
        for copy in q_copies:
            copy.start()

    loads[7].wait()
    vup_t[...] = vup[...].astype(jnp.float32).T.astype(jnp.bfloat16)

    taps = taps_ref.shape[0]
    chunk = 64

    def band_step(step, carry, slab):
        cols = slice(slab * 128, (slab + 1) * 128)
        coeff = taps_ref[:, cols]
        base = step * chunk
        total = jnp.zeros((chunk, 128), jnp.float32)
        for tap in range(taps):
            total = total + coeff[tap : tap + 1, :] * wide[
                slab, pl.ds(base + (edge - taps + 1 + tap), chunk), :
            ]
        conv[pl.ds(pl.multiple_of(base, chunk), chunk), cols] = total
        return carry

    slabs = conv.shape[1] // 128
    for slab in range(slabs):
        wide[slab, edge:, :] = gated[:, slab * 128 : (slab + 1) * 128].astype(jnp.float32)
        lax.fori_loop(1, rows // chunk, functools.partial(band_step, slab=slab), 0)
        if slab == slabs // 2:
            relay(1)
            descend(1)
    hand_over(0)

    @pl.when(me > 0)
    def _():
        rim_copy.wait_recv()

    @pl.when(me == 0)
    def _():
        rim[...] = jnp.zeros(rim.shape, jnp.bfloat16)

    for slab in range(slabs):
        wide[slab, :edge, :] = rim[:, slab * 128 : (slab + 1) * 128].astype(jnp.float32)
        band_step(0, 0, slab)

    values = conv[...]
    for slot, total in enumerate((values, values * values)):
        sq_mine[:, slot * 128 : (slot + 1) * 128] = jnp.broadcast_to(
            jnp.sum(total, axis=1, keepdims=True), (rows, 128)
        )
    sums = push(sq_mine, sq_other, sq_send, sq_recv, other)
    sums.start()

    def activate():
        sums.wait()
        values = conv[...]
        moments = (sq_mine[...] + sq_other[...]) / CONV_CH
        mean_val = moments[:, :1]
        spread_val = moments[:, 128:129] - mean_val * mean_val
        normed = (values - mean_val) * lax.rsqrt(spread_val + norm_eps)
        swished = jax.nn.silu(normed * ln_gain_ref[...] + ln_bias_ref[...])
        conv_act[0] = (swished * conv_gain_ref[...]).astype(jnp.bfloat16)
        end_mine[...] = jnp.broadcast_to(
            jnp.sum(swished * swished, axis=1, keepdims=True), (rows, 128)
        )
        conv_sum.start()
        conv_copy.start()

    conv_sum = push(end_mine, end_other, csq_send, csq_recv, other)
    conv_copy = push(conv_act.at[0], conv_act.at[1], conv_send, conv_recv, other)

    def gathered(step):
        for d in range(1, PLANE):
            core_copy((layer - step) * PLANE + spot_at(d)).wait_recv()

    strip = 256
    strips = keys_wide // strip

    def expand(group, slot, index, only=None):
        pieces = []
        low, left = index * strip, strip
        while left > 0:
            take = min(rows - low % rows, left)
            pieces.append(
                lat_ref[group * PLANE + low // rows, low % rows : low % rows + take, :]
            )
            low, left = low + take, left - take
        lat = pieces[0] if len(pieces) == 1 else jnp.concatenate(pieces, axis=0)
        cut = slice(index * strip, (index + 1) * strip)
        some = range(pairs) if only is None else range(only, only + 1)
        key_cols = slice(2 * NOPE_DIM * some[0], 2 * NOPE_DIM * (some[-1] + 1))
        value_cols = slice(2 * VALUE_DIM * some[0], 2 * VALUE_DIM * (some[-1] + 1))
        kn[slot, cut, : 2 * NOPE_DIM * len(some)] = jnp.dot(
            lat, kup[:, key_cols], preferred_element_type=jnp.float32
        ).astype(jnp.bfloat16)
        values = lax.dot_general(
            vup_t[value_cols, :],
            lat,
            (((1,), (1,)), ((), ())),
            preferred_element_type=jnp.float32,
        ).astype(jnp.bfloat16)
        for pair in range(len(some)):
            low = 2 * VALUE_DIM * pair
            vt[slot, pair, :ones_low, cut] = values[low : low + VALUE_DIM]
            vt[slot, pair, ones_high:, cut] = values[low + VALUE_DIM : low + 2 * VALUE_DIM]
        for blk in range(index, PLANE, strips):
            pieces = []
            for piece in range(rows // 128):
                band = rows + piece // across * ROT_DIM
                lanes = slice(piece % across * 128, piece % across * 128 + 128)
                pieces.append(lat_ref[group * PLANE + blk, band : band + ROT_DIM, lanes])
            rot = jnp.concatenate(pieces, axis=1).astype(jnp.float32)
            rot = jnp.concatenate([rot, jnp.zeros((128 - ROT_DIM, rows), jnp.float32)], axis=0)
            kr[slot, blk * rows : (blk + 1) * rows, :] = rot.T.astype(jnp.bfloat16)

    tiles = both // 256
    tile_rows = tuple(
        (
            0 if 256 * tile < rows else ones_low,
            ones_high if 256 * (tile + 1) <= rows else vt.shape[2],
        )
        for tile in range(tiles)
    )

    def hidden_keys(first_key, first_query):
        key = first_key + lax.broadcasted_iota(jnp.int32, (strip, both), 0)
        query = lax.broadcasted_iota(jnp.int32, (strip, both), 1)
        return key > first_query + jnp.where(query >= rows, query - rows, query)

    def weigh(slot, place_id, index, weights, sums):
        cut = slice(index * strip, (index + 1) * strip)
        for tile, (low, high) in enumerate(tile_rows):
            new = jnp.dot(
                vt[slot, place_id, low:high, cut],
                weights[:, 256 * tile : 256 * (tile + 1)],
                preferred_element_type=jnp.float32,
            )
            sums[tile] = new if sums[tile] is None else sums[tile] + new

    def attend(slot, first, hidden, middle, following):
        def score(pair, index):
            cut = slice(index * strip, (index + 1) * strip)
            keys = jnp.concatenate(
                [kn[slot, cut, 128 * pair : 128 * pair + 128], kr[slot, cut, :]], axis=1
            )
            scores = jnp.dot(keys, q2[pair], preferred_element_type=jnp.float32)
            if hidden is not None:
                scores = jnp.where(hidden(index), far_below, scores)
            s_ref[pair % 2, cut, :] = scores
            return jnp.max(scores, axis=0, keepdims=True)

        def settle_top(pair, tops):
            top = functools.reduce(jnp.maximum, tops)
            fade = None
            if not first:
                old = run_max[pair : pair + 1, :]
                top = jnp.maximum(old, top)
                fade = jnp.exp2(old - top)
            run_max[pair : pair + 1, :] = top
            return top, fade

        def weights_of(pair, index, top):
            cut = slice(index * strip, (index + 1) * strip)
            return jnp.exp2(s_ref[pair % 2, cut, :] - top).astype(jnp.bfloat16)

        def close(pair, sums, fade):
            for tile, (low, high) in enumerate(tile_rows):
                new = sums[tile]
                if not first:
                    new = new + acc[pair, tile, : high - low, :] * fade[
                        :, 256 * tile : 256 * (tile + 1)
                    ]
                acc[pair, tile, : high - low, :] = new

        tops = [score(0, index) for index in range(strips)]
        for pair in range(lent):
            middle(pair)
            top, fade = settle_top(pair, tops)
            tops = []
            sums = [None] * tiles
            for index in range(strips):
                if pair + 1 < lent:
                    tops.append(score(pair + 1, index))
                weigh(slot, pair, index, weights_of(pair, index, top), sums)
                if pair + 1 == lent and following is not None:
                    expand(following, 1 - slot, index)
            close(pair, sums, fade)

        @pl.when(layer < top_layer)
        def _():
            top, fade = settle_top(lent, [score(lent, index) for index in range(strips)])
            sums = [None] * tiles
            for index in range(strips):
                weigh(slot, lent, index, weights_of(lent, index, top), sums)
            close(lent, sums, fade)

    def hidden(index):
        return hidden_keys(layer * keys_wide + index * strip, me * rows)

    loads[6].wait()
    gathered(0)
    for index in range(strips):
        expand(layer, 0, index)
    descend(2)
    relay(2)


    def ready_layer(which):
        for d in range(PLANE):
            core_copy(which * PLANE + spot_at(d)).wait_recv()

    def ready(step):
        @pl.when(step <= layer)
        def _():
            ready_layer(layer - step)

    def first_middle(pair):
        if pair == 1:
            hand_over(1)

            for distance in range(3, layers):
                descend(distance)
            activate()
        if pair == lent - 1:
            ready(1)

    attend(0, True, hidden, first_middle, jnp.maximum(layer - 1, 0))

    def far(step, carry):
        def middle(pair):
            if pair == 0:
                relay(step + 2)
            if pair == 1:
                hand_over(step + 1)
            if pair == lent - 1:
                ready(step + 1)

        attend(step % 2, False, None, middle, layer - step - 1)
        return carry

    lax.fori_loop(1, layer, far, 0)

    @pl.when(layer > 0)
    def _():
        attend(layer % 2, False, None, lambda pair: None, None)

    def finish(pair, keep):
        for side in range(2):
            pieces = []
            for tile, (low, high) in enumerate(tile_rows):
                start = max(side * rows, 256 * tile)
                stop = min((side + 1) * rows, 256 * (tile + 1))
                if start >= stop:
                    continue
                total = acc[pair, tile, : high - low, start - 256 * tile : stop - 256 * tile]
                base = 0 if side == 0 else ones_high - low
                pieces.append(
                    total[base : base + VALUE_DIM] / total[ones_low - low : ones_low - low + 1]
                )
            keep(side, jnp.concatenate(pieces, axis=1).astype(jnp.bfloat16))

    def keep_local(pair):
        def keep(side, block):
            low = (2 * pair + side) * VALUE_DIM
            att_t[low : low + VALUE_DIM, :] = block.astype(jnp.float32)

        return keep

    for pair in range(lent):
        finish(pair, keep_local(pair))

    @pl.when(layer < top_layer)
    def _():
        finish(lent, keep_local(lent))

    help_copy = push(help_out, help_in, help_send, help_recv, opposite)

    @pl.when(layer == 0)
    def _():
        for copy in q_copies:
            copy.wait_recv()
        run_max[0:1, :] = jnp.full((1, both), far_below, jnp.float32)
        acc[0] = jnp.zeros(acc.shape[1:], jnp.float32)
        guest = top_layer * PLANE + spot

        def lend(which, carry):
            @pl.when(which + 1 < layers)
            def _():
                hand_layer(which + 1)

            @pl.when(which > 0)
            def _():
                ready_layer(which)

            tops = []
            for index in range(strips):
                expand(which, 0, index, lent)
            for index in range(strips):
                cut = slice(index * strip, (index + 1) * strip)
                keys = jnp.concatenate([kn[0, cut, :128], kr[0, cut, :]], axis=1)
                scores = jnp.dot(keys, q_help[...], preferred_element_type=jnp.float32)
                scores = jnp.where(
                    hidden_keys(which * keys_wide + index * strip, guest * rows), far_below, scores
                )
                s_ref[0, cut, :] = scores
                tops.append(jnp.max(scores, axis=0, keepdims=True))
            old = run_max[0:1, :]
            top = jnp.maximum(old, functools.reduce(jnp.maximum, tops))
            fade = jnp.exp2(old - top)
            run_max[0:1, :] = top
            sums = [None] * tiles
            for index in range(strips):
                cut = slice(index * strip, (index + 1) * strip)
                weights = jnp.exp2(s_ref[0, cut, :] - top).astype(jnp.bfloat16)
                weigh(0, 0, index, weights, sums)
            for tile, (low, high) in enumerate(tile_rows):
                acc[0, tile, : high - low, :] = sums[tile] + acc[0, tile, : high - low, :] * fade[
                    :, 256 * tile : 256 * (tile + 1)
                ]
            return carry

        lax.fori_loop(0, layers, lend, 0)

        def keep(side, block):
            help_out[side * VALUE_DIM : (side + 1) * VALUE_DIM, :] = block

        finish(0, keep)
        help_copy.start()

    for index in (8, 9):
        loads[index].wait()
    for gift in gifts:
        gift.wait()
    conv_sum.wait()
    conv_copy.wait()
    conv_scale = lax.rsqrt((end_mine[...] + end_other[...])[:, :1] / CONV_CH + norm_eps)

    def product(activations, weight):
        return jnp.dot(activations, weight, preferred_element_type=jnp.float32)

    bulk = 2 * lent * VALUE_DIM
    total_width = bulk + 2 * VALUE_DIM

    def hand_in(low, high, slot):
        attended = att_t[low:high, :]
        att_act[0, :, low:high] = (attended.T * att_gain_ref[:, low:high]).astype(jnp.bfloat16)
        copy = push(
            att_act.at[0, :, pl.ds(low, high - low)],
            att_act.at[1, :, pl.ds(low, high - low)],
            att_send.at[slot],
            att_recv.at[slot],
            other,
        )
        copy.start()
        return copy, jnp.sum(attended * attended, axis=0, keepdims=True)

    def share(core, low, high):
        return product(att_act[core, :, low:high], att_w[core, low:high, :])

    bulk_copy, bulk_sq = hand_in(0, bulk, 0)
    att_sq[...] = jnp.broadcast_to(bulk_sq, att_sq.shape)
    base_part[...] = (
        product(conv_act[0], conv_w[0]) + product(conv_act[1], conv_w[1])
    ) * conv_scale
    own_part[...] = share(0, 0, bulk)
    bulk_copy.wait()
    @pl.when(me < seats - 1)
    def _():
        rim_copy.wait_send()

    def settle(step, carry):
        base = (layer - step) * PLANE
        for d in range(1, PLANE):
            plane_copy(base + spot, d).wait_send()
            core_copy(base + spot_at(d)).wait_send()

        @pl.when(layer + 1 < layers)
        def _():
            column_copy(base + spot).wait_send()

        @pl.when(step > 0)
        def _():
            core_copy(base + spot).wait_send()

        return carry

    lax.fori_loop(0, layer + 1, settle, 0)

    @pl.when(layer > 0)
    def _():
        down_copy.wait_send()

    def settle_guest(which, carry):
        for d in range(1, PLANE):
            plane_copy(which * PLANE + spot, d).wait_send()
        for d in range(PLANE):
            core_copy(which * PLANE + spot_at(d)).wait_send()
        return carry

    @pl.when(layer == 0)
    def _():
        lax.fori_loop(1, layers, settle_guest, 0)
        help_copy.wait_send()

    @pl.when(layer == top_layer)
    def _():
        for copy in q_copies:
            copy.wait_send()

    @pl.when(layer == top_layer)
    def _():
        help_copy.wait_recv()
        att_t[bulk:total_width, :] = help_in[...].astype(jnp.float32)

    rest_copy, rest_sq = hand_in(bulk, total_width, 1)
    att_sq[...] = att_sq[...] + rest_sq
    att_sum = push(att_sq, att_sq_other, asq_send, asq_recv, other)
    att_sum.start()
    own_part[...] = own_part[...] + share(1, 0, bulk) + share(0, bulk, total_width)
    att_sum.wait()
    squares_t = jnp.broadcast_to(att_sq[:1] + att_sq_other[:1], (128, rows)).T
    att_scale = lax.rsqrt(squares_t[:, :1] / ATT_WIDTH + norm_eps)
    rest_copy.wait()
    leaves = []
    for index in range(width // 256):
        cols = slice(index * 256, (index + 1) * 256)
        out_stage[:, cols] = (
            (
                own_part[:, cols]
                + product(att_act[1, :, bulk:total_width], att_w[1, bulk:total_width, cols])
            )
            * att_scale
            + base_part[:, cols]
        ).astype(jnp.bfloat16)
        leave = pltpu.make_async_copy(
            out_stage.at[:, cols], out_ref.at[:, cols], out_sem.at[index]
        )
        leave.start()
        leaves.append(leave)

    for leave in leaves:
        leave.wait()


def angle_tables(seats, rows):
    frequency = rope_base ** (-np.arange(ROT_DIM // 2) / (ROT_DIM // 2))

    def table(positions):
        angles = frequency[:, None] * positions[None, :]
        return jnp.asarray(
            np.concatenate([np.cos(angles), np.sin(angles)], axis=0), jnp.float32
        )

    return table(np.arange(rows)), table(rows * np.arange(-(-seats // 128) * 128))


def fused(tokens, gains, matrices, taps, seats):
    rows, width = tokens.shape
    chans = taps.shape[1]
    rank = matrices[0].shape[1]
    heads = matrices[4].shape[1] // NOPE_DIM
    pairs = heads // 2
    keys_wide = PLANE * rows
    layers = seats // PLANE
    across = rank // 128
    height = rows + -(-(rows // 128) // across) * ROT_DIM
    vmem = pl.BlockSpec(memory_space=pltpu.VMEM)
    anywhere = pl.BlockSpec(memory_space=pltpu.HBM)
    dma = pltpu.SemaphoreType.DMA
    edge = 32
    bf16 = jnp.bfloat16
    f32 = jnp.float32
    value_rows = 2 * VALUE_DIM + 16
    base, seat = angle_tables(seats, rows)
    input_gain, kv_gain, ln_gain, ln_bias, att_gain, conv_gain = gains
    return pl.pallas_call(
        layer_kernel,
        out_shape=jax.ShapeDtypeStruct((rows, width), bf16),
        in_specs=[anywhere] + [vmem] * 9 + [anywhere] * 10,
        out_specs=anywhere,
        scratch_shapes=[pltpu.VMEM(matrix.shape, bf16) for matrix in matrices[:8]]
        + [
            pltpu.VMEM((2, matrix.shape[0], width), bf16) for matrix in matrices[8:]
        ]
        + [
            pltpu.VMEM(matrices[7].shape[::-1], bf16),
            pltpu.VMEM((rows, width), bf16),
            pltpu.VMEM((rows, width), bf16),
            pltpu.VMEM((rows, 2 * width), bf16),
            pltpu.VMEM((rows, rank), f32),
            pltpu.VMEM((rows, 128), f32),
            pltpu.VMEM((rows, chans), bf16),
            pltpu.VMEM((edge, chans), bf16),
            pltpu.VMEM((chans // 128, rows + edge, 128), f32),
            pltpu.VMEM((rows, chans), f32),
            pltpu.VMEM((rows, 256), f32),
            pltpu.VMEM((rows, 256), f32),
            pltpu.VMEM((seats, height, rank), bf16),
            pltpu.VMEM((pairs, 256, 2 * rows), bf16),
            pltpu.VMEM((2, keys_wide, heads * NOPE_DIM), bf16),
            pltpu.VMEM((2, keys_wide, 128), bf16),
            pltpu.VMEM((2, pairs, value_rows, keys_wide), bf16),
            pltpu.VMEM((max(pairs, 8), 2 * rows), f32),
            pltpu.VMEM((pairs, 2 * rows // 256, value_rows, 256), f32),
            pltpu.VMEM((2, keys_wide, 2 * rows), f32),
            pltpu.VMEM((heads * VALUE_DIM, rows), f32),
            pltpu.VMEM((rows, 128), f32),
            pltpu.VMEM((rows, 128), f32),
            pltpu.VMEM((8, rows), f32),
            pltpu.VMEM((8, rows), f32),
            pltpu.VMEM((2, rows, heads * VALUE_DIM), bf16),
            pltpu.VMEM((2, rows, chans), bf16),
            pltpu.VMEM((rows, width), bf16),
            pltpu.VMEM((rows, width), f32),
            pltpu.VMEM((rows, width), f32),
            dma((len(matrices),)),
            dma((2,)),
            dma((2,)),
        ]
        + [dma] * 13
        + [
            dma((2,)),
            dma((2,)),
            dma((layers,)),
            dma,
            dma((layers, PLANE - 1)),
            dma((seats,)),
            dma((seats,)),
            dma((seats,)),
            dma((width // 256,)),
            pltpu.VMEM((256, 2 * rows), bf16),
            pltpu.VMEM((2 * VALUE_DIM, rows), bf16),
            pltpu.VMEM((2 * VALUE_DIM, rows), bf16),
            dma((3,)),
            dma((3,)),
            dma,
            dma,
        ],
        compiler_params=pltpu.CompilerParams(
            vmem_limit_bytes=60 << 20, collective_id=0, has_side_effects=True
        ),
        name="layer",
    )(tokens, input_gain, kv_gain, base, seat, taps, ln_gain, ln_bias, att_gain, conv_gain, *matrices)


def gathered_kernel(q_ref, lat_ref, kup_ref, vup_ref, o_ref, kt, vt, run_max, acc):
    heads, rows, lanes = q_ref.shape
    blocks = lat_ref.shape[0]
    rank = kup_ref.shape[1]
    nope = kup_ref.shape[0] // heads
    vdim = vup_ref.shape[0] // heads
    rot = lat_ref.shape[1] - rank
    wide = kt.shape[2]
    group = wide // rows
    me = lax.axis_index("sp")
    last = me // group
    kt[:, nope + rot :, :] = jnp.zeros((heads, lanes - nope - rot, wide), jnp.bfloat16)
    vt[:, vdim:, :] = jnp.ones((heads, lanes - vdim, wide), jnp.bfloat16)

    def expand(block):
        for part in range(group):
            src = jnp.minimum(block * group + part, blocks - 1)
            lat = lat_ref[src, :rank, :]
            turned = lat_ref[src, rank:, :]
            cols = slice(part * rows, (part + 1) * rows)
            keys = jnp.dot(kup_ref[...], lat, preferred_element_type=jnp.float32)
            values = jnp.dot(vup_ref[...], lat, preferred_element_type=jnp.float32)
            for head in range(heads):
                kt[head, :nope, cols] = keys[head * nope : (head + 1) * nope].astype(jnp.bfloat16)
                kt[head, nope : nope + rot, cols] = turned
                vt[head, :vdim, cols] = values[head * vdim : (head + 1) * vdim].astype(
                    jnp.bfloat16
                )

    def weigh(head, scores, top):
        weights = jnp.exp2(scores - top).astype(jnp.bfloat16)
        return lax.dot_general(
            weights, vt[head], (((1,), (1,)), ((), ())), preferred_element_type=jnp.float32
        )

    expand(last)
    key_pos = last * wide + lax.broadcasted_iota(jnp.int32, (rows, wide), 1)
    query_pos = me * rows + lax.broadcasted_iota(jnp.int32, (rows, wide), 0)
    hidden = key_pos > query_pos
    for head in range(heads):
        scores = jnp.dot(q_ref[head], kt[head], preferred_element_type=jnp.float32)
        scores = jnp.where(hidden, far_below, scores)
        top = jnp.max(scores, axis=1, keepdims=True)
        run_max[head] = jnp.broadcast_to(top, (rows, lanes))
        acc[head] = weigh(head, scores, top)

    def visit(step, carry):
        expand(step)
        for head in range(heads):
            scores = jnp.dot(q_ref[head], kt[head], preferred_element_type=jnp.float32)
            old = run_max[head]
            top = jnp.maximum(old[:, :1], jnp.max(scores, axis=1, keepdims=True))
            wide_top = jnp.broadcast_to(top, (rows, lanes))
            run_max[head] = wide_top
            acc[head] = acc[head] * jnp.exp2(old - wide_top) + weigh(head, scores, top)
        return carry

    lax.fori_loop(0, last, visit, 0)
    lane = lax.broadcasted_iota(jnp.int32, (rows, lanes), 1)
    for pair in range(heads // 2):
        halves = []
        for head in (2 * pair, 2 * pair + 1):
            total = acc[head]
            halves.append(total / pltpu.roll(total, vdim, axis=1))
        both = jnp.where(lane < vdim, halves[0], pltpu.roll(halves[1], vdim, axis=1))
        o_ref[:, pair * lanes : (pair + 1) * lanes] = both.astype(jnp.bfloat16)


def gathered_attention(q_heads, lat_all, key_up_t, value_up_t):
    heads, rows, lanes = q_heads.shape
    blocks = lat_all.shape[0]
    wide = 2 * rows if blocks % 2 == 0 else rows
    vmem = pl.BlockSpec(memory_space=pltpu.VMEM)
    return pl.pallas_call(
        gathered_kernel,
        out_shape=jax.ShapeDtypeStruct((rows, value_up_t.shape[0]), jnp.bfloat16),
        in_specs=[vmem] * 4,
        out_specs=vmem,
        scratch_shapes=[
            pltpu.VMEM((heads, lanes, wide), jnp.bfloat16),
            pltpu.VMEM((heads, lanes, wide), jnp.bfloat16),
            pltpu.VMEM((heads, rows, lanes), jnp.float32),
            pltpu.VMEM((heads, rows, lanes), jnp.float32),
        ],
        compiler_params=pltpu.CompilerParams(vmem_limit_bytes=48 << 20),
        cost_estimate=pl.CostEstimate(
            flops=20_000_000_000, bytes_accessed=8 << 20, transcendentals=20_000_000
        ),
        name="gathered_attention",
    )(q_heads, lat_all, key_up_t, value_up_t)


def conv_kernel(gated_ref, rim_ref, taps_ref, out_ref, wide):
    rows, chans = gated_ref.shape
    rim = rim_ref.shape[0]
    taps = taps_ref.shape[0]
    chunk = 64
    for part in range(chans // 128):
        cols = slice(part * 128, (part + 1) * 128)
        wide[part, :rim, :] = rim_ref[:, cols].astype(jnp.float32)
        wide[part, rim:, :] = gated_ref[:, cols].astype(jnp.float32)
        coeff = taps_ref[:, cols]

        def band(step, carry):
            base = step * chunk
            total = jnp.zeros((chunk, 128), jnp.float32)
            for tap in range(taps):
                total = total + coeff[tap : tap + 1, :] * wide[
                    part, pl.ds(base + (rim - taps + 1 + tap), chunk), :
                ]
            out_ref[pl.ds(pl.multiple_of(base, chunk), chunk), cols] = total
            return carry

        lax.fori_loop(0, rows // chunk, band, 0)


def convolve(gated, rim, taps):
    rows, chans = gated.shape
    vmem = pl.BlockSpec(memory_space=pltpu.VMEM)
    return pl.pallas_call(
        conv_kernel,
        out_shape=jax.ShapeDtypeStruct((rows, chans), jnp.float32),
        in_specs=[vmem] * 3,
        out_specs=vmem,
        scratch_shapes=[pltpu.VMEM((chans // 128, rows + rim.shape[0], 128), jnp.float32)],
        cost_estimate=pl.CostEstimate(
            flops=2 * rows * chans * 31, bytes_accessed=2 << 20, transcendentals=0
        ),
        name="depthwise",
    )(gated, rim, taps)


def shards(
    tokens,
    input_gain,
    query_weight,
    query_rot_weight,
    kv_down,
    rot_down,
    kv_gain,
    key_up,
    value_up,
    conv_value_weight,
    conv_gate_weight,
    conv_taps,
    conv_ln_gain,
    conv_ln_bias,
    att_out_gain,
    conv_out_gain,
    att_out_weight,
    conv_out_weight,
):
    tok_rows = tokens.shape[0]
    heads_here = key_up.shape[1] // NOPE_DIM
    chan_here = conv_taps.shape[1]
    weight_list = (
        query_weight,
        query_rot_weight,
        kv_down,
        rot_down,
        conv_value_weight,
        conv_gate_weight,
    )
    seats = lax.axis_size("sp")
    if (
        lax.axis_size("tp") == 2
        and seats % PLANE == 0
        and tok_rows % 128 == 0
        and heads_here % 2 == 0
        and heads_here > 2
        and seats > PLANE
    ):
        gains = (
            input_gain, kv_gain, conv_ln_gain, conv_ln_bias, att_out_gain, conv_out_gain
        )
        return fused(
            tokens,
            tuple(gain[None, :] for gain in gains),
            (
                kv_down, rot_down.T, conv_gate_weight, conv_value_weight, query_weight,
                query_rot_weight, key_up, value_up, att_out_weight, conv_out_weight,
            ),
            conv_taps,
            seats,
        )
    whole_rows = lax.all_gather(tokens, "tp", axis=1, tiled=True).astype(jnp.float32)
    scaled = (whole_rows * input_gain[None, :]).astype(jnp.bfloat16)
    row_scale = lax.rsqrt(jnp.mean(whole_rows * whole_rows, axis=1, keepdims=True) + norm_eps)

    def add_product(weight):
        return jnp.dot(scaled, weight, preferred_element_type=jnp.float32)

    summed = tuple((add_product(weight) for weight in weight_list))
    q_acc, qrot_acc, latent_raw, rot_acc, value_acc, gate_acc = summed
    positions = lax.axis_index("sp") * tok_rows + jnp.arange(tok_rows, dtype=jnp.int32)
    cos_table, sine_table = rotary_tables(positions, ROT_DIM // 2)
    fold = math.log2(math.e) / math.sqrt(NOPE_DIM + ROT_DIM)
    query_scale = row_scale * fold
    plain_q = (q_acc * query_scale).reshape(tok_rows, heads_here, NOPE_DIM)
    turned_q = rotate_half(
        (qrot_acc * query_scale).reshape(tok_rows, heads_here, ROT_DIM),
        cos_table[:, None, :],
        sine_table[:, None, :],
    )
    blank = jnp.zeros((tok_rows, heads_here, 128 - NOPE_DIM - ROT_DIM), jnp.float32)
    q_heads = jnp.transpose(
        jnp.concatenate([plain_q, turned_q, blank], axis=2).astype(jnp.bfloat16), (1, 0, 2)
    )
    latent = (
        latent_raw
        * lax.rsqrt(jnp.mean(latent_raw * latent_raw, axis=1, keepdims=True) + norm_eps)
        * kv_gain[None, :]
    ).astype(jnp.bfloat16)
    key_rot = rotate_half(rot_acc * row_scale, cos_table, sine_table).astype(jnp.bfloat16)
    gated_input = (value_acc * row_scale * jax.nn.sigmoid(gate_acc * row_scale)).astype(
        jnp.bfloat16
    )
    packed = jnp.concatenate([latent.T, key_rot.T], axis=0)
    rim_rows = shifted(gated_input[tok_rows - (KERNEL + 1) :], "sp", 1)
    conv_out = convolve(gated_input, rim_rows, conv_taps)
    moment_one, moment_two = lax.psum(
        (jnp.sum(conv_out, axis=1), jnp.sum(conv_out * conv_out, axis=1)), "tp"
    )
    mean_val = moment_one / CONV_CH
    spread = moment_two / CONV_CH - mean_val * mean_val
    normed = (conv_out - mean_val[:, None]) * lax.rsqrt(spread + norm_eps)[:, None]
    swished = jax.nn.silu(normed * conv_ln_gain[None, :] + conv_ln_bias[None, :])
    lat_all = lax.all_gather(packed, "sp", axis=0)
    attended = gathered_attention(q_heads, lat_all, key_up.T, value_up.T).astype(jnp.float32)
    att_sq, conv_sq = lax.psum(
        (
            jnp.sum(attended * attended, axis=1, keepdims=True),
            jnp.sum(swished * swished, axis=1, keepdims=True),
        ),
        "tp",
    )
    att_mixed = (
        attended * lax.rsqrt(att_sq / ATT_WIDTH + norm_eps) * att_out_gain[None, :]
    ).astype(jnp.bfloat16)
    conv_mixed = (
        swished * lax.rsqrt(conv_sq / CONV_CH + norm_eps) * conv_out_gain[None, :]
    ).astype(jnp.bfloat16)
    share = (
        jnp.dot(att_mixed, att_out_weight, preferred_element_type=jnp.float32)
        + jnp.dot(conv_mixed, conv_out_weight, preferred_element_type=jnp.float32)
    ).astype(jnp.bfloat16)
    return lax.psum_scatter(share, "tp", scatter_dimension=1, tiled=True)


def solution(mesh):
    return jax.shard_map(
        shards,
        mesh=mesh,
        in_specs=(
            P("sp", "tp"),
            P(),
            P(None, "tp"),
            P(None, "tp"),
            P(),
            P(),
            P(),
            P(None, "tp"),
            P(None, "tp"),
            P(None, "tp"),
            P(None, "tp"),
            P(None, "tp"),
            P("tp"),
            P("tp"),
            P("tp"),
            P("tp"),
            P("tp", None),
            P("tp", None),
        ),
        out_specs=P("sp", "tp"),
        check_vma=False,
    )
```

```python
import functools
import math

import jax
import jax.numpy as jnp
import numpy as np
from jax import lax
from jax.experimental import pallas as pl
from jax.experimental.pallas import tpu as pltpu
from jax.sharding import PartitionSpec as P

D_MODEL = 2048
NOPE_DIM = 64
ROT_DIM = 32
VALUE_DIM = 64
CONV_CH = 1024
KERNEL = 31
ATT_WIDTH = 1024


norm_eps = 1e-06
far_below = -1e30
rope_base = 10000.0


def shifted(block, axis, distance):
    devices = range(lax.axis_size(axis))
    route = [(i - distance, i) for i in devices if i - distance in devices]
    return lax.ppermute(block, axis, route)


def rotary_tables(positions, half_dim):
    frequency = rope_base ** (-jnp.arange(half_dim, dtype=jnp.float32) / half_dim)
    angles = positions.astype(jnp.float32)[:, None] * frequency[None, :]
    return (jnp.cos(angles), jnp.sin(angles))


def rotate_half(values, cos_table, sine_table):
    half_dim = cos_table.shape[-1]
    front_half = values[..., :half_dim]
    back_half = values[..., half_dim:]
    return jnp.concatenate(
        [
            front_half * cos_table - back_half * sine_table,
            back_half * cos_table + front_half * sine_table,
        ],
        axis=-1,
    )


MESH = pl.DeviceIdType.MESH


def push(src, dst, send, recv, target):
    return pltpu.make_async_remote_copy(
        src_ref=src,
        dst_ref=dst,
        send_sem=send,
        recv_sem=recv,
        device_id=target,
        device_id_type=MESH,
    )


def other_core():
    return {"sp": lax.axis_index("sp"), "tp": 1 - lax.axis_index("tp")}


PLANE = 4


FAR_FIRST = (3, 1, 2)


def layer_kernel(
    tok_hbm, gain_ref, kv_gain_ref, base_ref, seat_ref, taps_ref, ln_gain_ref, ln_bias_ref,
    att_gain_ref, conv_gain_ref,
    kvd_hbm, rotw_hbm, cgw_hbm, cvw_hbm, qw_hbm, qrw_hbm, kup_hbm, vup_hbm, att_hbm, conv_hbm,
    out_ref,
    kvd, rotw, cgw, cvw, qw, qrw, kup, vup, att_w, conv_w, vup_t,
    tok, landed, scaled, own_raw, narrow, gated, rim, wide, conv, sq_mine, sq_other,
    lat_ref, q2, kn, kr, vt, run_max, acc, s_ref, att_t, end_mine, end_other,
    att_sq, att_sq_other, att_act, conv_act, out_stage, base_part, own_part,
    w_sem, w_send, w_recv, tok_load, tok_send, tok_recv, rim_send, rim_recv, sq_send, sq_recv,
    csq_send, csq_recv, asq_send, asq_recv, conv_send, conv_recv, att_send, att_recv,
    col_send, down_send, plane_send, core_send, link_recv, core_recv, out_sem,
    q_help, help_out, help_in, qh_send, qh_recv, help_send, help_recv,
):
    mine = lax.axis_index("tp")
    me = lax.axis_index("sp")
    seats = lax.axis_size("sp")
    rows, width = tok.shape
    blocks = lat_ref.shape[0]
    rank = kvd.shape[1]
    layers = blocks // PLANE
    layer = me // PLANE
    spot = me % PLANE
    height = lat_ref.shape[1] // 2
    half = pl.ds(pl.multiple_of(mine * height, 16), height)
    other = other_core()
    ahead = {"sp": (me + 1) % seats, "tp": mine}
    behind = {"sp": (me + seats - 1) % seats, "tp": mine}

    def columns(owner):
        return pl.ds(pl.multiple_of(owner * width, 128), width)

    loads = [
        pltpu.make_async_copy(src, dst, w_sem.at[index])
        for index, (src, dst) in enumerate(
            (
                (kvd_hbm, kvd), (rotw_hbm, rotw), (cgw_hbm, cgw), (cvw_hbm, cvw),
                (qw_hbm, qw), (qrw_hbm, qrw), (kup_hbm, kup), (vup_hbm, vup),
                (att_hbm.at[:, columns(mine)], att_w.at[0]),
                (conv_hbm.at[:, columns(mine)], conv_w.at[0]),
            )
        )
    ]
    fetch = pltpu.make_async_copy(tok_hbm, tok, tok_load)
    fetch.start()
    for load in loads[:2]:
        load.start()
    gifts = [
        push(src.at[:, columns(1 - mine)], dst.at[1], w_send.at[index], w_recv.at[index], other)
        for index, (src, dst) in enumerate(((att_hbm, att_w), (conv_hbm, conv_w)))
    ]

    def spot_at(step):
        return (spot % 2 + step % 2) % 2 + 2 * ((spot // 2 + step // 2) % 2)

    def at(layer_id, spot_id):
        return {"sp": layer_id * PLANE + spot_id, "tp": mine}

    q_help[...] = jnp.zeros(q_help.shape, jnp.bfloat16)
    barrier = pltpu.get_barrier_semaphore()
    peers = [at(layer, spot_at(d)) for d in range(1, PLANE)] + [other]
    for peer in peers:
        pl.semaphore_signal(barrier, inc=1, device_id=peer, device_id_type=MESH)
    above = at(jnp.minimum(layer + 1, layers - 1), spot)
    below = at(jnp.maximum(layer - 1, 0), spot)
    top_layer = layers - 1
    opposite = at(top_layer - layer, spot)
    root = at(0, spot)
    for condition, peer in [
        (layer == 0, at(other_layer, spot)) for other_layer in range(2, layers)
    ] + [
        (layer > 1, root), (layer < layers - 1, above), (layer > 0, below), (me < seats - 1, ahead), (me > 0, behind),
    ]:

        @pl.when(condition)
        def _(peer=peer):
            pl.semaphore_signal(barrier, inc=1, device_id=peer, device_id_type=MESH)

    pairs, _, both = q2.shape
    keys_wide = kn.shape[1]
    q2[...] = jnp.zeros(q2.shape, jnp.bfloat16)
    ones_low = VALUE_DIM
    ones_high = vt.shape[2] - VALUE_DIM
    vt[:, :, ones_low:ones_high, :] = jnp.ones(
        (2, pairs, ones_high - ones_low, keys_wide), jnp.bfloat16
    )
    pl.semaphore_wait(
        barrier,
        len(peers)
        + jnp.minimum(me, 1)
        + jnp.minimum(seats - 1 - me, 1)
        + jnp.minimum(layer, 1)
        + jnp.minimum(layers - 1 - layer, 1)
        + jnp.where(layer == 0, layers - 2, jnp.where(layer > 1, 1, 0)),
    )
    fetch.wait()
    tok_copy = push(tok, landed, tok_send, tok_recv, other)
    tok_copy.start()
    for load in loads[2:]:
        load.start()

    def place(block, index):
        cols = pl.ds(pl.multiple_of(index * width, 128), width)
        full = block[...].astype(jnp.float32)
        scaled[:, cols] = (full * gain_ref[:, cols]).astype(jnp.bfloat16)
        return jnp.sum(full * full, axis=1, keepdims=True)

    squares = place(tok, mine)
    column = lax.broadcasted_iota(jnp.int32, seat_ref.shape, 1)
    seat_turn = jnp.sum(
        jnp.where(column == me, seat_ref[...], 0.0), axis=1, keepdims=True
    )
    turn = ROT_DIM // 2
    seat_cos, seat_sin = seat_turn[:turn], seat_turn[turn:]
    base_cos, base_sin = base_ref[:turn], base_ref[turn:]
    cos_table = seat_cos * base_cos - seat_sin * base_sin
    sin_table = seat_sin * base_cos + seat_cos * base_sin

    def rotate(block):
        front = block[:turn]
        back = block[turn : 2 * turn]
        return jnp.concatenate(
            [front * cos_table - back * sin_table, back * cos_table + front * sin_table], axis=0
        )

    loads[0].wait()
    own_raw[...] = jnp.dot(
        scaled[:, columns(mine)], kvd[columns(mine), :], preferred_element_type=jnp.float32
    )
    tok_copy.wait()
    squares = squares + place(landed, 1 - mine)
    row_scale = lax.rsqrt(squares / (2 * width) + norm_eps)

    def project(weight):
        return jnp.dot(scaled[...], weight[...], preferred_element_type=jnp.float32)

    loads[1].wait()
    raw = own_raw[...] + jnp.dot(
        scaled[:, columns(1 - mine)], kvd[columns(1 - mine), :], preferred_element_type=jnp.float32
    )
    latent = (
        raw
        * lax.rsqrt(jnp.mean(raw * raw, axis=1, keepdims=True) + norm_eps)
        * kv_gain_ref[...]
    )
    lat_ref[me, :rows, :] = latent.astype(jnp.bfloat16)
    narrow[...] = jnp.broadcast_to(row_scale, narrow.shape)
    key_turn = lax.dot_general(
        rotw[...], scaled[...], (((1,), (1,)), ((), ())), preferred_element_type=jnp.float32
    )
    key_rot = rotate(key_turn * narrow[...].T[:ROT_DIM]).astype(jnp.bfloat16)
    across = rank // 128
    for piece in range(across * ((rows // 128 + across - 1) // across)):
        band = rows + piece // across * ROT_DIM
        lanes = slice(piece % across * 128, piece % across * 128 + 128)
        lat_ref[me, band : band + ROT_DIM, lanes] = (
            key_rot[:, piece * 128 : piece * 128 + 128]
            if piece < rows // 128
            else jnp.zeros((ROT_DIM, 128), jnp.bfloat16)
        )

    def column_copy(block):
        spread = lat_ref.at[block, half]
        return push(spread, spread, col_send.at[block // PLANE], link_recv.at[block], above)

    def down_copy(block, target):
        spread = lat_ref.at[block, half]
        return push(spread, spread, down_send.at[block // PLANE], link_recv.at[block], target)

    lower = at(jnp.where(layer == top_layer, 0, jnp.maximum(layer - 1, 0)), spot)

    def rise(block):
        @pl.when(layer + 1 < layers)
        def _():
            column_copy(block).start()

    def plane_copy(block, distance):
        return push(
            lat_ref.at[block, half],
            lat_ref.at[block, half],
            plane_send.at[block // PLANE, distance - 1],
            link_recv.at[block],
            at(layer, spot_at(distance)),
        )

    def core_copy(block):
        spread = lat_ref.at[block, half]
        return push(spread, spread, core_send.at[block], core_recv.at[block], other)

    rise(me)

    @pl.when(layer > 0)
    def _():
        down_copy(me, lower).start()

    for d in FAR_FIRST:
        plane_copy(me, d).start()
    for gift in gifts:
        gift.start()

    def arrive(block):
        spread = lat_ref.at[block, half]
        push(spread, spread, core_send.at[block], link_recv.at[block], other).wait_recv()

    def spread_layer(which, upward):
        block = which * PLANE + spot
        arrive(block)
        if upward:
            rise(block)
        for d in FAR_FIRST:
            plane_copy(block, d).start()
        core_copy(block).start()

    def hand_layer(which):
        for d in range(1, PLANE):
            block = which * PLANE + spot_at(d)
            arrive(block)
            core_copy(block).start()

    def relay(step):
        @pl.when(step <= layer)
        def _():
            spread_layer(layer - step, True)

    def hand_over(step):
        @pl.when(step <= layer)
        def _():
            hand_layer(layer - step)

    def descend(distance):
        @pl.when((layer > 0) & (layer + distance < top_layer))
        def _():
            block = (layer + distance) * PLANE + spot
            arrive(block)
            down_copy(block, below).start()

        @pl.when((layer == 0) & (distance < layers))
        def _():
            spread_layer(distance, False)

    loads[2].wait()
    loads[3].wait()
    gate = project(cgw) * row_scale
    gated[...] = (project(cvw) * row_scale * jax.nn.sigmoid(gate)).astype(jnp.bfloat16)
    edge = rim.shape[0]
    rim_copy = push(gated.at[pl.ds(rows - edge, edge)], rim, rim_send, rim_recv, ahead)

    @pl.when(me < seats - 1)
    def _():
        rim_copy.start()

    loads[4].wait()
    loads[5].wait()
    query_scale = row_scale * (math.log2(math.e) / math.sqrt(NOPE_DIM + ROT_DIM))
    plain = (project(qw) * query_scale).T.astype(jnp.bfloat16)
    turned = (project(qrw) * query_scale).T
    for head in range(2 * pairs):
        side = head % 2
        cols = slice(side * rows, (side + 1) * rows)
        q2[head // 2, side * NOPE_DIM : (side + 1) * NOPE_DIM, cols] = plain[
            head * NOPE_DIM : (head + 1) * NOPE_DIM
        ]
        q2[head // 2, 2 * NOPE_DIM : 2 * NOPE_DIM + ROT_DIM, cols] = rotate(
            turned[head * ROT_DIM : (head + 1) * ROT_DIM]
        ).astype(jnp.bfloat16)

    lent = pairs - 1
    q_parts = tuple(
        (pl.ds(low, count), pl.ds(first_col, cols))
        for low, count, first_col, cols in (
            (0, NOPE_DIM, 0, rows),
            (NOPE_DIM, NOPE_DIM, rows, rows),
            (2 * NOPE_DIM, ROT_DIM, 0, 2 * rows),
        )
    )
    q_copies = [
        push(
            q2.at[lent, part_rows, part_cols],
            q_help.at[part_rows, part_cols],
            qh_send.at[index],
            qh_recv.at[index],
            opposite,
        )
        for index, (part_rows, part_cols) in enumerate(q_parts)
    ]

    @pl.when(layer == top_layer)
    def _():
        for copy in q_copies:
            copy.start()

    loads[7].wait()
    vup_t[...] = vup[...].astype(jnp.float32).T.astype(jnp.bfloat16)

    taps = taps_ref.shape[0]
    chunk = 64

    def band_step(step, carry, slab):
        cols = slice(slab * 128, (slab + 1) * 128)
        coeff = taps_ref[:, cols]
        base = step * chunk
        total = jnp.zeros((chunk, 128), jnp.float32)
        for tap in range(taps):
            total = total + coeff[tap : tap + 1, :] * wide[
                slab, pl.ds(base + (edge - taps + 1 + tap), chunk), :
            ]
        conv[pl.ds(pl.multiple_of(base, chunk), chunk), cols] = total
        return carry

    slabs = conv.shape[1] // 128
    for slab in range(slabs):
        wide[slab, edge:, :] = gated[:, slab * 128 : (slab + 1) * 128].astype(jnp.float32)
        lax.fori_loop(1, rows // chunk, functools.partial(band_step, slab=slab), 0)
        if slab == slabs // 2:
            relay(1)
            descend(1)
    hand_over(0)

    @pl.when(me > 0)
    def _():
        rim_copy.wait_recv()

    @pl.when(me == 0)
    def _():
        rim[...] = jnp.zeros(rim.shape, jnp.bfloat16)

    for slab in range(slabs):
        wide[slab, :edge, :] = rim[:, slab * 128 : (slab + 1) * 128].astype(jnp.float32)
        band_step(0, 0, slab)

    values = conv[...]
    for slot, total in enumerate((values, values * values)):
        sq_mine[:, slot * 128 : (slot + 1) * 128] = jnp.broadcast_to(
            jnp.sum(total, axis=1, keepdims=True), (rows, 128)
        )
    sums = push(sq_mine, sq_other, sq_send, sq_recv, other)
    sums.start()

    def activate():
        sums.wait()
        values = conv[...]
        moments = (sq_mine[...] + sq_other[...]) / CONV_CH
        mean_val = moments[:, :1]
        spread_val = moments[:, 128:129] - mean_val * mean_val
        normed = (values - mean_val) * lax.rsqrt(spread_val + norm_eps)
        swished = jax.nn.silu(normed * ln_gain_ref[...] + ln_bias_ref[...])
        conv_act[0] = (swished * conv_gain_ref[...]).astype(jnp.bfloat16)
        end_mine[...] = jnp.broadcast_to(
            jnp.sum(swished * swished, axis=1, keepdims=True), (rows, 128)
        )
        conv_sum.start()
        conv_copy.start()

    conv_sum = push(end_mine, end_other, csq_send, csq_recv, other)
    conv_copy = push(conv_act.at[0], conv_act.at[1], conv_send, conv_recv, other)

    def gathered(step):
        for d in range(1, PLANE):
            core_copy((layer - step) * PLANE + spot_at(d)).wait_recv()

    strip = 256
    strips = keys_wide // strip

    def expand(group, slot, index, only=None):
        pieces = []
        low, left = index * strip, strip
        while left > 0:
            take = min(rows - low % rows, left)
            pieces.append(
                lat_ref[group * PLANE + low // rows, low % rows : low % rows + take, :]
            )
            low, left = low + take, left - take
        lat = pieces[0] if len(pieces) == 1 else jnp.concatenate(pieces, axis=0)
        cut = slice(index * strip, (index + 1) * strip)
        some = range(pairs) if only is None else range(only, only + 1)
        key_cols = slice(2 * NOPE_DIM * some[0], 2 * NOPE_DIM * (some[-1] + 1))
        value_cols = slice(2 * VALUE_DIM * some[0], 2 * VALUE_DIM * (some[-1] + 1))
        kn[slot, cut, : 2 * NOPE_DIM * len(some)] = jnp.dot(
            lat, kup[:, key_cols], preferred_element_type=jnp.float32
        ).astype(jnp.bfloat16)
        values = lax.dot_general(
            vup_t[value_cols, :],
            lat,
            (((1,), (1,)), ((), ())),
            preferred_element_type=jnp.float32,
        ).astype(jnp.bfloat16)
        for pair in range(len(some)):
            low = 2 * VALUE_DIM * pair
            vt[slot, pair, :ones_low, cut] = values[low : low + VALUE_DIM]
            vt[slot, pair, ones_high:, cut] = values[low + VALUE_DIM : low + 2 * VALUE_DIM]
        for blk in range(index, PLANE, strips):
            pieces = []
            for piece in range(rows // 128):
                band = rows + piece // across * ROT_DIM
                lanes = slice(piece % across * 128, piece % across * 128 + 128)
                pieces.append(lat_ref[group * PLANE + blk, band : band + ROT_DIM, lanes])
            rot = jnp.concatenate(pieces, axis=1).astype(jnp.float32)
            rot = jnp.concatenate([rot, jnp.zeros((128 - ROT_DIM, rows), jnp.float32)], axis=0)
            kr[slot, blk * rows : (blk + 1) * rows, :] = rot.T.astype(jnp.bfloat16)

    tiles = both // 256
    tile_rows = tuple(
        (
            0 if 256 * tile < rows else ones_low,
            ones_high if 256 * (tile + 1) <= rows else vt.shape[2],
        )
        for tile in range(tiles)
    )

    def hidden_keys(first_key, first_query):
        key = first_key + lax.broadcasted_iota(jnp.int32, (strip, both), 0)
        query = lax.broadcasted_iota(jnp.int32, (strip, both), 1)
        return key > first_query + jnp.where(query >= rows, query - rows, query)

    def weigh(slot, place_id, index, weights, sums):
        cut = slice(index * strip, (index + 1) * strip)
        for tile, (low, high) in enumerate(tile_rows):
            new = jnp.dot(
                vt[slot, place_id, low:high, cut],
                weights[:, 256 * tile : 256 * (tile + 1)],
                preferred_element_type=jnp.float32,
            )
            sums[tile] = new if sums[tile] is None else sums[tile] + new

    def attend(slot, first, hidden, middle, following):
        def score(pair, index):
            cut = slice(index * strip, (index + 1) * strip)
            keys = jnp.concatenate(
                [kn[slot, cut, 128 * pair : 128 * pair + 128], kr[slot, cut, :]], axis=1
            )
            scores = jnp.dot(keys, q2[pair], preferred_element_type=jnp.float32)
            if hidden is not None:
                scores = jnp.where(hidden(index), far_below, scores)
            s_ref[pair % 2, cut, :] = scores
            return jnp.max(scores, axis=0, keepdims=True)

        def settle_top(pair, tops):
            top = functools.reduce(jnp.maximum, tops)
            fade = None
            if not first:
                old = run_max[pair : pair + 1, :]
                top = jnp.maximum(old, top)
                fade = jnp.exp2(old - top)
            run_max[pair : pair + 1, :] = top
            return top, fade

        def weights_of(pair, index, top):
            cut = slice(index * strip, (index + 1) * strip)
            return jnp.exp2(s_ref[pair % 2, cut, :] - top).astype(jnp.bfloat16)

        def close(pair, sums, fade):
            for tile, (low, high) in enumerate(tile_rows):
                new = sums[tile]
                if not first:
                    new = new + acc[pair, tile, : high - low, :] * fade[
                        :, 256 * tile : 256 * (tile + 1)
                    ]
                acc[pair, tile, : high - low, :] = new

        tops = [score(0, index) for index in range(strips)]
        for pair in range(lent):
            middle(pair)
            top, fade = settle_top(pair, tops)
            tops = []
            sums = [None] * tiles
            for index in range(strips):
                if pair + 1 < lent:
                    tops.append(score(pair + 1, index))
                weigh(slot, pair, index, weights_of(pair, index, top), sums)
                if pair + 1 == lent and following is not None:
                    expand(following, 1 - slot, index)
            close(pair, sums, fade)

        @pl.when(layer < top_layer)
        def _():
            top, fade = settle_top(lent, [score(lent, index) for index in range(strips)])
            sums = [None] * tiles
            for index in range(strips):
                weigh(slot, lent, index, weights_of(lent, index, top), sums)
            close(lent, sums, fade)

    def hidden(index):
        return hidden_keys(layer * keys_wide + index * strip, me * rows)

    loads[6].wait()
    gathered(0)
    for index in range(strips):
        expand(layer, 0, index)
    for distance in range(2, layers - 2):

        @pl.when(layer > 0)
        def _(distance=distance):
            descend(distance)

    @pl.when(layer == 0)
    def _():
        if layers > 2:
            descend(layers - 1)

    relay(2)


    def ready_layer(which):
        for d in range(PLANE):
            core_copy(which * PLANE + spot_at(d)).wait_recv()

    def ready(step):
        @pl.when(step <= layer)
        def _():
            ready_layer(layer - step)

    def first_middle(pair):
        if pair == 1:
            hand_over(1)


            @pl.when(layer == 0)
            def _():
                for distance in range(2, layers - 1):
                    descend(distance)

            activate()
        if pair == lent - 1:
            ready(1)

    attend(0, True, hidden, first_middle, jnp.maximum(layer - 1, 0))

    def far(step, carry):
        def middle(pair):
            if pair == 0:
                relay(step + 2)
            if pair == 1:
                hand_over(step + 1)
            if pair == lent - 1:
                ready(step + 1)

        attend(step % 2, False, None, middle, layer - step - 1)
        return carry

    lax.fori_loop(1, layer, far, 0)

    @pl.when(layer > 0)
    def _():
        attend(layer % 2, False, None, lambda pair: None, None)

    def finish(pair, keep):
        for side in range(2):
            pieces = []
            for tile, (low, high) in enumerate(tile_rows):
                start = max(side * rows, 256 * tile)
                stop = min((side + 1) * rows, 256 * (tile + 1))
                if start >= stop:
                    continue
                total = acc[pair, tile, : high - low, start - 256 * tile : stop - 256 * tile]
                base = 0 if side == 0 else ones_high - low
                pieces.append(
                    total[base : base + VALUE_DIM] / total[ones_low - low : ones_low - low + 1]
                )
            keep(side, jnp.concatenate(pieces, axis=1).astype(jnp.bfloat16))

    def keep_local(pair):
        def keep(side, block):
            low = (2 * pair + side) * VALUE_DIM
            att_t[low : low + VALUE_DIM, :] = block.astype(jnp.float32)

        return keep

    for pair in range(lent):
        finish(pair, keep_local(pair))

    @pl.when(layer < top_layer)
    def _():
        finish(lent, keep_local(lent))

    help_copy = push(help_out, help_in, help_send, help_recv, opposite)

    @pl.when(layer == 0)
    def _():
        for copy in q_copies:
            copy.wait_recv()
        run_max[0:1, :] = jnp.full((1, both), far_below, jnp.float32)
        acc[0] = jnp.zeros(acc.shape[1:], jnp.float32)
        guest = top_layer * PLANE + spot

        def visited(turn_id):
            return jnp.where(
                turn_id <= 1, turn_id, jnp.where(turn_id == 2, top_layer, turn_id - 1)
            )

        def lend(turn_id, carry):
            which = visited(turn_id)

            @pl.when(turn_id + 1 < layers)
            def _():
                hand_layer(visited(turn_id + 1))

            @pl.when(turn_id > 0)
            def _():
                ready_layer(which)

            tops = []
            for index in range(strips):
                expand(which, 0, index, lent)
            for index in range(strips):
                cut = slice(index * strip, (index + 1) * strip)
                keys = jnp.concatenate([kn[0, cut, :128], kr[0, cut, :]], axis=1)
                scores = jnp.dot(keys, q_help[...], preferred_element_type=jnp.float32)
                scores = jnp.where(
                    hidden_keys(which * keys_wide + index * strip, guest * rows), far_below, scores
                )
                s_ref[0, cut, :] = scores
                tops.append(jnp.max(scores, axis=0, keepdims=True))
            old = run_max[0:1, :]
            top = jnp.maximum(old, functools.reduce(jnp.maximum, tops))
            fade = jnp.exp2(old - top)
            run_max[0:1, :] = top
            sums = [None] * tiles
            for index in range(strips):
                cut = slice(index * strip, (index + 1) * strip)
                weights = jnp.exp2(s_ref[0, cut, :] - top).astype(jnp.bfloat16)
                weigh(0, 0, index, weights, sums)
            for tile, (low, high) in enumerate(tile_rows):
                acc[0, tile, : high - low, :] = sums[tile] + acc[0, tile, : high - low, :] * fade[
                    :, 256 * tile : 256 * (tile + 1)
                ]
            return carry

        lax.fori_loop(0, layers, lend, 0)

        def keep(side, block):
            help_out[side * VALUE_DIM : (side + 1) * VALUE_DIM, :] = block

        finish(0, keep)
        help_copy.start()

    for index in (8, 9):
        loads[index].wait()
    for gift in gifts:
        gift.wait()
    conv_sum.wait()
    conv_copy.wait()
    conv_scale = lax.rsqrt((end_mine[...] + end_other[...])[:, :1] / CONV_CH + norm_eps)

    def product(activations, weight):
        return jnp.dot(activations, weight, preferred_element_type=jnp.float32)

    bulk = 2 * lent * VALUE_DIM
    total_width = bulk + 2 * VALUE_DIM

    def hand_in(low, high, slot):
        attended = att_t[low:high, :]
        att_act[0, :, low:high] = (attended.T * att_gain_ref[:, low:high]).astype(jnp.bfloat16)
        copy = push(
            att_act.at[0, :, pl.ds(low, high - low)],
            att_act.at[1, :, pl.ds(low, high - low)],
            att_send.at[slot],
            att_recv.at[slot],
            other,
        )
        copy.start()
        return copy, jnp.sum(attended * attended, axis=0, keepdims=True)

    def share(core, low, high):
        return product(att_act[core, :, low:high], att_w[core, low:high, :])

    bulk_copy, bulk_sq = hand_in(0, bulk, 0)
    att_sq[...] = jnp.broadcast_to(bulk_sq, att_sq.shape)
    base_part[...] = (
        product(conv_act[0], conv_w[0]) + product(conv_act[1], conv_w[1])
    ) * conv_scale
    own_part[...] = share(0, 0, bulk)
    bulk_copy.wait()
    @pl.when(me < seats - 1)
    def _():
        rim_copy.wait_send()

    def settle(step, carry):
        base = (layer - step) * PLANE
        for d in range(1, PLANE):
            plane_copy(base + spot, d).wait_send()
            core_copy(base + spot_at(d)).wait_send()

        @pl.when(layer + 1 < layers)
        def _():
            column_copy(base + spot).wait_send()

        @pl.when(step > 0)
        def _():
            core_copy(base + spot).wait_send()

        return carry

    lax.fori_loop(0, layer + 1, settle, 0)

    @pl.when(layer > 0)
    def _():
        down_copy(me, lower).wait_send()

        def settle_down(which, carry):
            down_copy(which * PLANE + spot, below).wait_send()
            return carry

        lax.fori_loop(layer + 1, top_layer, settle_down, 0)

    def settle_guest(which, carry):
        for d in range(1, PLANE):
            plane_copy(which * PLANE + spot, d).wait_send()
        for d in range(PLANE):
            core_copy(which * PLANE + spot_at(d)).wait_send()
        return carry

    @pl.when(layer == 0)
    def _():
        lax.fori_loop(1, layers, settle_guest, 0)
        help_copy.wait_send()

    @pl.when(layer == top_layer)
    def _():
        for copy in q_copies:
            copy.wait_send()

    @pl.when(layer == top_layer)
    def _():
        help_copy.wait_recv()
        att_t[bulk:total_width, :] = help_in[...].astype(jnp.float32)

    rest_copy, rest_sq = hand_in(bulk, total_width, 1)
    att_sq[...] = att_sq[...] + rest_sq
    att_sum = push(att_sq, att_sq_other, asq_send, asq_recv, other)
    att_sum.start()
    own_part[...] = own_part[...] + share(1, 0, bulk) + share(0, bulk, total_width)
    att_sum.wait()
    squares_t = jnp.broadcast_to(att_sq[:1] + att_sq_other[:1], (128, rows)).T
    att_scale = lax.rsqrt(squares_t[:, :1] / ATT_WIDTH + norm_eps)
    rest_copy.wait()
    leaves = []
    for index in range(width // 256):
        cols = slice(index * 256, (index + 1) * 256)
        out_stage[:, cols] = (
            (
                own_part[:, cols]
                + product(att_act[1, :, bulk:total_width], att_w[1, bulk:total_width, cols])
            )
            * att_scale
            + base_part[:, cols]
        ).astype(jnp.bfloat16)
        leave = pltpu.make_async_copy(
            out_stage.at[:, cols], out_ref.at[:, cols], out_sem.at[index]
        )
        leave.start()
        leaves.append(leave)

    for leave in leaves:
        leave.wait()


def angle_tables(seats, rows):
    frequency = rope_base ** (-np.arange(ROT_DIM // 2) / (ROT_DIM // 2))

    def table(positions):
        angles = frequency[:, None] * positions[None, :]
        return jnp.asarray(
            np.concatenate([np.cos(angles), np.sin(angles)], axis=0), jnp.float32
        )

    return table(np.arange(rows)), table(rows * np.arange(-(-seats // 128) * 128))


def fused(tokens, gains, matrices, taps, seats):
    rows, width = tokens.shape
    chans = taps.shape[1]
    rank = matrices[0].shape[1]
    heads = matrices[4].shape[1] // NOPE_DIM
    pairs = heads // 2
    keys_wide = PLANE * rows
    layers = seats // PLANE
    across = rank // 128
    height = rows + -(-(rows // 128) // across) * ROT_DIM
    vmem = pl.BlockSpec(memory_space=pltpu.VMEM)
    anywhere = pl.BlockSpec(memory_space=pltpu.HBM)
    dma = pltpu.SemaphoreType.DMA
    edge = 32
    bf16 = jnp.bfloat16
    f32 = jnp.float32
    value_rows = 2 * VALUE_DIM + 16
    base, seat = angle_tables(seats, rows)
    input_gain, kv_gain, ln_gain, ln_bias, att_gain, conv_gain = gains
    return pl.pallas_call(
        layer_kernel,
        out_shape=jax.ShapeDtypeStruct((rows, width), bf16),
        in_specs=[anywhere] + [vmem] * 9 + [anywhere] * 10,
        out_specs=anywhere,
        scratch_shapes=[pltpu.VMEM(matrix.shape, bf16) for matrix in matrices[:8]]
        + [
            pltpu.VMEM((2, matrix.shape[0], width), bf16) for matrix in matrices[8:]
        ]
        + [
            pltpu.VMEM(matrices[7].shape[::-1], bf16),
            pltpu.VMEM((rows, width), bf16),
            pltpu.VMEM((rows, width), bf16),
            pltpu.VMEM((rows, 2 * width), bf16),
            pltpu.VMEM((rows, rank), f32),
            pltpu.VMEM((rows, 128), f32),
            pltpu.VMEM((rows, chans), bf16),
            pltpu.VMEM((edge, chans), bf16),
            pltpu.VMEM((chans // 128, rows + edge, 128), f32),
            pltpu.VMEM((rows, chans), f32),
            pltpu.VMEM((rows, 256), f32),
            pltpu.VMEM((rows, 256), f32),
            pltpu.VMEM((seats, height, rank), bf16),
            pltpu.VMEM((pairs, 256, 2 * rows), bf16),
            pltpu.VMEM((2, keys_wide, heads * NOPE_DIM), bf16),
            pltpu.VMEM((2, keys_wide, 128), bf16),
            pltpu.VMEM((2, pairs, value_rows, keys_wide), bf16),
            pltpu.VMEM((max(pairs, 8), 2 * rows), f32),
            pltpu.VMEM((pairs, 2 * rows // 256, value_rows, 256), f32),
            pltpu.VMEM((2, keys_wide, 2 * rows), f32),
            pltpu.VMEM((heads * VALUE_DIM, rows), f32),
            pltpu.VMEM((rows, 128), f32),
            pltpu.VMEM((rows, 128), f32),
            pltpu.VMEM((8, rows), f32),
            pltpu.VMEM((8, rows), f32),
            pltpu.VMEM((2, rows, heads * VALUE_DIM), bf16),
            pltpu.VMEM((2, rows, chans), bf16),
            pltpu.VMEM((rows, width), bf16),
            pltpu.VMEM((rows, width), f32),
            pltpu.VMEM((rows, width), f32),
            dma((len(matrices),)),
            dma((2,)),
            dma((2,)),
        ]
        + [dma] * 13
        + [
            dma((2,)),
            dma((2,)),
            dma((layers,)),
            dma((layers,)),
            dma((layers, PLANE - 1)),
            dma((seats,)),
            dma((seats,)),
            dma((seats,)),
            dma((width // 256,)),
            pltpu.VMEM((256, 2 * rows), bf16),
            pltpu.VMEM((2 * VALUE_DIM, rows), bf16),
            pltpu.VMEM((2 * VALUE_DIM, rows), bf16),
            dma((3,)),
            dma((3,)),
            dma,
            dma,
        ],
        compiler_params=pltpu.CompilerParams(
            vmem_limit_bytes=60 << 20, collective_id=0, has_side_effects=True
        ),
        name="layer",
    )(tokens, input_gain, kv_gain, base, seat, taps, ln_gain, ln_bias, att_gain, conv_gain, *matrices)


def gathered_kernel(q_ref, lat_ref, kup_ref, vup_ref, o_ref, kt, vt, run_max, acc):
    heads, rows, lanes = q_ref.shape
    blocks = lat_ref.shape[0]
    rank = kup_ref.shape[1]
    nope = kup_ref.shape[0] // heads
    vdim = vup_ref.shape[0] // heads
    rot = lat_ref.shape[1] - rank
    wide = kt.shape[2]
    group = wide // rows
    me = lax.axis_index("sp")
    last = me // group
    kt[:, nope + rot :, :] = jnp.zeros((heads, lanes - nope - rot, wide), jnp.bfloat16)
    vt[:, vdim:, :] = jnp.ones((heads, lanes - vdim, wide), jnp.bfloat16)

    def expand(block):
        for part in range(group):
            src = jnp.minimum(block * group + part, blocks - 1)
            lat = lat_ref[src, :rank, :]
            turned = lat_ref[src, rank:, :]
            cols = slice(part * rows, (part + 1) * rows)
            keys = jnp.dot(kup_ref[...], lat, preferred_element_type=jnp.float32)
            values = jnp.dot(vup_ref[...], lat, preferred_element_type=jnp.float32)
            for head in range(heads):
                kt[head, :nope, cols] = keys[head * nope : (head + 1) * nope].astype(jnp.bfloat16)
                kt[head, nope : nope + rot, cols] = turned
                vt[head, :vdim, cols] = values[head * vdim : (head + 1) * vdim].astype(
                    jnp.bfloat16
                )

    def weigh(head, scores, top):
        weights = jnp.exp2(scores - top).astype(jnp.bfloat16)
        return lax.dot_general(
            weights, vt[head], (((1,), (1,)), ((), ())), preferred_element_type=jnp.float32
        )

    expand(last)
    key_pos = last * wide + lax.broadcasted_iota(jnp.int32, (rows, wide), 1)
    query_pos = me * rows + lax.broadcasted_iota(jnp.int32, (rows, wide), 0)
    hidden = key_pos > query_pos
    for head in range(heads):
        scores = jnp.dot(q_ref[head], kt[head], preferred_element_type=jnp.float32)
        scores = jnp.where(hidden, far_below, scores)
        top = jnp.max(scores, axis=1, keepdims=True)
        run_max[head] = jnp.broadcast_to(top, (rows, lanes))
        acc[head] = weigh(head, scores, top)

    def visit(step, carry):
        expand(step)
        for head in range(heads):
            scores = jnp.dot(q_ref[head], kt[head], preferred_element_type=jnp.float32)
            old = run_max[head]
            top = jnp.maximum(old[:, :1], jnp.max(scores, axis=1, keepdims=True))
            wide_top = jnp.broadcast_to(top, (rows, lanes))
            run_max[head] = wide_top
            acc[head] = acc[head] * jnp.exp2(old - wide_top) + weigh(head, scores, top)
        return carry

    lax.fori_loop(0, last, visit, 0)
    lane = lax.broadcasted_iota(jnp.int32, (rows, lanes), 1)
    for pair in range(heads // 2):
        halves = []
        for head in (2 * pair, 2 * pair + 1):
            total = acc[head]
            halves.append(total / pltpu.roll(total, vdim, axis=1))
        both = jnp.where(lane < vdim, halves[0], pltpu.roll(halves[1], vdim, axis=1))
        o_ref[:, pair * lanes : (pair + 1) * lanes] = both.astype(jnp.bfloat16)


def gathered_attention(q_heads, lat_all, key_up_t, value_up_t):
    heads, rows, lanes = q_heads.shape
    blocks = lat_all.shape[0]
    wide = 2 * rows if blocks % 2 == 0 else rows
    vmem = pl.BlockSpec(memory_space=pltpu.VMEM)
    return pl.pallas_call(
        gathered_kernel,
        out_shape=jax.ShapeDtypeStruct((rows, value_up_t.shape[0]), jnp.bfloat16),
        in_specs=[vmem] * 4,
        out_specs=vmem,
        scratch_shapes=[
            pltpu.VMEM((heads, lanes, wide), jnp.bfloat16),
            pltpu.VMEM((heads, lanes, wide), jnp.bfloat16),
            pltpu.VMEM((heads, rows, lanes), jnp.float32),
            pltpu.VMEM((heads, rows, lanes), jnp.float32),
        ],
        compiler_params=pltpu.CompilerParams(vmem_limit_bytes=48 << 20),
        cost_estimate=pl.CostEstimate(
            flops=20_000_000_000, bytes_accessed=8 << 20, transcendentals=20_000_000
        ),
        name="gathered_attention",
    )(q_heads, lat_all, key_up_t, value_up_t)


def conv_kernel(gated_ref, rim_ref, taps_ref, out_ref, wide):
    rows, chans = gated_ref.shape
    rim = rim_ref.shape[0]
    taps = taps_ref.shape[0]
    chunk = 64
    for part in range(chans // 128):
        cols = slice(part * 128, (part + 1) * 128)
        wide[part, :rim, :] = rim_ref[:, cols].astype(jnp.float32)
        wide[part, rim:, :] = gated_ref[:, cols].astype(jnp.float32)
        coeff = taps_ref[:, cols]

        def band(step, carry):
            base = step * chunk
            total = jnp.zeros((chunk, 128), jnp.float32)
            for tap in range(taps):
                total = total + coeff[tap : tap + 1, :] * wide[
                    part, pl.ds(base + (rim - taps + 1 + tap), chunk), :
                ]
            out_ref[pl.ds(pl.multiple_of(base, chunk), chunk), cols] = total
            return carry

        lax.fori_loop(0, rows // chunk, band, 0)


def convolve(gated, rim, taps):
    rows, chans = gated.shape
    vmem = pl.BlockSpec(memory_space=pltpu.VMEM)
    return pl.pallas_call(
        conv_kernel,
        out_shape=jax.ShapeDtypeStruct((rows, chans), jnp.float32),
        in_specs=[vmem] * 3,
        out_specs=vmem,
        scratch_shapes=[pltpu.VMEM((chans // 128, rows + rim.shape[0], 128), jnp.float32)],
        cost_estimate=pl.CostEstimate(
            flops=2 * rows * chans * 31, bytes_accessed=2 << 20, transcendentals=0
        ),
        name="depthwise",
    )(gated, rim, taps)


def shards(
    tokens,
    input_gain,
    query_weight,
    query_rot_weight,
    kv_down,
    rot_down,
    kv_gain,
    key_up,
    value_up,
    conv_value_weight,
    conv_gate_weight,
    conv_taps,
    conv_ln_gain,
    conv_ln_bias,
    att_out_gain,
    conv_out_gain,
    att_out_weight,
    conv_out_weight,
):
    tok_rows = tokens.shape[0]
    heads_here = key_up.shape[1] // NOPE_DIM
    chan_here = conv_taps.shape[1]
    weight_list = (
        query_weight,
        query_rot_weight,
        kv_down,
        rot_down,
        conv_value_weight,
        conv_gate_weight,
    )
    seats = lax.axis_size("sp")
    if (
        lax.axis_size("tp") == 2
        and seats % PLANE == 0
        and tok_rows % 128 == 0
        and heads_here % 2 == 0
        and heads_here > 2
        and seats > PLANE
    ):
        gains = (
            input_gain, kv_gain, conv_ln_gain, conv_ln_bias, att_out_gain, conv_out_gain
        )
        return fused(
            tokens,
            tuple(gain[None, :] for gain in gains),
            (
                kv_down, rot_down.T, conv_gate_weight, conv_value_weight, query_weight,
                query_rot_weight, key_up, value_up, att_out_weight, conv_out_weight,
            ),
            conv_taps,
            seats,
        )
    whole_rows = lax.all_gather(tokens, "tp", axis=1, tiled=True).astype(jnp.float32)
    scaled = (whole_rows * input_gain[None, :]).astype(jnp.bfloat16)
    row_scale = lax.rsqrt(jnp.mean(whole_rows * whole_rows, axis=1, keepdims=True) + norm_eps)

    def add_product(weight):
        return jnp.dot(scaled, weight, preferred_element_type=jnp.float32)

    summed = tuple((add_product(weight) for weight in weight_list))
    q_acc, qrot_acc, latent_raw, rot_acc, value_acc, gate_acc = summed
    positions = lax.axis_index("sp") * tok_rows + jnp.arange(tok_rows, dtype=jnp.int32)
    cos_table, sine_table = rotary_tables(positions, ROT_DIM // 2)
    fold = math.log2(math.e) / math.sqrt(NOPE_DIM + ROT_DIM)
    query_scale = row_scale * fold
    plain_q = (q_acc * query_scale).reshape(tok_rows, heads_here, NOPE_DIM)
    turned_q = rotate_half(
        (qrot_acc * query_scale).reshape(tok_rows, heads_here, ROT_DIM),
        cos_table[:, None, :],
        sine_table[:, None, :],
    )
    blank = jnp.zeros((tok_rows, heads_here, 128 - NOPE_DIM - ROT_DIM), jnp.float32)
    q_heads = jnp.transpose(
        jnp.concatenate([plain_q, turned_q, blank], axis=2).astype(jnp.bfloat16), (1, 0, 2)
    )
    latent = (
        latent_raw
        * lax.rsqrt(jnp.mean(latent_raw * latent_raw, axis=1, keepdims=True) + norm_eps)
        * kv_gain[None, :]
    ).astype(jnp.bfloat16)
    key_rot = rotate_half(rot_acc * row_scale, cos_table, sine_table).astype(jnp.bfloat16)
    gated_input = (value_acc * row_scale * jax.nn.sigmoid(gate_acc * row_scale)).astype(
        jnp.bfloat16
    )
    packed = jnp.concatenate([latent.T, key_rot.T], axis=0)
    rim_rows = shifted(gated_input[tok_rows - (KERNEL + 1) :], "sp", 1)
    conv_out = convolve(gated_input, rim_rows, conv_taps)
    moment_one, moment_two = lax.psum(
        (jnp.sum(conv_out, axis=1), jnp.sum(conv_out * conv_out, axis=1)), "tp"
    )
    mean_val = moment_one / CONV_CH
    spread = moment_two / CONV_CH - mean_val * mean_val
    normed = (conv_out - mean_val[:, None]) * lax.rsqrt(spread + norm_eps)[:, None]
    swished = jax.nn.silu(normed * conv_ln_gain[None, :] + conv_ln_bias[None, :])
    lat_all = lax.all_gather(packed, "sp", axis=0)
    attended = gathered_attention(q_heads, lat_all, key_up.T, value_up.T).astype(jnp.float32)
    att_sq, conv_sq = lax.psum(
        (
            jnp.sum(attended * attended, axis=1, keepdims=True),
            jnp.sum(swished * swished, axis=1, keepdims=True),
        ),
        "tp",
    )
    att_mixed = (
        attended * lax.rsqrt(att_sq / ATT_WIDTH + norm_eps) * att_out_gain[None, :]
    ).astype(jnp.bfloat16)
    conv_mixed = (
        swished * lax.rsqrt(conv_sq / CONV_CH + norm_eps) * conv_out_gain[None, :]
    ).astype(jnp.bfloat16)
    share = (
        jnp.dot(att_mixed, att_out_weight, preferred_element_type=jnp.float32)
        + jnp.dot(conv_mixed, conv_out_weight, preferred_element_type=jnp.float32)
    ).astype(jnp.bfloat16)
    return lax.psum_scatter(share, "tp", scatter_dimension=1, tiled=True)


def solution(mesh):
    return jax.shard_map(
        shards,
        mesh=mesh,
        in_specs=(
            P("sp", "tp"),
            P(),
            P(None, "tp"),
            P(None, "tp"),
            P(),
            P(),
            P(),
            P(None, "tp"),
            P(None, "tp"),
            P(None, "tp"),
            P(None, "tp"),
            P(None, "tp"),
            P("tp"),
            P("tp"),
            P("tp"),
            P("tp"),
            P("tp", None),
            P("tp", None),
        ),
        out_specs=P("sp", "tp"),
        check_vma=False,
    )
```

```python
import functools
import math

import jax
import jax.numpy as jnp
import numpy as np
from jax import lax
from jax.experimental import pallas as pl
from jax.experimental.pallas import tpu as pltpu
from jax.sharding import PartitionSpec as P

D_MODEL = 2048
NOPE_DIM = 64
ROT_DIM = 32
VALUE_DIM = 64
CONV_CH = 1024
KERNEL = 31
ATT_WIDTH = 1024


norm_eps = 1e-06
far_below = -1e30
rope_base = 10000.0


def shifted(block, axis, distance):
    devices = range(lax.axis_size(axis))
    route = [(i - distance, i) for i in devices if i - distance in devices]
    return lax.ppermute(block, axis, route)


def rotary_tables(positions, half_dim):
    frequency = rope_base ** (-jnp.arange(half_dim, dtype=jnp.float32) / half_dim)
    angles = positions.astype(jnp.float32)[:, None] * frequency[None, :]
    return (jnp.cos(angles), jnp.sin(angles))


def rotate_half(values, cos_table, sine_table):
    half_dim = cos_table.shape[-1]
    front_half = values[..., :half_dim]
    back_half = values[..., half_dim:]
    return jnp.concatenate(
        [
            front_half * cos_table - back_half * sine_table,
            back_half * cos_table + front_half * sine_table,
        ],
        axis=-1,
    )


MESH = pl.DeviceIdType.MESH


def push(src, dst, send, recv, target):
    return pltpu.make_async_remote_copy(
        src_ref=src,
        dst_ref=dst,
        send_sem=send,
        recv_sem=recv,
        device_id=target,
        device_id_type=MESH,
    )


def other_core():
    return {"sp": lax.axis_index("sp"), "tp": 1 - lax.axis_index("tp")}


PLANE = 4


FAR_FIRST = (3, 1, 2)


def layer_kernel(
    tok_hbm, gain_ref, kv_gain_ref, base_ref, seat_ref, taps_ref, ln_gain_ref, ln_bias_ref,
    att_gain_ref, conv_gain_ref,
    kvd_hbm, rotw_hbm, cgw_hbm, cvw_hbm, qw_hbm, qrw_hbm, kup_hbm, vup_hbm, att_hbm, conv_hbm,
    out_ref,
    kvd, rotw, cgw, cvw, qw, qrw, kup, vup, att_w, conv_w, vup_t,
    tok, landed, scaled, own_raw, narrow, gated, rim, wide, conv, sq_mine, sq_other,
    lat_ref, q2, kn, kr, vt, run_max, acc, s_ref, att_t, end_mine, end_other,
    att_sq, att_sq_other, att_act, conv_act, out_stage, base_part, own_part,
    w_sem, w_send, w_recv, tok_load, tok_send, tok_recv, rim_send, rim_recv, sq_send, sq_recv,
    csq_send, csq_recv, asq_send, asq_recv, conv_send, conv_recv, att_send, att_recv,
    col_send, down_send, plane_send, core_send, link_recv, core_recv, out_sem,
    q_help, help_out, help_in, qh_send, qh_recv, help_send, help_recv,
):
    mine = lax.axis_index("tp")
    me = lax.axis_index("sp")
    seats = lax.axis_size("sp")
    rows, width = tok.shape
    blocks = lat_ref.shape[0]
    rank = kvd.shape[1]
    layers = blocks // PLANE
    layer = me // PLANE
    spot = me % PLANE
    height = lat_ref.shape[1] // 2
    half = pl.ds(pl.multiple_of(mine * height, 16), height)
    other = other_core()
    ahead = {"sp": (me + 1) % seats, "tp": mine}
    behind = {"sp": (me + seats - 1) % seats, "tp": mine}

    def columns(owner):
        return pl.ds(pl.multiple_of(owner * width, 128), width)

    loads = [
        pltpu.make_async_copy(src, dst, w_sem.at[index])
        for index, (src, dst) in enumerate(
            (
                (kvd_hbm, kvd), (rotw_hbm, rotw), (cgw_hbm, cgw), (cvw_hbm, cvw),
                (qw_hbm, qw), (qrw_hbm, qrw), (kup_hbm, kup), (vup_hbm, vup),
                (att_hbm.at[:, columns(mine)], att_w.at[0]),
                (conv_hbm.at[:, columns(mine)], conv_w.at[0]),
            )
        )
    ]
    fetch = pltpu.make_async_copy(tok_hbm, tok, tok_load)
    fetch.start()
    for load in loads[:2]:
        load.start()
    gifts = [
        push(src.at[:, columns(1 - mine)], dst.at[1], w_send.at[index], w_recv.at[index], other)
        for index, (src, dst) in enumerate(((att_hbm, att_w), (conv_hbm, conv_w)))
    ]

    def spot_at(step):
        return (spot % 2 + step % 2) % 2 + 2 * ((spot // 2 + step // 2) % 2)

    def at(layer_id, spot_id):
        return {"sp": layer_id * PLANE + spot_id, "tp": mine}

    q_help[...] = jnp.zeros(q_help.shape, jnp.bfloat16)
    barrier = pltpu.get_barrier_semaphore()
    peers = [at(layer, spot_at(d)) for d in range(1, PLANE)] + [other]
    for peer in peers:
        pl.semaphore_signal(barrier, inc=1, device_id=peer, device_id_type=MESH)
    above = at(jnp.minimum(layer + 1, layers - 1), spot)
    below = at(jnp.maximum(layer - 1, 0), spot)
    top_layer = layers - 1
    opposite = at(top_layer - layer, spot)
    root = at(0, spot)
    for condition, peer in [
        (layer == 0, at(other_layer, spot)) for other_layer in range(2, layers)
    ] + [
        (layer > 1, root), (layer < layers - 1, above), (layer > 0, below), (me < seats - 1, ahead), (me > 0, behind),
    ]:

        @pl.when(condition)
        def _(peer=peer):
            pl.semaphore_signal(barrier, inc=1, device_id=peer, device_id_type=MESH)

    pairs, _, both = q2.shape
    keys_wide = kn.shape[1]
    q2[...] = jnp.zeros(q2.shape, jnp.bfloat16)
    ones_low = VALUE_DIM
    ones_high = vt.shape[2] - VALUE_DIM
    vt[:, :, ones_low:ones_high, :] = jnp.ones(
        (2, pairs, ones_high - ones_low, keys_wide), jnp.bfloat16
    )
    pl.semaphore_wait(
        barrier,
        len(peers)
        + jnp.minimum(me, 1)
        + jnp.minimum(seats - 1 - me, 1)
        + jnp.minimum(layer, 1)
        + jnp.minimum(layers - 1 - layer, 1)
        + jnp.where(layer == 0, layers - 2, jnp.where(layer > 1, 1, 0)),
    )
    fetch.wait()
    tok_copy = push(tok, landed, tok_send, tok_recv, other)
    tok_copy.start()
    for load in loads[2:]:
        load.start()

    def place(block, index):
        cols = pl.ds(pl.multiple_of(index * width, 128), width)
        full = block[...].astype(jnp.float32)
        scaled[:, cols] = (full * gain_ref[:, cols]).astype(jnp.bfloat16)
        return jnp.sum(full * full, axis=1, keepdims=True)

    squares = place(tok, mine)
    column = lax.broadcasted_iota(jnp.int32, seat_ref.shape, 1)
    seat_turn = jnp.sum(
        jnp.where(column == me, seat_ref[...], 0.0), axis=1, keepdims=True
    )
    turn = ROT_DIM // 2
    seat_cos, seat_sin = seat_turn[:turn], seat_turn[turn:]
    base_cos, base_sin = base_ref[:turn], base_ref[turn:]
    cos_table = seat_cos * base_cos - seat_sin * base_sin
    sin_table = seat_sin * base_cos + seat_cos * base_sin

    def rotate(block):
        front = block[:turn]
        back = block[turn : 2 * turn]
        return jnp.concatenate(
            [front * cos_table - back * sin_table, back * cos_table + front * sin_table], axis=0
        )

    loads[0].wait()
    own_raw[...] = jnp.dot(
        scaled[:, columns(mine)], kvd[columns(mine), :], preferred_element_type=jnp.float32
    )
    tok_copy.wait()
    squares = squares + place(landed, 1 - mine)
    row_scale = lax.rsqrt(squares / (2 * width) + norm_eps)

    def project(weight):
        return jnp.dot(scaled[...], weight[...], preferred_element_type=jnp.float32)

    loads[1].wait()
    raw = own_raw[...] + jnp.dot(
        scaled[:, columns(1 - mine)], kvd[columns(1 - mine), :], preferred_element_type=jnp.float32
    )
    latent = (
        raw
        * lax.rsqrt(jnp.mean(raw * raw, axis=1, keepdims=True) + norm_eps)
        * kv_gain_ref[...]
    )
    lat_ref[me, :rows, :] = latent.astype(jnp.bfloat16)
    narrow[...] = jnp.broadcast_to(row_scale, narrow.shape)
    key_turn = lax.dot_general(
        rotw[...], scaled[...], (((1,), (1,)), ((), ())), preferred_element_type=jnp.float32
    )
    key_rot = rotate(key_turn * narrow[...].T[:ROT_DIM]).astype(jnp.bfloat16)
    across = rank // 128
    for piece in range(across * ((rows // 128 + across - 1) // across)):
        band = rows + piece // across * ROT_DIM
        lanes = slice(piece % across * 128, piece % across * 128 + 128)
        lat_ref[me, band : band + ROT_DIM, lanes] = (
            key_rot[:, piece * 128 : piece * 128 + 128]
            if piece < rows // 128
            else jnp.zeros((ROT_DIM, 128), jnp.bfloat16)
        )

    def column_copy(block):
        spread = lat_ref.at[block, half]
        return push(spread, spread, col_send.at[block // PLANE], link_recv.at[block], above)

    def down_copy(block, target):
        spread = lat_ref.at[block, half]
        return push(spread, spread, down_send.at[block // PLANE], link_recv.at[block], target)

    lower = at(jnp.where(layer == top_layer, 0, jnp.maximum(layer - 1, 0)), spot)

    def rise(block):
        @pl.when(layer + 1 < layers)
        def _():
            column_copy(block).start()

    def plane_copy(block, distance):
        return push(
            lat_ref.at[block, half],
            lat_ref.at[block, half],
            plane_send.at[block // PLANE, distance - 1],
            link_recv.at[block],
            at(layer, spot_at(distance)),
        )

    def core_copy(block):
        spread = lat_ref.at[block, half]
        return push(spread, spread, core_send.at[block], core_recv.at[block], other)

    rise(me)

    @pl.when(layer > 0)
    def _():
        down_copy(me, lower).start()

    for d in FAR_FIRST:
        plane_copy(me, d).start()
    for gift in gifts:
        gift.start()

    def arrive(block):
        spread = lat_ref.at[block, half]
        push(spread, spread, core_send.at[block], link_recv.at[block], other).wait_recv()

    def spread_layer(which, upward):
        block = which * PLANE + spot
        arrive(block)
        if upward:
            rise(block)
        for d in FAR_FIRST:
            plane_copy(block, d).start()
        core_copy(block).start()

    def hand_layer(which):
        for d in range(1, PLANE):
            block = which * PLANE + spot_at(d)
            arrive(block)
            core_copy(block).start()

    def relay(step):
        @pl.when(step <= layer)
        def _():
            spread_layer(layer - step, True)

    def hand_over(step):
        @pl.when(step <= layer)
        def _():
            hand_layer(layer - step)

    def descend(distance):
        @pl.when((layer > 0) & (layer + distance < top_layer))
        def _():
            block = (layer + distance) * PLANE + spot
            arrive(block)
            down_copy(block, below).start()

        @pl.when((layer == 0) & (distance < layers))
        def _():
            spread_layer(distance, False)

    loads[2].wait()
    loads[3].wait()
    gate = project(cgw) * row_scale
    gated[...] = (project(cvw) * row_scale * jax.nn.sigmoid(gate)).astype(jnp.bfloat16)
    edge = rim.shape[0]
    rim_copy = push(gated.at[pl.ds(rows - edge, edge)], rim, rim_send, rim_recv, ahead)

    @pl.when(me < seats - 1)
    def _():
        rim_copy.start()

    loads[4].wait()
    loads[5].wait()
    query_scale = row_scale * (math.log2(math.e) / math.sqrt(NOPE_DIM + ROT_DIM))
    plain = (project(qw) * query_scale).T.astype(jnp.bfloat16)
    turned = (project(qrw) * query_scale).T
    for head in range(2 * pairs):
        side = head % 2
        cols = slice(side * rows, (side + 1) * rows)
        q2[head // 2, side * NOPE_DIM : (side + 1) * NOPE_DIM, cols] = plain[
            head * NOPE_DIM : (head + 1) * NOPE_DIM
        ]
        q2[head // 2, 2 * NOPE_DIM : 2 * NOPE_DIM + ROT_DIM, cols] = rotate(
            turned[head * ROT_DIM : (head + 1) * ROT_DIM]
        ).astype(jnp.bfloat16)

    lent = pairs - 1
    q_parts = tuple(
        (pl.ds(low, count), pl.ds(first_col, cols))
        for low, count, first_col, cols in (
            (0, NOPE_DIM, 0, rows),
            (NOPE_DIM, NOPE_DIM, rows, rows),
            (2 * NOPE_DIM, ROT_DIM, 0, 2 * rows),
        )
    )
    q_copies = [
        push(
            q2.at[lent, part_rows, part_cols],
            q_help.at[part_rows, part_cols],
            qh_send.at[index],
            qh_recv.at[index],
            opposite,
        )
        for index, (part_rows, part_cols) in enumerate(q_parts)
    ]

    @pl.when(layer == top_layer)
    def _():
        for copy in q_copies:
            copy.start()

    loads[7].wait()
    vup_t[...] = vup[...].astype(jnp.float32).T.astype(jnp.bfloat16)

    taps = taps_ref.shape[0]
    chunk = 64

    def band_step(step, carry, slab):
        cols = slice(slab * 128, (slab + 1) * 128)
        coeff = taps_ref[:, cols]
        base = step * chunk
        total = jnp.zeros((chunk, 128), jnp.float32)
        for tap in range(taps):
            total = total + coeff[tap : tap + 1, :] * wide[
                slab, pl.ds(base + (edge - taps + 1 + tap), chunk), :
            ]
        conv[pl.ds(pl.multiple_of(base, chunk), chunk), cols] = total
        return carry

    slabs = conv.shape[1] // 128
    for slab in range(slabs):
        wide[slab, edge:, :] = gated[:, slab * 128 : (slab + 1) * 128].astype(jnp.float32)
        lax.fori_loop(1, rows // chunk, functools.partial(band_step, slab=slab), 0)
        if slab == slabs // 2:
            relay(1)
            descend(1)
    hand_over(0)

    @pl.when(me > 0)
    def _():
        rim_copy.wait_recv()

    @pl.when(me == 0)
    def _():
        rim[...] = jnp.zeros(rim.shape, jnp.bfloat16)

    for slab in range(slabs):
        wide[slab, :edge, :] = rim[:, slab * 128 : (slab + 1) * 128].astype(jnp.float32)
        band_step(0, 0, slab)

    values = conv[...]
    for slot, total in enumerate((values, values * values)):
        sq_mine[:, slot * 128 : (slot + 1) * 128] = jnp.broadcast_to(
            jnp.sum(total, axis=1, keepdims=True), (rows, 128)
        )
    sums = push(sq_mine, sq_other, sq_send, sq_recv, other)
    sums.start()

    def activate():
        sums.wait()
        values = conv[...]
        moments = (sq_mine[...] + sq_other[...]) / CONV_CH
        mean_val = moments[:, :1]
        spread_val = moments[:, 128:129] - mean_val * mean_val
        normed = (values - mean_val) * lax.rsqrt(spread_val + norm_eps)
        swished = jax.nn.silu(normed * ln_gain_ref[...] + ln_bias_ref[...])
        conv_act[0] = (swished * conv_gain_ref[...]).astype(jnp.bfloat16)
        end_mine[...] = jnp.broadcast_to(
            jnp.sum(swished * swished, axis=1, keepdims=True), (rows, 128)
        )
        conv_sum.start()
        conv_copy.start()

    conv_sum = push(end_mine, end_other, csq_send, csq_recv, other)
    conv_copy = push(conv_act.at[0], conv_act.at[1], conv_send, conv_recv, other)

    def gathered(step):
        for d in range(1, PLANE):
            core_copy((layer - step) * PLANE + spot_at(d)).wait_recv()

    strip = 256
    strips = keys_wide // strip

    def expand(group, slot, index, only=None):
        pieces = []
        low, left = index * strip, strip
        while left > 0:
            take = min(rows - low % rows, left)
            pieces.append(
                lat_ref[group * PLANE + low // rows, low % rows : low % rows + take, :]
            )
            low, left = low + take, left - take
        lat = pieces[0] if len(pieces) == 1 else jnp.concatenate(pieces, axis=0)
        cut = slice(index * strip, (index + 1) * strip)
        some = range(pairs) if only is None else range(only, only + 1)
        key_cols = slice(2 * NOPE_DIM * some[0], 2 * NOPE_DIM * (some[-1] + 1))
        value_cols = slice(2 * VALUE_DIM * some[0], 2 * VALUE_DIM * (some[-1] + 1))
        kn[slot, cut, : 2 * NOPE_DIM * len(some)] = jnp.dot(
            lat, kup[:, key_cols], preferred_element_type=jnp.float32
        ).astype(jnp.bfloat16)
        values = lax.dot_general(
            vup_t[value_cols, :],
            lat,
            (((1,), (1,)), ((), ())),
            preferred_element_type=jnp.float32,
        ).astype(jnp.bfloat16)
        for pair in range(len(some)):
            low = 2 * VALUE_DIM * pair
            vt[slot, pair, :ones_low, cut] = values[low : low + VALUE_DIM]
            vt[slot, pair, ones_high:, cut] = values[low + VALUE_DIM : low + 2 * VALUE_DIM]
        for blk in range(index, PLANE, strips):
            pieces = []
            for piece in range(rows // 128):
                band = rows + piece // across * ROT_DIM
                lanes = slice(piece % across * 128, piece % across * 128 + 128)
                pieces.append(lat_ref[group * PLANE + blk, band : band + ROT_DIM, lanes])
            rot = jnp.concatenate(pieces, axis=1).astype(jnp.float32)
            rot = jnp.concatenate([rot, jnp.zeros((128 - ROT_DIM, rows), jnp.float32)], axis=0)
            kr[slot, blk * rows : (blk + 1) * rows, :] = rot.T.astype(jnp.bfloat16)

    tiles = both // 256
    tile_rows = tuple(
        (
            0 if 256 * tile < rows else ones_low,
            ones_high if 256 * (tile + 1) <= rows else vt.shape[2],
        )
        for tile in range(tiles)
    )

    def hidden_keys(first_key, first_query):
        key = first_key + lax.broadcasted_iota(jnp.int32, (strip, both), 0)
        query = lax.broadcasted_iota(jnp.int32, (strip, both), 1)
        return key > first_query + jnp.where(query >= rows, query - rows, query)

    def weigh(slot, place_id, index, weights, sums):
        cut = slice(index * strip, (index + 1) * strip)
        for tile, (low, high) in enumerate(tile_rows):
            new = jnp.dot(
                vt[slot, place_id, low:high, cut],
                weights[:, 256 * tile : 256 * (tile + 1)],
                preferred_element_type=jnp.float32,
            )
            sums[tile] = new if sums[tile] is None else sums[tile] + new

    def attend(slot, first, hidden, middle, following):
        def score(pair, index):
            cut = slice(index * strip, (index + 1) * strip)
            keys = jnp.concatenate(
                [kn[slot, cut, 128 * pair : 128 * pair + 128], kr[slot, cut, :]], axis=1
            )
            scores = jnp.dot(keys, q2[pair], preferred_element_type=jnp.float32)
            if hidden is not None:
                scores = jnp.where(hidden(index), far_below, scores)
            s_ref[pair % 2, cut, :] = scores
            return jnp.max(scores, axis=0, keepdims=True)

        def settle_top(pair, tops):
            top = functools.reduce(jnp.maximum, tops)
            fade = None
            if not first:
                old = run_max[pair : pair + 1, :]
                top = jnp.maximum(old, top)
                fade = jnp.exp2(old - top)
            run_max[pair : pair + 1, :] = top
            return top, fade

        def weights_of(pair, index, top):
            cut = slice(index * strip, (index + 1) * strip)
            return jnp.exp2(s_ref[pair % 2, cut, :] - top).astype(jnp.bfloat16)

        def close(pair, sums, fade):
            for tile, (low, high) in enumerate(tile_rows):
                new = sums[tile]
                if not first:
                    new = new + acc[pair, tile, : high - low, :] * fade[
                        :, 256 * tile : 256 * (tile + 1)
                    ]
                acc[pair, tile, : high - low, :] = new

        tops = [score(0, index) for index in range(strips)]
        for pair in range(lent):
            middle(pair)
            top, fade = settle_top(pair, tops)
            tops = []
            sums = [None] * tiles
            for index in range(strips):
                if pair + 1 < lent:
                    tops.append(score(pair + 1, index))
                weigh(slot, pair, index, weights_of(pair, index, top), sums)
                if pair + 1 == lent and following is not None:
                    expand(following, 1 - slot, index)
            close(pair, sums, fade)

        @pl.when(layer < top_layer)
        def _():
            top, fade = settle_top(lent, [score(lent, index) for index in range(strips)])
            sums = [None] * tiles
            for index in range(strips):
                weigh(slot, lent, index, weights_of(lent, index, top), sums)
            close(lent, sums, fade)

    def hidden(index):
        return hidden_keys(layer * keys_wide + index * strip, me * rows)

    loads[6].wait()
    gathered(0)
    for index in range(strips):
        expand(layer, 0, index)
    for distance in range(2, layers - 2):

        @pl.when(layer > 0)
        def _(distance=distance):
            descend(distance)

    @pl.when(layer == 0)
    def _():
        if layers > 2:
            descend(layers - 1)

    relay(2)


    def ready_layer(which):
        for d in range(PLANE):
            core_copy(which * PLANE + spot_at(d)).wait_recv()

    def ready(step):
        @pl.when(step <= layer)
        def _():
            ready_layer(layer - step)

    def first_middle(pair):
        if pair == 1:
            hand_over(1)


            @pl.when(layer == 0)
            def _():
                for distance in range(2, layers - 1):
                    descend(distance)

            activate()
        if pair == lent - 1:
            ready(1)

    attend(0, True, hidden, first_middle, jnp.maximum(layer - 1, 0))

    def far(step, carry):
        def middle(pair):
            if pair == 0:
                relay(step + 2)
            if pair == 1:
                hand_over(step + 1)
            if pair == lent - 1:
                ready(step + 1)

        attend(step % 2, False, None, middle, layer - step - 1)
        return carry

    lax.fori_loop(1, layer, far, 0)

    @pl.when(layer > 0)
    def _():
        attend(layer % 2, False, None, lambda pair: None, None)

    def finish(pair, keep):
        for side in range(2):
            pieces = []
            for tile, (low, high) in enumerate(tile_rows):
                start = max(side * rows, 256 * tile)
                stop = min((side + 1) * rows, 256 * (tile + 1))
                if start >= stop:
                    continue
                total = acc[pair, tile, : high - low, start - 256 * tile : stop - 256 * tile]
                base = 0 if side == 0 else ones_high - low
                pieces.append(
                    total[base : base + VALUE_DIM] / total[ones_low - low : ones_low - low + 1]
                )
            keep(side, jnp.concatenate(pieces, axis=1).astype(jnp.bfloat16))

    def keep_local(pair):
        def keep(side, block):
            low = (2 * pair + side) * VALUE_DIM
            att_t[low : low + VALUE_DIM, :] = block.astype(jnp.float32)

        return keep

    for pair in range(lent):
        finish(pair, keep_local(pair))

    @pl.when(layer < top_layer)
    def _():
        finish(lent, keep_local(lent))

    help_copy = push(help_out, help_in, help_send, help_recv, opposite)

    @pl.when(layer == 0)
    def _():
        for copy in q_copies:
            copy.wait_recv()
        run_max[0:1, :] = jnp.full((1, both), far_below, jnp.float32)
        acc[0] = jnp.zeros(acc.shape[1:], jnp.float32)
        guest = top_layer * PLANE + spot

        def visited(turn_id):
            return jnp.where(
                turn_id <= 1, turn_id, jnp.where(turn_id == 2, top_layer, turn_id - 1)
            )

        def lend(turn_id, carry):
            which = visited(turn_id)

            @pl.when(turn_id + 1 < layers)
            def _():
                hand_layer(visited(turn_id + 1))

            @pl.when(turn_id > 0)
            def _():
                ready_layer(which)

            tops = []
            for index in range(strips):
                expand(which, 0, index, lent)
            for index in range(strips):
                cut = slice(index * strip, (index + 1) * strip)
                keys = jnp.concatenate([kn[0, cut, :128], kr[0, cut, :]], axis=1)
                scores = jnp.dot(keys, q_help[...], preferred_element_type=jnp.float32)
                scores = jnp.where(
                    hidden_keys(which * keys_wide + index * strip, guest * rows), far_below, scores
                )
                s_ref[0, cut, :] = scores
                tops.append(jnp.max(scores, axis=0, keepdims=True))
            old = run_max[0:1, :]
            top = jnp.maximum(old, functools.reduce(jnp.maximum, tops))
            fade = jnp.exp2(old - top)
            run_max[0:1, :] = top
            sums = [None] * tiles
            for index in range(strips):
                cut = slice(index * strip, (index + 1) * strip)
                weights = jnp.exp2(s_ref[0, cut, :] - top).astype(jnp.bfloat16)
                weigh(0, 0, index, weights, sums)
            for tile, (low, high) in enumerate(tile_rows):
                acc[0, tile, : high - low, :] = sums[tile] + acc[0, tile, : high - low, :] * fade[
                    :, 256 * tile : 256 * (tile + 1)
                ]
            return carry

        lax.fori_loop(0, layers, lend, 0)

        def keep(side, block):
            help_out[side * VALUE_DIM : (side + 1) * VALUE_DIM, :] = block

        finish(0, keep)
        help_copy.start()

    for index in (8, 9):
        loads[index].wait()
    for gift in gifts:
        gift.wait()
    conv_sum.wait()
    conv_copy.wait()
    conv_scale = lax.rsqrt((end_mine[...] + end_other[...])[:, :1] / CONV_CH + norm_eps)

    def product(activations, weight):
        return jnp.dot(activations, weight, preferred_element_type=jnp.float32)

    bulk = 2 * lent * VALUE_DIM
    total_width = bulk + 2 * VALUE_DIM

    def hand_in(low, high, slot):
        attended = att_t[low:high, :]
        att_act[0, :, low:high] = (attended.T * att_gain_ref[:, low:high]).astype(jnp.bfloat16)
        copy = push(
            att_act.at[0, :, pl.ds(low, high - low)],
            att_act.at[1, :, pl.ds(low, high - low)],
            att_send.at[slot],
            att_recv.at[slot],
            other,
        )
        copy.start()
        return copy, jnp.sum(attended * attended, axis=0, keepdims=True)

    def share(core, low, high):
        return product(att_act[core, :, low:high], att_w[core, low:high, :])

    bulk_copy, bulk_sq = hand_in(0, bulk, 0)
    att_sq[...] = jnp.broadcast_to(bulk_sq, att_sq.shape)
    base_part[...] = (
        product(conv_act[0], conv_w[0]) + product(conv_act[1], conv_w[1])
    ) * conv_scale
    own_part[...] = share(0, 0, bulk)

    @pl.when(layer == top_layer)
    def _():
        help_copy.wait_recv()
        att_t[bulk:total_width, :] = help_in[...].astype(jnp.float32)

    rest_copy, rest_sq = hand_in(bulk, total_width, 1)
    att_sq[...] = att_sq[...] + rest_sq
    att_sum = push(att_sq, att_sq_other, asq_send, asq_recv, other)
    att_sum.start()
    bulk_copy.wait()
    own_part[...] = own_part[...] + share(1, 0, bulk) + share(0, bulk, total_width)
    att_sum.wait()
    squares_t = jnp.broadcast_to(att_sq[:1] + att_sq_other[:1], (128, rows)).T
    att_scale = lax.rsqrt(squares_t[:, :1] / ATT_WIDTH + norm_eps)
    rest_copy.wait()
    leaves = []
    for index in range(width // 256):
        cols = slice(index * 256, (index + 1) * 256)
        out_stage[:, cols] = (
            (
                own_part[:, cols]
                + product(att_act[1, :, bulk:total_width], att_w[1, bulk:total_width, cols])
            )
            * att_scale
            + base_part[:, cols]
        ).astype(jnp.bfloat16)
        leave = pltpu.make_async_copy(
            out_stage.at[:, cols], out_ref.at[:, cols], out_sem.at[index]
        )
        leave.start()
        leaves.append(leave)

    @pl.when(me < seats - 1)
    def _():
        rim_copy.wait_send()

    def settle(step, carry):
        base = (layer - step) * PLANE
        for d in range(1, PLANE):
            plane_copy(base + spot, d).wait_send()
            core_copy(base + spot_at(d)).wait_send()

        @pl.when(layer + 1 < layers)
        def _():
            column_copy(base + spot).wait_send()

        @pl.when(step > 0)
        def _():
            core_copy(base + spot).wait_send()

        return carry

    lax.fori_loop(0, layer + 1, settle, 0)

    @pl.when(layer > 0)
    def _():
        down_copy(me, lower).wait_send()

        def settle_down(which, carry):
            down_copy(which * PLANE + spot, below).wait_send()
            return carry

        lax.fori_loop(layer + 1, top_layer, settle_down, 0)

    def settle_guest(which, carry):
        for d in range(1, PLANE):
            plane_copy(which * PLANE + spot, d).wait_send()
        for d in range(PLANE):
            core_copy(which * PLANE + spot_at(d)).wait_send()
        return carry

    @pl.when(layer == 0)
    def _():
        lax.fori_loop(1, layers, settle_guest, 0)
        help_copy.wait_send()

    @pl.when(layer == top_layer)
    def _():
        for copy in q_copies:
            copy.wait_send()

    for leave in leaves:
        leave.wait()


def angle_tables(seats, rows):
    frequency = rope_base ** (-np.arange(ROT_DIM // 2) / (ROT_DIM // 2))

    def table(positions):
        angles = frequency[:, None] * positions[None, :]
        return jnp.asarray(
            np.concatenate([np.cos(angles), np.sin(angles)], axis=0), jnp.float32
        )

    return table(np.arange(rows)), table(rows * np.arange(-(-seats // 128) * 128))


def fused(tokens, gains, matrices, taps, seats):
    rows, width = tokens.shape
    chans = taps.shape[1]
    rank = matrices[0].shape[1]
    heads = matrices[4].shape[1] // NOPE_DIM
    pairs = heads // 2
    keys_wide = PLANE * rows
    layers = seats // PLANE
    across = rank // 128
    height = rows + -(-(rows // 128) // across) * ROT_DIM
    vmem = pl.BlockSpec(memory_space=pltpu.VMEM)
    anywhere = pl.BlockSpec(memory_space=pltpu.HBM)
    dma = pltpu.SemaphoreType.DMA
    edge = 32
    bf16 = jnp.bfloat16
    f32 = jnp.float32
    value_rows = 2 * VALUE_DIM + 16
    base, seat = angle_tables(seats, rows)
    input_gain, kv_gain, ln_gain, ln_bias, att_gain, conv_gain = gains
    return pl.pallas_call(
        layer_kernel,
        out_shape=jax.ShapeDtypeStruct((rows, width), bf16),
        in_specs=[anywhere] + [vmem] * 9 + [anywhere] * 10,
        out_specs=anywhere,
        scratch_shapes=[pltpu.VMEM(matrix.shape, bf16) for matrix in matrices[:8]]
        + [
            pltpu.VMEM((2, matrix.shape[0], width), bf16) for matrix in matrices[8:]
        ]
        + [
            pltpu.VMEM(matrices[7].shape[::-1], bf16),
            pltpu.VMEM((rows, width), bf16),
            pltpu.VMEM((rows, width), bf16),
            pltpu.VMEM((rows, 2 * width), bf16),
            pltpu.VMEM((rows, rank), f32),
            pltpu.VMEM((rows, 128), f32),
            pltpu.VMEM((rows, chans), bf16),
            pltpu.VMEM((edge, chans), bf16),
            pltpu.VMEM((chans // 128, rows + edge, 128), f32),
            pltpu.VMEM((rows, chans), f32),
            pltpu.VMEM((rows, 256), f32),
            pltpu.VMEM((rows, 256), f32),
            pltpu.VMEM((seats, height, rank), bf16),
            pltpu.VMEM((pairs, 256, 2 * rows), bf16),
            pltpu.VMEM((2, keys_wide, heads * NOPE_DIM), bf16),
            pltpu.VMEM((2, keys_wide, 128), bf16),
            pltpu.VMEM((2, pairs, value_rows, keys_wide), bf16),
            pltpu.VMEM((max(pairs, 8), 2 * rows), f32),
            pltpu.VMEM((pairs, 2 * rows // 256, value_rows, 256), f32),
            pltpu.VMEM((2, keys_wide, 2 * rows), f32),
            pltpu.VMEM((heads * VALUE_DIM, rows), f32),
            pltpu.VMEM((rows, 128), f32),
            pltpu.VMEM((rows, 128), f32),
            pltpu.VMEM((8, rows), f32),
            pltpu.VMEM((8, rows), f32),
            pltpu.VMEM((2, rows, heads * VALUE_DIM), bf16),
            pltpu.VMEM((2, rows, chans), bf16),
            pltpu.VMEM((rows, width), bf16),
            pltpu.VMEM((rows, width), f32),
            pltpu.VMEM((rows, width), f32),
            dma((len(matrices),)),
            dma((2,)),
            dma((2,)),
        ]
        + [dma] * 13
        + [
            dma((2,)),
            dma((2,)),
            dma((layers,)),
            dma((layers,)),
            dma((layers, PLANE - 1)),
            dma((seats,)),
            dma((seats,)),
            dma((seats,)),
            dma((width // 256,)),
            pltpu.VMEM((256, 2 * rows), bf16),
            pltpu.VMEM((2 * VALUE_DIM, rows), bf16),
            pltpu.VMEM((2 * VALUE_DIM, rows), bf16),
            dma((3,)),
            dma((3,)),
            dma,
            dma,
        ],
        compiler_params=pltpu.CompilerParams(
            vmem_limit_bytes=60 << 20, collective_id=0, has_side_effects=True
        ),
        name="layer",
    )(tokens, input_gain, kv_gain, base, seat, taps, ln_gain, ln_bias, att_gain, conv_gain, *matrices)


def gathered_kernel(q_ref, lat_ref, kup_ref, vup_ref, o_ref, kt, vt, run_max, acc):
    heads, rows, lanes = q_ref.shape
    blocks = lat_ref.shape[0]
    rank = kup_ref.shape[1]
    nope = kup_ref.shape[0] // heads
    vdim = vup_ref.shape[0] // heads
    rot = lat_ref.shape[1] - rank
    wide = kt.shape[2]
    group = wide // rows
    me = lax.axis_index("sp")
    last = me // group
    kt[:, nope + rot :, :] = jnp.zeros((heads, lanes - nope - rot, wide), jnp.bfloat16)
    vt[:, vdim:, :] = jnp.ones((heads, lanes - vdim, wide), jnp.bfloat16)

    def expand(block):
        for part in range(group):
            src = jnp.minimum(block * group + part, blocks - 1)
            lat = lat_ref[src, :rank, :]
            turned = lat_ref[src, rank:, :]
            cols = slice(part * rows, (part + 1) * rows)
            keys = jnp.dot(kup_ref[...], lat, preferred_element_type=jnp.float32)
            values = jnp.dot(vup_ref[...], lat, preferred_element_type=jnp.float32)
            for head in range(heads):
                kt[head, :nope, cols] = keys[head * nope : (head + 1) * nope].astype(jnp.bfloat16)
                kt[head, nope : nope + rot, cols] = turned
                vt[head, :vdim, cols] = values[head * vdim : (head + 1) * vdim].astype(
                    jnp.bfloat16
                )

    def weigh(head, scores, top):
        weights = jnp.exp2(scores - top).astype(jnp.bfloat16)
        return lax.dot_general(
            weights, vt[head], (((1,), (1,)), ((), ())), preferred_element_type=jnp.float32
        )

    expand(last)
    key_pos = last * wide + lax.broadcasted_iota(jnp.int32, (rows, wide), 1)
    query_pos = me * rows + lax.broadcasted_iota(jnp.int32, (rows, wide), 0)
    hidden = key_pos > query_pos
    for head in range(heads):
        scores = jnp.dot(q_ref[head], kt[head], preferred_element_type=jnp.float32)
        scores = jnp.where(hidden, far_below, scores)
        top = jnp.max(scores, axis=1, keepdims=True)
        run_max[head] = jnp.broadcast_to(top, (rows, lanes))
        acc[head] = weigh(head, scores, top)

    def visit(step, carry):
        expand(step)
        for head in range(heads):
            scores = jnp.dot(q_ref[head], kt[head], preferred_element_type=jnp.float32)
            old = run_max[head]
            top = jnp.maximum(old[:, :1], jnp.max(scores, axis=1, keepdims=True))
            wide_top = jnp.broadcast_to(top, (rows, lanes))
            run_max[head] = wide_top
            acc[head] = acc[head] * jnp.exp2(old - wide_top) + weigh(head, scores, top)
        return carry

    lax.fori_loop(0, last, visit, 0)
    lane = lax.broadcasted_iota(jnp.int32, (rows, lanes), 1)
    for pair in range(heads // 2):
        halves = []
        for head in (2 * pair, 2 * pair + 1):
            total = acc[head]
            halves.append(total / pltpu.roll(total, vdim, axis=1))
        both = jnp.where(lane < vdim, halves[0], pltpu.roll(halves[1], vdim, axis=1))
        o_ref[:, pair * lanes : (pair + 1) * lanes] = both.astype(jnp.bfloat16)


def gathered_attention(q_heads, lat_all, key_up_t, value_up_t):
    heads, rows, lanes = q_heads.shape
    blocks = lat_all.shape[0]
    wide = 2 * rows if blocks % 2 == 0 else rows
    vmem = pl.BlockSpec(memory_space=pltpu.VMEM)
    return pl.pallas_call(
        gathered_kernel,
        out_shape=jax.ShapeDtypeStruct((rows, value_up_t.shape[0]), jnp.bfloat16),
        in_specs=[vmem] * 4,
        out_specs=vmem,
        scratch_shapes=[
            pltpu.VMEM((heads, lanes, wide), jnp.bfloat16),
            pltpu.VMEM((heads, lanes, wide), jnp.bfloat16),
            pltpu.VMEM((heads, rows, lanes), jnp.float32),
            pltpu.VMEM((heads, rows, lanes), jnp.float32),
        ],
        compiler_params=pltpu.CompilerParams(vmem_limit_bytes=48 << 20),
        cost_estimate=pl.CostEstimate(
            flops=20_000_000_000, bytes_accessed=8 << 20, transcendentals=20_000_000
        ),
        name="gathered_attention",
    )(q_heads, lat_all, key_up_t, value_up_t)


def conv_kernel(gated_ref, rim_ref, taps_ref, out_ref, wide):
    rows, chans = gated_ref.shape
    rim = rim_ref.shape[0]
    taps = taps_ref.shape[0]
    chunk = 64
    for part in range(chans // 128):
        cols = slice(part * 128, (part + 1) * 128)
        wide[part, :rim, :] = rim_ref[:, cols].astype(jnp.float32)
        wide[part, rim:, :] = gated_ref[:, cols].astype(jnp.float32)
        coeff = taps_ref[:, cols]

        def band(step, carry):
            base = step * chunk
            total = jnp.zeros((chunk, 128), jnp.float32)
            for tap in range(taps):
                total = total + coeff[tap : tap + 1, :] * wide[
                    part, pl.ds(base + (rim - taps + 1 + tap), chunk), :
                ]
            out_ref[pl.ds(pl.multiple_of(base, chunk), chunk), cols] = total
            return carry

        lax.fori_loop(0, rows // chunk, band, 0)


def convolve(gated, rim, taps):
    rows, chans = gated.shape
    vmem = pl.BlockSpec(memory_space=pltpu.VMEM)
    return pl.pallas_call(
        conv_kernel,
        out_shape=jax.ShapeDtypeStruct((rows, chans), jnp.float32),
        in_specs=[vmem] * 3,
        out_specs=vmem,
        scratch_shapes=[pltpu.VMEM((chans // 128, rows + rim.shape[0], 128), jnp.float32)],
        cost_estimate=pl.CostEstimate(
            flops=2 * rows * chans * 31, bytes_accessed=2 << 20, transcendentals=0
        ),
        name="depthwise",
    )(gated, rim, taps)


def shards(
    tokens,
    input_gain,
    query_weight,
    query_rot_weight,
    kv_down,
    rot_down,
    kv_gain,
    key_up,
    value_up,
    conv_value_weight,
    conv_gate_weight,
    conv_taps,
    conv_ln_gain,
    conv_ln_bias,
    att_out_gain,
    conv_out_gain,
    att_out_weight,
    conv_out_weight,
):
    tok_rows = tokens.shape[0]
    heads_here = key_up.shape[1] // NOPE_DIM
    chan_here = conv_taps.shape[1]
    weight_list = (
        query_weight,
        query_rot_weight,
        kv_down,
        rot_down,
        conv_value_weight,
        conv_gate_weight,
    )
    seats = lax.axis_size("sp")
    if (
        lax.axis_size("tp") == 2
        and seats % PLANE == 0
        and tok_rows % 128 == 0
        and heads_here % 2 == 0
        and heads_here > 2
        and seats > PLANE
    ):
        gains = (
            input_gain, kv_gain, conv_ln_gain, conv_ln_bias, att_out_gain, conv_out_gain
        )
        return fused(
            tokens,
            tuple(gain[None, :] for gain in gains),
            (
                kv_down, rot_down.T, conv_gate_weight, conv_value_weight, query_weight,
                query_rot_weight, key_up, value_up, att_out_weight, conv_out_weight,
            ),
            conv_taps,
            seats,
        )
    whole_rows = lax.all_gather(tokens, "tp", axis=1, tiled=True).astype(jnp.float32)
    scaled = (whole_rows * input_gain[None, :]).astype(jnp.bfloat16)
    row_scale = lax.rsqrt(jnp.mean(whole_rows * whole_rows, axis=1, keepdims=True) + norm_eps)

    def add_product(weight):
        return jnp.dot(scaled, weight, preferred_element_type=jnp.float32)

    summed = tuple((add_product(weight) for weight in weight_list))
    q_acc, qrot_acc, latent_raw, rot_acc, value_acc, gate_acc = summed
    positions = lax.axis_index("sp") * tok_rows + jnp.arange(tok_rows, dtype=jnp.int32)
    cos_table, sine_table = rotary_tables(positions, ROT_DIM // 2)
    fold = math.log2(math.e) / math.sqrt(NOPE_DIM + ROT_DIM)
    query_scale = row_scale * fold
    plain_q = (q_acc * query_scale).reshape(tok_rows, heads_here, NOPE_DIM)
    turned_q = rotate_half(
        (qrot_acc * query_scale).reshape(tok_rows, heads_here, ROT_DIM),
        cos_table[:, None, :],
        sine_table[:, None, :],
    )
    blank = jnp.zeros((tok_rows, heads_here, 128 - NOPE_DIM - ROT_DIM), jnp.float32)
    q_heads = jnp.transpose(
        jnp.concatenate([plain_q, turned_q, blank], axis=2).astype(jnp.bfloat16), (1, 0, 2)
    )
    latent = (
        latent_raw
        * lax.rsqrt(jnp.mean(latent_raw * latent_raw, axis=1, keepdims=True) + norm_eps)
        * kv_gain[None, :]
    ).astype(jnp.bfloat16)
    key_rot = rotate_half(rot_acc * row_scale, cos_table, sine_table).astype(jnp.bfloat16)
    gated_input = (value_acc * row_scale * jax.nn.sigmoid(gate_acc * row_scale)).astype(
        jnp.bfloat16
    )
    packed = jnp.concatenate([latent.T, key_rot.T], axis=0)
    rim_rows = shifted(gated_input[tok_rows - (KERNEL + 1) :], "sp", 1)
    conv_out = convolve(gated_input, rim_rows, conv_taps)
    moment_one, moment_two = lax.psum(
        (jnp.sum(conv_out, axis=1), jnp.sum(conv_out * conv_out, axis=1)), "tp"
    )
    mean_val = moment_one / CONV_CH
    spread = moment_two / CONV_CH - mean_val * mean_val
    normed = (conv_out - mean_val[:, None]) * lax.rsqrt(spread + norm_eps)[:, None]
    swished = jax.nn.silu(normed * conv_ln_gain[None, :] + conv_ln_bias[None, :])
    lat_all = lax.all_gather(packed, "sp", axis=0)
    attended = gathered_attention(q_heads, lat_all, key_up.T, value_up.T).astype(jnp.float32)
    att_sq, conv_sq = lax.psum(
        (
            jnp.sum(attended * attended, axis=1, keepdims=True),
            jnp.sum(swished * swished, axis=1, keepdims=True),
        ),
        "tp",
    )
    att_mixed = (
        attended * lax.rsqrt(att_sq / ATT_WIDTH + norm_eps) * att_out_gain[None, :]
    ).astype(jnp.bfloat16)
    conv_mixed = (
        swished * lax.rsqrt(conv_sq / CONV_CH + norm_eps) * conv_out_gain[None, :]
    ).astype(jnp.bfloat16)
    share = (
        jnp.dot(att_mixed, att_out_weight, preferred_element_type=jnp.float32)
        + jnp.dot(conv_mixed, conv_out_weight, preferred_element_type=jnp.float32)
    ).astype(jnp.bfloat16)
    return lax.psum_scatter(share, "tp", scatter_dimension=1, tiled=True)


def solution(mesh):
    return jax.shard_map(
        shards,
        mesh=mesh,
        in_specs=(
            P("sp", "tp"),
            P(),
            P(None, "tp"),
            P(None, "tp"),
            P(),
            P(),
            P(),
            P(None, "tp"),
            P(None, "tp"),
            P(None, "tp"),
            P(None, "tp"),
            P(None, "tp"),
            P("tp"),
            P("tp"),
            P("tp"),
            P("tp"),
            P("tp", None),
            P("tp", None),
        ),
        out_specs=P("sp", "tp"),
        check_vma=False,
    )
```

```python
import functools
import math

import jax
import jax.numpy as jnp
import numpy as np
from jax import lax
from jax.experimental import pallas as pl
from jax.experimental.pallas import tpu as pltpu
from jax.sharding import PartitionSpec as P

D_MODEL = 2048
NOPE_DIM = 64
ROT_DIM = 32
VALUE_DIM = 64
CONV_CH = 1024
KERNEL = 31
ATT_WIDTH = 1024


norm_eps = 1e-06
far_below = -1e30
rope_base = 10000.0


def shifted(block, axis, distance):
    devices = range(lax.axis_size(axis))
    route = [(i - distance, i) for i in devices if i - distance in devices]
    return lax.ppermute(block, axis, route)


def rotary_tables(positions, half_dim):
    frequency = rope_base ** (-jnp.arange(half_dim, dtype=jnp.float32) / half_dim)
    angles = positions.astype(jnp.float32)[:, None] * frequency[None, :]
    return (jnp.cos(angles), jnp.sin(angles))


def rotate_half(values, cos_table, sine_table):
    half_dim = cos_table.shape[-1]
    front_half = values[..., :half_dim]
    back_half = values[..., half_dim:]
    return jnp.concatenate(
        [
            front_half * cos_table - back_half * sine_table,
            back_half * cos_table + front_half * sine_table,
        ],
        axis=-1,
    )


MESH = pl.DeviceIdType.MESH


def push(src, dst, send, recv, target):
    return pltpu.make_async_remote_copy(
        src_ref=src,
        dst_ref=dst,
        send_sem=send,
        recv_sem=recv,
        device_id=target,
        device_id_type=MESH,
    )


def other_core():
    return {"sp": lax.axis_index("sp"), "tp": 1 - lax.axis_index("tp")}


PLANE = 4


FAR_FIRST = (3, 1, 2)


def layer_kernel(
    tok_hbm, gain_ref, kv_gain_ref, base_ref, seat_ref, taps_ref, ln_gain_ref, ln_bias_ref,
    att_gain_ref, conv_gain_ref,
    kvd_hbm, rotw_hbm, cgw_hbm, cvw_hbm, qw_hbm, qrw_hbm, kup_hbm, vup_hbm, att_hbm, conv_hbm,
    out_ref,
    kvd, rotw, cgw, cvw, qw, qrw, kup, vup, att_w, conv_w, vup_t,
    tok, landed, scaled, own_raw, narrow, gated, rim, wide, conv, sq_mine, sq_other,
    lat_ref, q2, kn, kr, vt, run_max, acc, s_ref, att_t, end_mine, end_other,
    att_sq, att_sq_other, att_act, conv_act, out_stage, base_part, own_part,
    w_sem, w_send, w_recv, tok_load, tok_send, tok_recv, rim_send, rim_recv, sq_send, sq_recv,
    csq_send, csq_recv, asq_send, asq_recv, conv_send, conv_recv, att_send, att_recv,
    col_send, down_send, plane_send, core_send, link_recv, core_recv, out_sem,
    q_help, help_out, help_in, qh_send, qh_recv, help_send, help_recv,
):
    mine = lax.axis_index("tp")
    me = lax.axis_index("sp")
    seats = lax.axis_size("sp")
    rows, width = tok.shape
    blocks = lat_ref.shape[0]
    rank = kvd.shape[1]
    layers = blocks // PLANE
    layer = me // PLANE
    spot = me % PLANE
    height = lat_ref.shape[1] // 2
    half = pl.ds(pl.multiple_of(mine * height, 16), height)
    other = other_core()
    ahead = {"sp": (me + 1) % seats, "tp": mine}
    behind = {"sp": (me + seats - 1) % seats, "tp": mine}

    def columns(owner):
        return pl.ds(pl.multiple_of(owner * width, 128), width)

    loads = [
        pltpu.make_async_copy(src, dst, w_sem.at[index])
        for index, (src, dst) in enumerate(
            (
                (kvd_hbm, kvd), (rotw_hbm, rotw), (cgw_hbm, cgw), (cvw_hbm, cvw),
                (qw_hbm, qw), (qrw_hbm, qrw), (kup_hbm, kup), (vup_hbm, vup),
                (att_hbm.at[:, columns(mine)], att_w.at[0]),
                (conv_hbm.at[:, columns(mine)], conv_w.at[0]),
            )
        )
    ]
    fetch = pltpu.make_async_copy(tok_hbm, tok, tok_load)
    fetch.start()
    for load in loads[:2]:
        load.start()
    gifts = [
        push(src.at[:, columns(1 - mine)], dst.at[1], w_send.at[index], w_recv.at[index], other)
        for index, (src, dst) in enumerate(((att_hbm, att_w), (conv_hbm, conv_w)))
    ]

    def spot_at(step):
        return (spot % 2 + step % 2) % 2 + 2 * ((spot // 2 + step // 2) % 2)

    def at(layer_id, spot_id):
        return {"sp": layer_id * PLANE + spot_id, "tp": mine}

    q_help[...] = jnp.zeros(q_help.shape, jnp.bfloat16)
    barrier = pltpu.get_barrier_semaphore()
    peers = [at(layer, spot_at(d)) for d in range(1, PLANE)] + [other]
    for peer in peers:
        pl.semaphore_signal(barrier, inc=1, device_id=peer, device_id_type=MESH)
    above = at(jnp.minimum(layer + 1, layers - 1), spot)
    below = at(jnp.maximum(layer - 1, 0), spot)
    top_layer = layers - 1
    opposite = at(top_layer - layer, spot)
    root = at(0, spot)
    for condition, peer in [
        (layer == 0, at(other_layer, spot)) for other_layer in range(2, layers)
    ] + [
        (layer > 1, root), (layer < layers - 1, above), (layer > 0, below), (me < seats - 1, ahead), (me > 0, behind),
    ]:

        @pl.when(condition)
        def _(peer=peer):
            pl.semaphore_signal(barrier, inc=1, device_id=peer, device_id_type=MESH)

    pairs, _, both = q2.shape
    keys_wide = kn.shape[1]
    q2[...] = jnp.zeros(q2.shape, jnp.bfloat16)
    ones_low = VALUE_DIM
    ones_high = vt.shape[2] - VALUE_DIM
    vt[:, :, ones_low:ones_high, :] = jnp.ones(
        (2, pairs, ones_high - ones_low, keys_wide), jnp.bfloat16
    )
    pl.semaphore_wait(
        barrier,
        len(peers)
        + jnp.minimum(me, 1)
        + jnp.minimum(seats - 1 - me, 1)
        + jnp.minimum(layer, 1)
        + jnp.minimum(layers - 1 - layer, 1)
        + jnp.where(layer == 0, layers - 2, jnp.where(layer > 1, 1, 0)),
    )
    fetch.wait()
    tok_copy = push(tok, landed, tok_send, tok_recv, other)
    tok_copy.start()
    for load in loads[2:]:
        load.start()

    def place(block, index):
        cols = pl.ds(pl.multiple_of(index * width, 128), width)
        full = block[...].astype(jnp.float32)
        scaled[:, cols] = (full * gain_ref[:, cols]).astype(jnp.bfloat16)
        return jnp.sum(full * full, axis=1, keepdims=True)

    squares = place(tok, mine)
    column = lax.broadcasted_iota(jnp.int32, seat_ref.shape, 1)
    seat_turn = jnp.sum(
        jnp.where(column == me, seat_ref[...], 0.0), axis=1, keepdims=True
    )
    turn = ROT_DIM // 2
    seat_cos, seat_sin = seat_turn[:turn], seat_turn[turn:]
    base_cos, base_sin = base_ref[:turn], base_ref[turn:]
    cos_table = seat_cos * base_cos - seat_sin * base_sin
    sin_table = seat_sin * base_cos + seat_cos * base_sin

    def rotate(block):
        front = block[:turn]
        back = block[turn : 2 * turn]
        return jnp.concatenate(
            [front * cos_table - back * sin_table, back * cos_table + front * sin_table], axis=0
        )

    loads[0].wait()
    own_raw[...] = jnp.dot(
        scaled[:, columns(mine)], kvd[columns(mine), :], preferred_element_type=jnp.float32
    )
    tok_copy.wait()
    squares = squares + place(landed, 1 - mine)
    row_scale = lax.rsqrt(squares / (2 * width) + norm_eps)

    def project(weight):
        return jnp.dot(scaled[...], weight[...], preferred_element_type=jnp.float32)

    loads[1].wait()
    raw = own_raw[...] + jnp.dot(
        scaled[:, columns(1 - mine)], kvd[columns(1 - mine), :], preferred_element_type=jnp.float32
    )
    latent = (
        raw
        * lax.rsqrt(jnp.mean(raw * raw, axis=1, keepdims=True) + norm_eps)
        * kv_gain_ref[...]
    )
    lat_ref[me, :rows, :] = latent.astype(jnp.bfloat16)
    narrow[...] = jnp.broadcast_to(row_scale, narrow.shape)
    key_turn = lax.dot_general(
        rotw[...], scaled[...], (((1,), (1,)), ((), ())), preferred_element_type=jnp.float32
    )
    key_rot = rotate(key_turn * narrow[...].T[:ROT_DIM]).astype(jnp.bfloat16)
    across = rank // 128
    for piece in range(across * ((rows // 128 + across - 1) // across)):
        band = rows + piece // across * ROT_DIM
        lanes = slice(piece % across * 128, piece % across * 128 + 128)
        lat_ref[me, band : band + ROT_DIM, lanes] = (
            key_rot[:, piece * 128 : piece * 128 + 128]
            if piece < rows // 128
            else jnp.zeros((ROT_DIM, 128), jnp.bfloat16)
        )

    def column_copy(block):
        spread = lat_ref.at[block, half]
        return push(spread, spread, col_send.at[block // PLANE], link_recv.at[block], above)

    def down_copy(block, target):
        spread = lat_ref.at[block, half]
        return push(spread, spread, down_send.at[block // PLANE], link_recv.at[block], target)

    lower = at(jnp.where(layer == top_layer, 0, jnp.maximum(layer - 1, 0)), spot)

    def rise(block):
        @pl.when(layer + 1 < layers)
        def _():
            column_copy(block).start()

    def plane_copy(block, distance):
        return push(
            lat_ref.at[block, half],
            lat_ref.at[block, half],
            plane_send.at[block // PLANE, distance - 1],
            link_recv.at[block],
            at(layer, spot_at(distance)),
        )

    def core_copy(block):
        spread = lat_ref.at[block, half]
        return push(spread, spread, core_send.at[block], core_recv.at[block], other)

    rise(me)

    @pl.when(layer > 0)
    def _():
        down_copy(me, lower).start()

    for d in FAR_FIRST:
        plane_copy(me, d).start()
    for gift in gifts:
        gift.start()

    def arrive(block):
        spread = lat_ref.at[block, half]
        push(spread, spread, core_send.at[block], link_recv.at[block], other).wait_recv()

    def spread_layer(which, upward):
        block = which * PLANE + spot
        arrive(block)
        if upward:
            rise(block)
        for d in FAR_FIRST:
            plane_copy(block, d).start()
        core_copy(block).start()

    def hand_layer(which):
        for d in range(1, PLANE):
            block = which * PLANE + spot_at(d)
            arrive(block)
            core_copy(block).start()

    def relay(step):
        @pl.when(step <= layer)
        def _():
            spread_layer(layer - step, True)

    def hand_over(step):
        @pl.when(step <= layer)
        def _():
            hand_layer(layer - step)

    def descend(distance):
        @pl.when((layer > 0) & (layer + distance < top_layer))
        def _():
            block = (layer + distance) * PLANE + spot
            arrive(block)
            down_copy(block, below).start()

        @pl.when((layer == 0) & (distance < layers))
        def _():
            spread_layer(distance, False)

    loads[2].wait()
    loads[3].wait()
    gate = project(cgw) * row_scale
    gated[...] = (project(cvw) * row_scale * jax.nn.sigmoid(gate)).astype(jnp.bfloat16)
    edge = rim.shape[0]
    rim_copy = push(gated.at[pl.ds(rows - edge, edge)], rim, rim_send, rim_recv, ahead)

    @pl.when(me < seats - 1)
    def _():
        rim_copy.start()

    loads[4].wait()
    loads[5].wait()
    query_scale = row_scale * (math.log2(math.e) / math.sqrt(NOPE_DIM + ROT_DIM))
    plain = (project(qw) * query_scale).T.astype(jnp.bfloat16)
    turned = (project(qrw) * query_scale).T
    for head in range(2 * pairs):
        side = head % 2
        cols = slice(side * rows, (side + 1) * rows)
        q2[head // 2, side * NOPE_DIM : (side + 1) * NOPE_DIM, cols] = plain[
            head * NOPE_DIM : (head + 1) * NOPE_DIM
        ]
        q2[head // 2, 2 * NOPE_DIM : 2 * NOPE_DIM + ROT_DIM, cols] = rotate(
            turned[head * ROT_DIM : (head + 1) * ROT_DIM]
        ).astype(jnp.bfloat16)

    lent = pairs - 1
    q_parts = tuple(
        (pl.ds(low, count), pl.ds(first_col, cols))
        for low, count, first_col, cols in (
            (0, NOPE_DIM, 0, rows),
            (NOPE_DIM, NOPE_DIM, rows, rows),
            (2 * NOPE_DIM, ROT_DIM, 0, 2 * rows),
        )
    )
    q_copies = [
        push(
            q2.at[lent, part_rows, part_cols],
            q_help.at[part_rows, part_cols],
            qh_send.at[index],
            qh_recv.at[index],
            opposite,
        )
        for index, (part_rows, part_cols) in enumerate(q_parts)
    ]

    loads[7].wait()
    vup_t[...] = vup[...].astype(jnp.float32).T.astype(jnp.bfloat16)

    taps = taps_ref.shape[0]
    chunk = 64

    def band_step(step, carry, slab):
        cols = slice(slab * 128, (slab + 1) * 128)
        coeff = taps_ref[:, cols]
        base = step * chunk
        total = jnp.zeros((chunk, 128), jnp.float32)
        for tap in range(taps):
            total = total + coeff[tap : tap + 1, :] * wide[
                slab, pl.ds(base + (edge - taps + 1 + tap), chunk), :
            ]
        conv[pl.ds(pl.multiple_of(base, chunk), chunk), cols] = total
        return carry

    slabs = conv.shape[1] // 128
    for slab in range(slabs):
        wide[slab, edge:, :] = gated[:, slab * 128 : (slab + 1) * 128].astype(jnp.float32)
        lax.fori_loop(1, rows // chunk, functools.partial(band_step, slab=slab), 0)
        if slab == slabs // 2:
            relay(1)
            descend(1)
    hand_over(0)

    @pl.when(layer == top_layer)
    def _():
        for copy in q_copies:
            copy.start()

    @pl.when(me > 0)
    def _():
        rim_copy.wait_recv()

    @pl.when(me == 0)
    def _():
        rim[...] = jnp.zeros(rim.shape, jnp.bfloat16)

    for slab in range(slabs):
        wide[slab, :edge, :] = rim[:, slab * 128 : (slab + 1) * 128].astype(jnp.float32)
        band_step(0, 0, slab)

    values = conv[...]
    for slot, total in enumerate((values, values * values)):
        sq_mine[:, slot * 128 : (slot + 1) * 128] = jnp.broadcast_to(
            jnp.sum(total, axis=1, keepdims=True), (rows, 128)
        )
    sums = push(sq_mine, sq_other, sq_send, sq_recv, other)
    sums.start()

    def activate():
        sums.wait()
        values = conv[...]
        moments = (sq_mine[...] + sq_other[...]) / CONV_CH
        mean_val = moments[:, :1]
        spread_val = moments[:, 128:129] - mean_val * mean_val
        normed = (values - mean_val) * lax.rsqrt(spread_val + norm_eps)
        swished = jax.nn.silu(normed * ln_gain_ref[...] + ln_bias_ref[...])
        conv_act[0] = (swished * conv_gain_ref[...]).astype(jnp.bfloat16)
        end_mine[...] = jnp.broadcast_to(
            jnp.sum(swished * swished, axis=1, keepdims=True), (rows, 128)
        )
        conv_sum.start()
        conv_copy.start()

    conv_sum = push(end_mine, end_other, csq_send, csq_recv, other)
    conv_copy = push(conv_act.at[0], conv_act.at[1], conv_send, conv_recv, other)

    def gathered(step):
        for d in range(1, PLANE):
            core_copy((layer - step) * PLANE + spot_at(d)).wait_recv()

    strip = 256
    strips = keys_wide // strip

    def expand(group, slot, index, only=None):
        pieces = []
        low, left = index * strip, strip
        while left > 0:
            take = min(rows - low % rows, left)
            pieces.append(
                lat_ref[group * PLANE + low // rows, low % rows : low % rows + take, :]
            )
            low, left = low + take, left - take
        lat = pieces[0] if len(pieces) == 1 else jnp.concatenate(pieces, axis=0)
        cut = slice(index * strip, (index + 1) * strip)
        some = range(pairs) if only is None else range(only, only + 1)
        key_cols = slice(2 * NOPE_DIM * some[0], 2 * NOPE_DIM * (some[-1] + 1))
        value_cols = slice(2 * VALUE_DIM * some[0], 2 * VALUE_DIM * (some[-1] + 1))
        kn[slot, cut, : 2 * NOPE_DIM * len(some)] = jnp.dot(
            lat, kup[:, key_cols], preferred_element_type=jnp.float32
        ).astype(jnp.bfloat16)
        values = lax.dot_general(
            vup_t[value_cols, :],
            lat,
            (((1,), (1,)), ((), ())),
            preferred_element_type=jnp.float32,
        ).astype(jnp.bfloat16)
        for pair in range(len(some)):
            low = 2 * VALUE_DIM * pair
            vt[slot, pair, :ones_low, cut] = values[low : low + VALUE_DIM]
            vt[slot, pair, ones_high:, cut] = values[low + VALUE_DIM : low + 2 * VALUE_DIM]
        for blk in range(index, PLANE, strips):
            pieces = []
            for piece in range(rows // 128):
                band = rows + piece // across * ROT_DIM
                lanes = slice(piece % across * 128, piece % across * 128 + 128)
                pieces.append(lat_ref[group * PLANE + blk, band : band + ROT_DIM, lanes])
            rot = jnp.concatenate(pieces, axis=1).astype(jnp.float32)
            rot = jnp.concatenate([rot, jnp.zeros((128 - ROT_DIM, rows), jnp.float32)], axis=0)
            kr[slot, blk * rows : (blk + 1) * rows, :] = rot.T.astype(jnp.bfloat16)

    tiles = both // 256
    tile_rows = tuple(
        (
            0 if 256 * tile < rows else ones_low,
            ones_high if 256 * (tile + 1) <= rows else vt.shape[2],
        )
        for tile in range(tiles)
    )

    def hidden_keys(first_key, first_query):
        key = first_key + lax.broadcasted_iota(jnp.int32, (strip, both), 0)
        query = lax.broadcasted_iota(jnp.int32, (strip, both), 1)
        return key > first_query + jnp.where(query >= rows, query - rows, query)

    def weigh(slot, place_id, index, weights, sums):
        cut = slice(index * strip, (index + 1) * strip)
        for tile, (low, high) in enumerate(tile_rows):
            new = jnp.dot(
                vt[slot, place_id, low:high, cut],
                weights[:, 256 * tile : 256 * (tile + 1)],
                preferred_element_type=jnp.float32,
            )
            sums[tile] = new if sums[tile] is None else sums[tile] + new

    def attend(slot, first, hidden, middle, following):
        def score(pair, index):
            cut = slice(index * strip, (index + 1) * strip)
            keys = jnp.concatenate(
                [kn[slot, cut, 128 * pair : 128 * pair + 128], kr[slot, cut, :]], axis=1
            )
            scores = jnp.dot(keys, q2[pair], preferred_element_type=jnp.float32)
            if hidden is not None:
                scores = jnp.where(hidden(index), far_below, scores)
            s_ref[pair % 2, cut, :] = scores
            return jnp.max(scores, axis=0, keepdims=True)

        def settle_top(pair, tops):
            top = functools.reduce(jnp.maximum, tops)
            fade = None
            if not first:
                old = run_max[pair : pair + 1, :]
                top = jnp.maximum(old, top)
                fade = jnp.exp2(old - top)
            run_max[pair : pair + 1, :] = top
            return top, fade

        def weights_of(pair, index, top):
            cut = slice(index * strip, (index + 1) * strip)
            return jnp.exp2(s_ref[pair % 2, cut, :] - top).astype(jnp.bfloat16)

        def close(pair, sums, fade):
            for tile, (low, high) in enumerate(tile_rows):
                new = sums[tile]
                if not first:
                    new = new + acc[pair, tile, : high - low, :] * fade[
                        :, 256 * tile : 256 * (tile + 1)
                    ]
                acc[pair, tile, : high - low, :] = new

        tops = [score(0, index) for index in range(strips)]
        for pair in range(lent):
            middle(pair)
            top, fade = settle_top(pair, tops)
            tops = []
            sums = [None] * tiles
            for index in range(strips):
                if pair + 1 < lent:
                    tops.append(score(pair + 1, index))
                weigh(slot, pair, index, weights_of(pair, index, top), sums)
                if pair + 1 == lent and following is not None:
                    expand(following, 1 - slot, index)
            close(pair, sums, fade)

        @pl.when(layer < top_layer)
        def _():
            top, fade = settle_top(lent, [score(lent, index) for index in range(strips)])
            sums = [None] * tiles
            for index in range(strips):
                weigh(slot, lent, index, weights_of(lent, index, top), sums)
            close(lent, sums, fade)

    def hidden(index):
        return hidden_keys(layer * keys_wide + index * strip, me * rows)

    loads[6].wait()
    gathered(0)
    for index in range(strips):
        expand(layer, 0, index)
    for distance in range(2, layers - 2):

        @pl.when(layer > 0)
        def _(distance=distance):
            descend(distance)

    @pl.when(layer == 0)
    def _():
        if layers > 2:
            descend(layers - 1)

    relay(2)


    def ready_layer(which):
        for d in range(PLANE):
            core_copy(which * PLANE + spot_at(d)).wait_recv()

    def ready(step):
        @pl.when(step <= layer)
        def _():
            ready_layer(layer - step)

    def first_middle(pair):
        if pair == 1:
            hand_over(1)


            @pl.when(layer == 0)
            def _():
                for distance in range(2, layers - 1):
                    descend(distance)

            activate()
        if pair == lent - 1:
            ready(1)

    attend(0, True, hidden, first_middle, jnp.maximum(layer - 1, 0))

    def far(step, carry):
        def middle(pair):
            if pair == 0:
                relay(step + 2)
            if pair == 1:
                hand_over(step + 1)
            if pair == lent - 1:
                ready(step + 1)

        attend(step % 2, False, None, middle, layer - step - 1)
        return carry

    lax.fori_loop(1, layer, far, 0)

    @pl.when(layer > 0)
    def _():
        attend(layer % 2, False, None, lambda pair: None, None)

    def finish(pair, keep):
        for side in range(2):
            pieces = []
            for tile, (low, high) in enumerate(tile_rows):
                start = max(side * rows, 256 * tile)
                stop = min((side + 1) * rows, 256 * (tile + 1))
                if start >= stop:
                    continue
                total = acc[pair, tile, : high - low, start - 256 * tile : stop - 256 * tile]
                base = 0 if side == 0 else ones_high - low
                pieces.append(
                    total[base : base + VALUE_DIM] / total[ones_low - low : ones_low - low + 1]
                )
            keep(side, jnp.concatenate(pieces, axis=1).astype(jnp.bfloat16))

    def keep_local(pair):
        def keep(side, block):
            low = (2 * pair + side) * VALUE_DIM
            att_t[low : low + VALUE_DIM, :] = block.astype(jnp.float32)

        return keep

    for pair in range(lent):
        finish(pair, keep_local(pair))

    @pl.when(layer < top_layer)
    def _():
        finish(lent, keep_local(lent))

    help_copy = push(help_out, help_in, help_send, help_recv, opposite)

    @pl.when(layer == 0)
    def _():
        for copy in q_copies:
            copy.wait_recv()
        run_max[0:1, :] = jnp.full((1, both), far_below, jnp.float32)
        acc[0] = jnp.zeros(acc.shape[1:], jnp.float32)
        guest = top_layer * PLANE + spot

        def visited(turn_id):
            return jnp.where(
                turn_id <= 1, turn_id, jnp.where(turn_id == 2, top_layer, turn_id - 1)
            )

        def lend(turn_id, carry):
            which = visited(turn_id)

            @pl.when(turn_id + 1 < layers)
            def _():
                hand_layer(visited(turn_id + 1))

            @pl.when(turn_id > 0)
            def _():
                ready_layer(which)

            tops = []
            for index in range(strips):
                expand(which, 0, index, lent)
            for index in range(strips):
                cut = slice(index * strip, (index + 1) * strip)
                keys = jnp.concatenate([kn[0, cut, :128], kr[0, cut, :]], axis=1)
                scores = jnp.dot(keys, q_help[...], preferred_element_type=jnp.float32)
                scores = jnp.where(
                    hidden_keys(which * keys_wide + index * strip, guest * rows), far_below, scores
                )
                s_ref[0, cut, :] = scores
                tops.append(jnp.max(scores, axis=0, keepdims=True))
            old = run_max[0:1, :]
            top = jnp.maximum(old, functools.reduce(jnp.maximum, tops))
            fade = jnp.exp2(old - top)
            run_max[0:1, :] = top
            sums = [None] * tiles
            for index in range(strips):
                cut = slice(index * strip, (index + 1) * strip)
                weights = jnp.exp2(s_ref[0, cut, :] - top).astype(jnp.bfloat16)
                weigh(0, 0, index, weights, sums)
            for tile, (low, high) in enumerate(tile_rows):
                acc[0, tile, : high - low, :] = sums[tile] + acc[0, tile, : high - low, :] * fade[
                    :, 256 * tile : 256 * (tile + 1)
                ]
            return carry

        lax.fori_loop(0, layers, lend, 0)

        def keep(side, block):
            help_out[side * VALUE_DIM : (side + 1) * VALUE_DIM, :] = block

        finish(0, keep)
        help_copy.start()

    for index in (8, 9):
        loads[index].wait()
    for gift in gifts:
        gift.wait()
    conv_sum.wait()
    conv_copy.wait()
    conv_scale = lax.rsqrt((end_mine[...] + end_other[...])[:, :1] / CONV_CH + norm_eps)

    def product(activations, weight):
        return jnp.dot(activations, weight, preferred_element_type=jnp.float32)

    bulk = 2 * lent * VALUE_DIM
    total_width = bulk + 2 * VALUE_DIM

    def hand_in(low, high, slot):
        attended = att_t[low:high, :]
        att_act[0, :, low:high] = (attended.T * att_gain_ref[:, low:high]).astype(jnp.bfloat16)
        copy = push(
            att_act.at[0, :, pl.ds(low, high - low)],
            att_act.at[1, :, pl.ds(low, high - low)],
            att_send.at[slot],
            att_recv.at[slot],
            other,
        )
        copy.start()
        return copy, jnp.sum(attended * attended, axis=0, keepdims=True)

    def share(core, low, high):
        return product(att_act[core, :, low:high], att_w[core, low:high, :])

    bulk_copy, bulk_sq = hand_in(0, bulk, 0)
    att_sq[...] = jnp.broadcast_to(bulk_sq, att_sq.shape)
    base_part[...] = (
        product(conv_act[0], conv_w[0]) + product(conv_act[1], conv_w[1])
    ) * conv_scale
    own_part[...] = share(0, 0, bulk)

    @pl.when(layer == top_layer)
    def _():
        help_copy.wait_recv()
        att_t[bulk:total_width, :] = help_in[...].astype(jnp.float32)

    rest_copy, rest_sq = hand_in(bulk, total_width, 1)
    att_sq[...] = att_sq[...] + rest_sq
    att_sum = push(att_sq, att_sq_other, asq_send, asq_recv, other)
    att_sum.start()
    bulk_copy.wait()
    own_part[...] = own_part[...] + share(1, 0, bulk) + share(0, bulk, total_width)
    att_sum.wait()
    squares_t = jnp.broadcast_to(att_sq[:1] + att_sq_other[:1], (128, rows)).T
    att_scale = lax.rsqrt(squares_t[:, :1] / ATT_WIDTH + norm_eps)
    rest_copy.wait()
    leaves = []
    for index in range(width // 256):
        cols = slice(index * 256, (index + 1) * 256)
        out_stage[:, cols] = (
            (
                own_part[:, cols]
                + product(att_act[1, :, bulk:total_width], att_w[1, bulk:total_width, cols])
            )
            * att_scale
            + base_part[:, cols]
        ).astype(jnp.bfloat16)
        leave = pltpu.make_async_copy(
            out_stage.at[:, cols], out_ref.at[:, cols], out_sem.at[index]
        )
        leave.start()
        leaves.append(leave)

    @pl.when(me < seats - 1)
    def _():
        rim_copy.wait_send()

    def settle(step, carry):
        base = (layer - step) * PLANE
        for d in range(1, PLANE):
            plane_copy(base + spot, d).wait_send()
            core_copy(base + spot_at(d)).wait_send()

        @pl.when(layer + 1 < layers)
        def _():
            column_copy(base + spot).wait_send()

        @pl.when(step > 0)
        def _():
            core_copy(base + spot).wait_send()

        return carry

    lax.fori_loop(0, layer + 1, settle, 0)

    @pl.when(layer > 0)
    def _():
        down_copy(me, lower).wait_send()

        def settle_down(which, carry):
            down_copy(which * PLANE + spot, below).wait_send()
            return carry

        lax.fori_loop(layer + 1, top_layer, settle_down, 0)

    def settle_guest(which, carry):
        for d in range(1, PLANE):
            plane_copy(which * PLANE + spot, d).wait_send()
        for d in range(PLANE):
            core_copy(which * PLANE + spot_at(d)).wait_send()
        return carry

    @pl.when(layer == 0)
    def _():
        lax.fori_loop(1, layers, settle_guest, 0)
        help_copy.wait_send()

    @pl.when(layer == top_layer)
    def _():
        for copy in q_copies:
            copy.wait_send()

    for leave in leaves:
        leave.wait()


def angle_tables(seats, rows):
    frequency = rope_base ** (-np.arange(ROT_DIM // 2) / (ROT_DIM // 2))

    def table(positions):
        angles = frequency[:, None] * positions[None, :]
        return jnp.asarray(
            np.concatenate([np.cos(angles), np.sin(angles)], axis=0), jnp.float32
        )

    return table(np.arange(rows)), table(rows * np.arange(-(-seats // 128) * 128))


def fused(tokens, gains, matrices, taps, seats):
    rows, width = tokens.shape
    chans = taps.shape[1]
    rank = matrices[0].shape[1]
    heads = matrices[4].shape[1] // NOPE_DIM
    pairs = heads // 2
    keys_wide = PLANE * rows
    layers = seats // PLANE
    across = rank // 128
    height = rows + -(-(rows // 128) // across) * ROT_DIM
    vmem = pl.BlockSpec(memory_space=pltpu.VMEM)
    anywhere = pl.BlockSpec(memory_space=pltpu.HBM)
    dma = pltpu.SemaphoreType.DMA
    edge = 32
    bf16 = jnp.bfloat16
    f32 = jnp.float32
    value_rows = 2 * VALUE_DIM + 16
    base, seat = angle_tables(seats, rows)
    input_gain, kv_gain, ln_gain, ln_bias, att_gain, conv_gain = gains
    return pl.pallas_call(
        layer_kernel,
        out_shape=jax.ShapeDtypeStruct((rows, width), bf16),
        in_specs=[anywhere] + [vmem] * 9 + [anywhere] * 10,
        out_specs=anywhere,
        scratch_shapes=[pltpu.VMEM(matrix.shape, bf16) for matrix in matrices[:8]]
        + [
            pltpu.VMEM((2, matrix.shape[0], width), bf16) for matrix in matrices[8:]
        ]
        + [
            pltpu.VMEM(matrices[7].shape[::-1], bf16),
            pltpu.VMEM((rows, width), bf16),
            pltpu.VMEM((rows, width), bf16),
            pltpu.VMEM((rows, 2 * width), bf16),
            pltpu.VMEM((rows, rank), f32),
            pltpu.VMEM((rows, 128), f32),
            pltpu.VMEM((rows, chans), bf16),
            pltpu.VMEM((edge, chans), bf16),
            pltpu.VMEM((chans // 128, rows + edge, 128), f32),
            pltpu.VMEM((rows, chans), f32),
            pltpu.VMEM((rows, 256), f32),
            pltpu.VMEM((rows, 256), f32),
            pltpu.VMEM((seats, height, rank), bf16),
            pltpu.VMEM((pairs, 256, 2 * rows), bf16),
            pltpu.VMEM((2, keys_wide, heads * NOPE_DIM), bf16),
            pltpu.VMEM((2, keys_wide, 128), bf16),
            pltpu.VMEM((2, pairs, value_rows, keys_wide), bf16),
            pltpu.VMEM((max(pairs, 8), 2 * rows), f32),
            pltpu.VMEM((pairs, 2 * rows // 256, value_rows, 256), f32),
            pltpu.VMEM((2, keys_wide, 2 * rows), f32),
            pltpu.VMEM((heads * VALUE_DIM, rows), f32),
            pltpu.VMEM((rows, 128), f32),
            pltpu.VMEM((rows, 128), f32),
            pltpu.VMEM((8, rows), f32),
            pltpu.VMEM((8, rows), f32),
            pltpu.VMEM((2, rows, heads * VALUE_DIM), bf16),
            pltpu.VMEM((2, rows, chans), bf16),
            pltpu.VMEM((rows, width), bf16),
            pltpu.VMEM((rows, width), f32),
            pltpu.VMEM((rows, width), f32),
            dma((len(matrices),)),
            dma((2,)),
            dma((2,)),
        ]
        + [dma] * 13
        + [
            dma((2,)),
            dma((2,)),
            dma((layers,)),
            dma((layers,)),
            dma((layers, PLANE - 1)),
            dma((seats,)),
            dma((seats,)),
            dma((seats,)),
            dma((width // 256,)),
            pltpu.VMEM((256, 2 * rows), bf16),
            pltpu.VMEM((2 * VALUE_DIM, rows), bf16),
            pltpu.VMEM((2 * VALUE_DIM, rows), bf16),
            dma((3,)),
            dma((3,)),
            dma,
            dma,
        ],
        compiler_params=pltpu.CompilerParams(
            vmem_limit_bytes=60 << 20, collective_id=0, has_side_effects=True
        ),
        name="layer",
    )(tokens, input_gain, kv_gain, base, seat, taps, ln_gain, ln_bias, att_gain, conv_gain, *matrices)


def gathered_kernel(q_ref, lat_ref, kup_ref, vup_ref, o_ref, kt, vt, run_max, acc):
    heads, rows, lanes = q_ref.shape
    blocks = lat_ref.shape[0]
    rank = kup_ref.shape[1]
    nope = kup_ref.shape[0] // heads
    vdim = vup_ref.shape[0] // heads
    rot = lat_ref.shape[1] - rank
    wide = kt.shape[2]
    group = wide // rows
    me = lax.axis_index("sp")
    last = me // group
    kt[:, nope + rot :, :] = jnp.zeros((heads, lanes - nope - rot, wide), jnp.bfloat16)
    vt[:, vdim:, :] = jnp.ones((heads, lanes - vdim, wide), jnp.bfloat16)

    def expand(block):
        for part in range(group):
            src = jnp.minimum(block * group + part, blocks - 1)
            lat = lat_ref[src, :rank, :]
            turned = lat_ref[src, rank:, :]
            cols = slice(part * rows, (part + 1) * rows)
            keys = jnp.dot(kup_ref[...], lat, preferred_element_type=jnp.float32)
            values = jnp.dot(vup_ref[...], lat, preferred_element_type=jnp.float32)
            for head in range(heads):
                kt[head, :nope, cols] = keys[head * nope : (head + 1) * nope].astype(jnp.bfloat16)
                kt[head, nope : nope + rot, cols] = turned
                vt[head, :vdim, cols] = values[head * vdim : (head + 1) * vdim].astype(
                    jnp.bfloat16
                )

    def weigh(head, scores, top):
        weights = jnp.exp2(scores - top).astype(jnp.bfloat16)
        return lax.dot_general(
            weights, vt[head], (((1,), (1,)), ((), ())), preferred_element_type=jnp.float32
        )

    expand(last)
    key_pos = last * wide + lax.broadcasted_iota(jnp.int32, (rows, wide), 1)
    query_pos = me * rows + lax.broadcasted_iota(jnp.int32, (rows, wide), 0)
    hidden = key_pos > query_pos
    for head in range(heads):
        scores = jnp.dot(q_ref[head], kt[head], preferred_element_type=jnp.float32)
        scores = jnp.where(hidden, far_below, scores)
        top = jnp.max(scores, axis=1, keepdims=True)
        run_max[head] = jnp.broadcast_to(top, (rows, lanes))
        acc[head] = weigh(head, scores, top)

    def visit(step, carry):
        expand(step)
        for head in range(heads):
            scores = jnp.dot(q_ref[head], kt[head], preferred_element_type=jnp.float32)
            old = run_max[head]
            top = jnp.maximum(old[:, :1], jnp.max(scores, axis=1, keepdims=True))
            wide_top = jnp.broadcast_to(top, (rows, lanes))
            run_max[head] = wide_top
            acc[head] = acc[head] * jnp.exp2(old - wide_top) + weigh(head, scores, top)
        return carry

    lax.fori_loop(0, last, visit, 0)
    lane = lax.broadcasted_iota(jnp.int32, (rows, lanes), 1)
    for pair in range(heads // 2):
        halves = []
        for head in (2 * pair, 2 * pair + 1):
            total = acc[head]
            halves.append(total / pltpu.roll(total, vdim, axis=1))
        both = jnp.where(lane < vdim, halves[0], pltpu.roll(halves[1], vdim, axis=1))
        o_ref[:, pair * lanes : (pair + 1) * lanes] = both.astype(jnp.bfloat16)


def gathered_attention(q_heads, lat_all, key_up_t, value_up_t):
    heads, rows, lanes = q_heads.shape
    blocks = lat_all.shape[0]
    wide = 2 * rows if blocks % 2 == 0 else rows
    vmem = pl.BlockSpec(memory_space=pltpu.VMEM)
    return pl.pallas_call(
        gathered_kernel,
        out_shape=jax.ShapeDtypeStruct((rows, value_up_t.shape[0]), jnp.bfloat16),
        in_specs=[vmem] * 4,
        out_specs=vmem,
        scratch_shapes=[
            pltpu.VMEM((heads, lanes, wide), jnp.bfloat16),
            pltpu.VMEM((heads, lanes, wide), jnp.bfloat16),
            pltpu.VMEM((heads, rows, lanes), jnp.float32),
            pltpu.VMEM((heads, rows, lanes), jnp.float32),
        ],
        compiler_params=pltpu.CompilerParams(vmem_limit_bytes=48 << 20),
        cost_estimate=pl.CostEstimate(
            flops=20_000_000_000, bytes_accessed=8 << 20, transcendentals=20_000_000
        ),
        name="gathered_attention",
    )(q_heads, lat_all, key_up_t, value_up_t)


def conv_kernel(gated_ref, rim_ref, taps_ref, out_ref, wide):
    rows, chans = gated_ref.shape
    rim = rim_ref.shape[0]
    taps = taps_ref.shape[0]
    chunk = 64
    for part in range(chans // 128):
        cols = slice(part * 128, (part + 1) * 128)
        wide[part, :rim, :] = rim_ref[:, cols].astype(jnp.float32)
        wide[part, rim:, :] = gated_ref[:, cols].astype(jnp.float32)
        coeff = taps_ref[:, cols]

        def band(step, carry):
            base = step * chunk
            total = jnp.zeros((chunk, 128), jnp.float32)
            for tap in range(taps):
                total = total + coeff[tap : tap + 1, :] * wide[
                    part, pl.ds(base + (rim - taps + 1 + tap), chunk), :
                ]
            out_ref[pl.ds(pl.multiple_of(base, chunk), chunk), cols] = total
            return carry

        lax.fori_loop(0, rows // chunk, band, 0)


def convolve(gated, rim, taps):
    rows, chans = gated.shape
    vmem = pl.BlockSpec(memory_space=pltpu.VMEM)
    return pl.pallas_call(
        conv_kernel,
        out_shape=jax.ShapeDtypeStruct((rows, chans), jnp.float32),
        in_specs=[vmem] * 3,
        out_specs=vmem,
        scratch_shapes=[pltpu.VMEM((chans // 128, rows + rim.shape[0], 128), jnp.float32)],
        cost_estimate=pl.CostEstimate(
            flops=2 * rows * chans * 31, bytes_accessed=2 << 20, transcendentals=0
        ),
        name="depthwise",
    )(gated, rim, taps)


def shards(
    tokens,
    input_gain,
    query_weight,
    query_rot_weight,
    kv_down,
    rot_down,
    kv_gain,
    key_up,
    value_up,
    conv_value_weight,
    conv_gate_weight,
    conv_taps,
    conv_ln_gain,
    conv_ln_bias,
    att_out_gain,
    conv_out_gain,
    att_out_weight,
    conv_out_weight,
):
    tok_rows = tokens.shape[0]
    heads_here = key_up.shape[1] // NOPE_DIM
    chan_here = conv_taps.shape[1]
    weight_list = (
        query_weight,
        query_rot_weight,
        kv_down,
        rot_down,
        conv_value_weight,
        conv_gate_weight,
    )
    seats = lax.axis_size("sp")
    if (
        lax.axis_size("tp") == 2
        and seats % PLANE == 0
        and tok_rows % 128 == 0
        and heads_here % 2 == 0
        and heads_here > 2
        and seats > PLANE
    ):
        gains = (
            input_gain, kv_gain, conv_ln_gain, conv_ln_bias, att_out_gain, conv_out_gain
        )
        return fused(
            tokens,
            tuple(gain[None, :] for gain in gains),
            (
                kv_down, rot_down.T, conv_gate_weight, conv_value_weight, query_weight,
                query_rot_weight, key_up, value_up, att_out_weight, conv_out_weight,
            ),
            conv_taps,
            seats,
        )
    whole_rows = lax.all_gather(tokens, "tp", axis=1, tiled=True).astype(jnp.float32)
    scaled = (whole_rows * input_gain[None, :]).astype(jnp.bfloat16)
    row_scale = lax.rsqrt(jnp.mean(whole_rows * whole_rows, axis=1, keepdims=True) + norm_eps)

    def add_product(weight):
        return jnp.dot(scaled, weight, preferred_element_type=jnp.float32)

    summed = tuple((add_product(weight) for weight in weight_list))
    q_acc, qrot_acc, latent_raw, rot_acc, value_acc, gate_acc = summed
    positions = lax.axis_index("sp") * tok_rows + jnp.arange(tok_rows, dtype=jnp.int32)
    cos_table, sine_table = rotary_tables(positions, ROT_DIM // 2)
    fold = math.log2(math.e) / math.sqrt(NOPE_DIM + ROT_DIM)
    query_scale = row_scale * fold
    plain_q = (q_acc * query_scale).reshape(tok_rows, heads_here, NOPE_DIM)
    turned_q = rotate_half(
        (qrot_acc * query_scale).reshape(tok_rows, heads_here, ROT_DIM),
        cos_table[:, None, :],
        sine_table[:, None, :],
    )
    blank = jnp.zeros((tok_rows, heads_here, 128 - NOPE_DIM - ROT_DIM), jnp.float32)
    q_heads = jnp.transpose(
        jnp.concatenate([plain_q, turned_q, blank], axis=2).astype(jnp.bfloat16), (1, 0, 2)
    )
    latent = (
        latent_raw
        * lax.rsqrt(jnp.mean(latent_raw * latent_raw, axis=1, keepdims=True) + norm_eps)
        * kv_gain[None, :]
    ).astype(jnp.bfloat16)
    key_rot = rotate_half(rot_acc * row_scale, cos_table, sine_table).astype(jnp.bfloat16)
    gated_input = (value_acc * row_scale * jax.nn.sigmoid(gate_acc * row_scale)).astype(
        jnp.bfloat16
    )
    packed = jnp.concatenate([latent.T, key_rot.T], axis=0)
    rim_rows = shifted(gated_input[tok_rows - (KERNEL + 1) :], "sp", 1)
    conv_out = convolve(gated_input, rim_rows, conv_taps)
    moment_one, moment_two = lax.psum(
        (jnp.sum(conv_out, axis=1), jnp.sum(conv_out * conv_out, axis=1)), "tp"
    )
    mean_val = moment_one / CONV_CH
    spread = moment_two / CONV_CH - mean_val * mean_val
    normed = (conv_out - mean_val[:, None]) * lax.rsqrt(spread + norm_eps)[:, None]
    swished = jax.nn.silu(normed * conv_ln_gain[None, :] + conv_ln_bias[None, :])
    lat_all = lax.all_gather(packed, "sp", axis=0)
    attended = gathered_attention(q_heads, lat_all, key_up.T, value_up.T).astype(jnp.float32)
    att_sq, conv_sq = lax.psum(
        (
            jnp.sum(attended * attended, axis=1, keepdims=True),
            jnp.sum(swished * swished, axis=1, keepdims=True),
        ),
        "tp",
    )
    att_mixed = (
        attended * lax.rsqrt(att_sq / ATT_WIDTH + norm_eps) * att_out_gain[None, :]
    ).astype(jnp.bfloat16)
    conv_mixed = (
        swished * lax.rsqrt(conv_sq / CONV_CH + norm_eps) * conv_out_gain[None, :]
    ).astype(jnp.bfloat16)
    share = (
        jnp.dot(att_mixed, att_out_weight, preferred_element_type=jnp.float32)
        + jnp.dot(conv_mixed, conv_out_weight, preferred_element_type=jnp.float32)
    ).astype(jnp.bfloat16)
    return lax.psum_scatter(share, "tp", scatter_dimension=1, tiled=True)


def solution(mesh):
    return jax.shard_map(
        shards,
        mesh=mesh,
        in_specs=(
            P("sp", "tp"),
            P(),
            P(None, "tp"),
            P(None, "tp"),
            P(),
            P(),
            P(),
            P(None, "tp"),
            P(None, "tp"),
            P(None, "tp"),
            P(None, "tp"),
            P(None, "tp"),
            P("tp"),
            P("tp"),
            P("tp"),
            P("tp"),
            P("tp", None),
            P("tp", None),
        ),
        out_specs=P("sp", "tp"),
        check_vma=False,
    )
```
